32 devices in a mesh: grp: 2 (over y), sp: 8 (over z, core), tp: 2 (over x).
Axes of the slice: x: 2, y: 2, z: 4, core: 2. Of those that a mesh axis runs over, the one named last changes fastest.
Arguments:
- out_gate: bfloat16 [6144, 1024], P(('grp', 'sp'), 'tp'), parts along dimension 0, may hold values from -6 to 6
- in_gate: bfloat16 [6144, 1024], P(('grp', 'sp'), 'tp'), parts along dimension 0, may hold values from -6 to 6
- conv_input: bfloat16 [6144, 1024], P(('grp', 'sp'), 'tp'), parts along dimension 0, may hold values from -6 to 6
- doc_ids: int32 [6144], P(('grp', 'sp')), parts along dimension 0, may hold values from 0 to 3, never falling along the last dimension, each value on 1 to 1536 neighbouring positions
- residual: bfloat16 [6144, 2048], P(('grp', 'sp'), 'tp'), parts along dimension 0, may hold values from -6 to 6
- conv_taps: float32 [3, 1024], P(None, 'tp'), may hold values from -6 to 6
- mix_gain: float32 [1024], P('tp'), may hold values from 0.1 to 1.9
- out_weight: bfloat16 [1024, 2048], P('tp'), may hold values from -0.1875 to 0.1875
- ffn_gain: float32 [2048], P('tp'), may hold values from 0.1 to 1.9
- routing: int32 [6144, 2], P(('grp', 'sp')), parts along dimension 0, may hold values from 0 to 15, as said below
- route_weight: float32 [6144, 2], P(('grp', 'sp')), parts along dimension 0, may hold values from 0.2 to 1.2
- expert_gate: bfloat16 [16, 2048, 512], P('sp', None, 'tp'), may hold values from -0.125 to 0.125
- expert_up: bfloat16 [16, 2048, 512], P('sp', None, 'tp'), may hold values from -0.125 to 0.125
- expert_down: bfloat16 [16, 512, 2048], P('sp', None, 'tp'), may hold values from -0.25 to 0.25
- shared_gate: bfloat16 [2048, 512], P(None, 'tp'), may hold values from -0.125 to 0.125
- shared_up: bfloat16 [2048, 512], P(None, 'tp'), may hold values from -0.125 to 0.125
- shared_down: bfloat16 [512, 2048], P(None, 'tp'), may hold values from -0.25 to 0.25
Outputs:
- layer_out: bfloat16 [6144, 2048], P(('grp', 'sp'), 'tp'), parts along dimension 0
The draws below stay inside these ranges and needn't reach their ends.
There are 2 independent parts, one for each index of `grp`. The reference program is written for one: setup_inputs(seed, part) draws one part's arguments, and reference() takes and returns one part's arrays. A program takes and returns all parts, laid end to end along the dimension named above; an argument that names none is the same for every part. Nothing has to cross between parts.
Inputs may be any that keep to these rules, and one draw needn't show every extreme that they name: `routing`: each row names 2 different experts. In each aligned block of 192 rows no expert is named by more than 48 rows, and some expert is named by exactly 48 rows. `doc_ids`: never falls along the sequence; a document holds at most 1536 positions.
All inputs are finite; a program needn't handle non-finite values.
Results may differ from the reference program's by a relative error of at most 0.017.
Values may be sent and summed in bfloat16 or wider, within the bound.
A program may use at most 64 MiB of HBM per device.

```python
import math
import jax
import jax.numpy as jnp
import numpy as np
from jax import lax

D = 2048
D_CONV = 1024
E_H = 512
CONV_K = 3
TOPK = 2
EXP_DEV = 2
TOK_DEV = 384
TOKENS = 3072
EXPERTS = 16
ROWS = 192
MOST = 48
CAP_ALL = 768
DOCS = 4
DOC_MOST = 1536
N_TP = 2


def draw_conv_taps(key, part):
    key_scale = jax.random.fold_in(key, 11)
    key_taps = jax.random.fold_in(key, 12)
    scales = jnp.exp(jax.random.uniform(key_scale, (8,), jnp.float32, minval=-1.1, maxval=1.1))
    taps = jax.random.truncated_normal(key_taps, -3.0, 3.0, (CONV_K, D_CONV), jnp.float32)
    return taps * CONV_K ** (-0.5) * jnp.repeat(scales, D_CONV // 8)[None, :]


def draw_routing(key, part):
    n_dest = EXPERTS // EXP_DEV
    n_source = TOKENS // TOK_DEV
    per_source = TOK_DEV // ROWS
    n_blocks = n_source * per_source
    routes = ROWS * TOPK
    filled = routes // MOST
    dest_iota = jnp.arange(n_dest, dtype=jnp.int32)
    hot_dest = jax.random.randint(jax.random.fold_in(key, 21), (), 0, n_dest, dtype=jnp.int32)
    order_key = jax.random.fold_in(key, 22)

    def source_order(source):
        scores = jax.random.randint(jax.random.fold_in(order_key, source), (n_dest,), 0, 1 << 20, dtype=jnp.int32) * n_dest + dest_iota
        scores = jnp.where(dest_iota == hot_dest, jnp.int32(-1), scores)
        dest_order = jnp.argsort(scores).astype(jnp.int32)
        return (dest_order[:, None] * EXP_DEV + jnp.arange(EXP_DEV, dtype=jnp.int32)[None, :]).reshape(-1)
    orders = jax.vmap(source_order)(jnp.arange(n_source, dtype=jnp.int32))
    position = jnp.arange(routes, dtype=jnp.int32)
    base = filled * MOST
    which = jnp.where(position < base, position // MOST, filled + (position - base) % (EXPERTS - filled))
    listing = orders[:, which]
    listing = jnp.repeat(listing, per_source, axis=0)
    table = jnp.transpose(listing.reshape(n_blocks, TOPK, ROWS), (0, 2, 1))
    perm_key = jax.random.fold_in(key, 23)
    perms = jax.vmap(lambda block: jax.random.permutation(jax.random.fold_in(perm_key, block), ROWS).astype(jnp.int32))(jnp.arange(n_blocks, dtype=jnp.int32))
    table = jnp.take_along_axis(table, perms[:, :, None], axis=1)
    return table.reshape(TOKENS, TOPK).astype(jnp.int32)


def block_levels(stream_key, extent, cuts, least, largest):
    def one(dim, shards_of):
        heights = jax.random.uniform(jax.random.fold_in(jax.random.fold_in(stream_key, 6), dim), (shards_of,), jnp.float32, least / len(cuts), largest / len(cuts))
        return jnp.repeat(jnp.exp(heights), extent[dim] // shards_of).reshape((-1,) + (1,) * (len(extent) - dim - 1))

    gain = one(*cuts[0])
    for cut in cuts[1:]:
        gain = gain * one(*cut)
    return gain


def profile(count, total, most, lean):
    portions = [(1 << 20) // math.isqrt(grade ** lean) + 1 for grade in range(2, count + 1)]
    rest, given = total - most - (count - 1), [1] * (count - 1)
    while rest > 0:
        movable = [i for i in range(count - 1) if given[i] < most]
        mass, left = sum([portions[i] for i in movable]), rest
        for i in movable:
            extra = min(most - given[i], max(1, left * portions[i] // mass), rest)
            given[i] = given[i] + extra
            rest = rest - extra
    return np.array([most] + given)


def uneven(rng, number_of, total, limit, slope):
    if number_of == 2:
        one = jax.random.randint(rng, (), max(1, total - limit), min(limit, total - 1) + 1)
        return jnp.stack([one, total - one])
    lengths = jnp.asarray(profile(number_of, total, limit, slope), jnp.int32)
    couples = (number_of - 1) // 2
    donor, sink = lengths[1:1 + 2 * couples:2], lengths[2:2 + 2 * couples:2]
    margin = jnp.minimum(donor - 1, limit - sink)
    passed = jax.random.randint(jax.random.fold_in(rng, 1), (couples,), 0, 1 << 20) % (margin + 1)
    lengths = lengths.at[1:1 + 2 * couples:2].set(donor - passed).at[2:2 + 2 * couples:2].set(sink + passed)
    return lengths[jax.random.permutation(jax.random.fold_in(rng, 2), number_of)]


def gaussian(stream_key, extent, spread, limit, split=(), held_as=jnp.bfloat16):
    values = spread * jax.random.normal(stream_key, extent, jnp.float32)
    if split:
        values = values * block_levels(stream_key, extent, split, -0.22, 0.18)
    return jnp.clip(values, -limit, limit).astype(held_as)


def setup_inputs(seed: int = 0, part: int = 0) -> dict:
    seeds = jax.random.split(jax.random.key(seed), 18)
    own_keys = jax.random.split(jax.random.fold_in(seeds[17], part), 18)
    out_gate = gaussian(own_keys[0], (TOKENS, D_CONV), 1.0, 6.0, ((0, 8), (1, 2)))
    in_gate = gaussian(own_keys[1], (TOKENS, D_CONV), 1.0, 6.0, ((0, 8), (1, 2)))
    conv_input = gaussian(own_keys[2], (TOKENS, D_CONV), 1.0, 6.0, ((0, 8), (1, 2)))
    doc_ids = jnp.searchsorted(jnp.cumsum(uneven(own_keys[3], DOCS, TOKENS, DOC_MOST, 1)), jnp.arange(TOKENS), side="right").astype(jnp.int32)
    residual = gaussian(own_keys[4], (TOKENS, D), 1.0, 6.0, ((0, 8), (1, 2)))
    conv_taps = draw_conv_taps(jax.random.fold_in(seeds[17], 71), part)
    mix_gain = jnp.clip(1.0 + 0.18 * jax.random.normal(seeds[6], (D_CONV,), jnp.float32), 0.1, 1.9)
    out_weight = gaussian(seeds[7], (D_CONV, D), D_CONV ** -0.5, 0.1875, ((0, 2),))
    ffn_gain = jnp.clip(1.0 + 0.18 * jax.random.normal(seeds[8], (D,), jnp.float32), 0.1, 1.9)
    routing = draw_routing(jax.random.fold_in(jax.random.fold_in(seeds[17], part), 71), part)
    route_weight = jnp.clip(0.2 + 1 * jax.random.uniform(own_keys[10], (TOKENS, TOPK), jnp.float32) ** block_levels(own_keys[10], (TOKENS, TOPK), ((0, 8),), -0.2, 0.2), 0.2, 1.2)
    expert_gate = gaussian(seeds[11], (EXPERTS, D, E_H), D ** -0.5, 0.125, ((0, 8), (2, 2)))
    expert_up = gaussian(seeds[12], (EXPERTS, D, E_H), D ** -0.5, 0.125, ((0, 8), (2, 2)))
    expert_down = gaussian(seeds[13], (EXPERTS, E_H, D), E_H ** -0.5, 0.25, ((0, 8), (2, 2)))
    shared_gate = gaussian(seeds[14], (D, E_H), D ** -0.5, 0.125, ((1, 2),))
    shared_up = gaussian(seeds[15], (D, E_H), D ** -0.5, 0.125, ((1, 2),))
    shared_down = gaussian(seeds[16], (E_H, D), E_H ** -0.5, 0.25, ((1, 2),))
    return dict(out_gate=out_gate, in_gate=in_gate, conv_input=conv_input, doc_ids=doc_ids, residual=residual, conv_taps=conv_taps, mix_gain=mix_gain, out_weight=out_weight, ffn_gain=ffn_gain, routing=routing, route_weight=route_weight, expert_gate=expert_gate, expert_up=expert_up, expert_down=expert_down, shared_gate=shared_gate, shared_up=shared_up, shared_down=shared_down)


def rounded(value):
    return lax.optimization_barrier(value.astype(jnp.bfloat16)).astype(jnp.float32)

def reference(out_gate, in_gate, conv_input, doc_ids, residual, conv_taps, mix_gain, out_weight, ffn_gain, routing, route_weight, expert_gate, expert_up, expert_down, shared_gate, shared_up, shared_down):
    length = out_gate.shape[0]
    product = rounded(in_gate.astype(jnp.float32) * conv_input.astype(jnp.float32))
    extended = jnp.pad(product, ((CONV_K - 1, 0), (0, 0)))
    ext_docs = jnp.pad(doc_ids, (CONV_K - 1, 0), constant_values=-1)
    mixed = jnp.zeros(product.shape, jnp.float32)
    for k in range(CONV_K):
        keep = (ext_docs[k:k + length] == doc_ids)[:, None]
        mixed = mixed + jnp.where(keep, conv_taps[k] * extended[k:k + length], jnp.float32(0.0))
    conv_out = out_gate.astype(jnp.float32) * mixed
    scale = lax.rsqrt(lax.optimization_barrier(jnp.mean(conv_out * conv_out, axis=1, keepdims=True)) + 1e-06)
    normed = (conv_out * scale * mix_gain).astype(jnp.bfloat16)
    width = D_CONV // N_TP
    proj = jnp.zeros((length, D), jnp.float32)
    for block in range(N_TP):
        part = jnp.dot(normed[:, block * width:(block + 1) * width], out_weight[block * width:(block + 1) * width], preferred_element_type=jnp.float32)
        proj = proj + rounded(part)
    stream = (residual.astype(jnp.float32) + proj).astype(jnp.bfloat16)
    stream32 = stream.astype(jnp.float32)
    normal = (stream32 * lax.rsqrt(lax.optimization_barrier(jnp.mean(stream32 * stream32, axis=1, keepdims=True)) + 1e-06) * ffn_gain).astype(jnp.bfloat16)
    shared_hid = (jax.nn.silu(jnp.dot(normal, shared_gate, preferred_element_type=jnp.float32)) * jnp.dot(normal, shared_up, preferred_element_type=jnp.float32)).astype(jnp.bfloat16)
    shared_out = jnp.dot(shared_hid, shared_down, preferred_element_type=jnp.float32)
    padded = jnp.concatenate([normal, jnp.zeros((1, D), jnp.bfloat16)], axis=0)

    def one_expert(expert, total):
        chosen = routing == expert
        weights = lax.optimization_barrier(jnp.sum(jnp.where(chosen, route_weight, jnp.float32(0.0)), axis=1))
        weights = jnp.concatenate([weights, jnp.zeros((1,), jnp.float32)])
        index = jnp.nonzero(jnp.any(chosen, axis=1), size=CAP_ALL, fill_value=length)[0].astype(jnp.int32)
        rows = padded[index]
        gate = jnp.dot(rows, expert_gate[expert], preferred_element_type=jnp.float32)
        upper = jnp.dot(rows, expert_up[expert], preferred_element_type=jnp.float32)
        hid = (jax.nn.silu(gate) * upper).astype(jnp.bfloat16)
        result = jnp.dot(hid, expert_down[expert], preferred_element_type=jnp.float32).astype(jnp.bfloat16)
        return total.at[index].add(weights[index][:, None] * result.astype(jnp.float32))
    routed = lax.fori_loop(0, EXPERTS, one_expert, jnp.zeros((length + 1, D), jnp.float32))
    return (stream32 + shared_out + routed[:length]).astype(jnp.bfloat16)
```

```python
import functools

import jax
import jax.numpy as jnp
from jax import lax
from jax.experimental import pallas as pl
from jax.experimental.pallas import tpu as pltpu
from jax.sharding import PartitionSpec as P

D_CONV = 1024
CONV_K = 3
TOPK = 2
EXP_DEV = 2


def from_behind(value, axis, steps):
    count = lax.axis_size(axis)
    first, last = (max(0, -steps), min(count, count - steps))
    return lax.ppermute(value, axis, [(source, source + steps) for source in range(first, last)])


def body(
    out_gate,
    in_gate,
    conv_input,
    doc_ids,
    residual,
    conv_taps,
    mix_gain,
    out_weight,
    ffn_gain,
    routing,
    route_weight,
    expert_gate,
    expert_up,
    expert_down,
    shared_gate,
    shared_up,
    shared_down,
):
    tokens = residual.shape[0]
    width = out_weight.shape[1]
    n_tp = lax.axis_size("tp")
    n_sp = lax.axis_size("sp")
    rows = tokens // n_tp
    experts = n_sp * EXP_DEV
    most = max(1, 2 * rows * TOPK // experts)
    slots = n_tp * most
    total = experts * slots
    cols = expert_down.shape[2]
    product = (in_gate.astype(jnp.float32) * conv_input.astype(jnp.float32)).astype(jnp.bfloat16)
    tail = (product[tokens - CONV_K + 1 :], doc_ids[tokens - CONV_K + 1 :].astype(jnp.bfloat16))
    prev_rows, prev_docs = from_behind((tail[0], tail[1]), "sp", 1)
    extended = jnp.concatenate([prev_rows, product], axis=0).astype(jnp.float32)
    ext_docs = jnp.concatenate([prev_docs.astype(jnp.int32), doc_ids])
    mixed = jnp.zeros(product.shape, jnp.float32)
    for k in range(CONV_K):
        keep = (ext_docs[k : k + tokens] == doc_ids)[:, None]
        mixed = mixed + jnp.where(keep, conv_taps[k] * extended[k : k + tokens], jnp.float32(0.0))
    conv_out = out_gate.astype(jnp.float32) * mixed
    squares = lax.psum(jnp.sum(conv_out * conv_out, axis=1), "tp")
    normed = (conv_out * lax.rsqrt(squares / D_CONV + 1e-06)[:, None] * mix_gain).astype(
        jnp.bfloat16
    )
    partial_value = jnp.dot(normed, out_weight, preferred_element_type=jnp.float32)
    proj = lax.psum_scatter(
        partial_value.astype(jnp.bfloat16), "tp", scatter_dimension=1, tiled=True
    ).astype(jnp.float32)
    stream = (residual.astype(jnp.float32) + proj).astype(jnp.bfloat16)
    stream32 = stream.astype(jnp.float32)
    stream_sq = lax.psum(jnp.sum(stream32 * stream32, axis=1), "tp")
    normal_cols = (stream32 * lax.rsqrt(stream_sq / width + 1e-06)[:, None] * ffn_gain).astype(
        jnp.bfloat16
    )
    flat_expert = routing.reshape(-1)
    onehot = (flat_expert[:, None] == jnp.arange(experts, dtype=jnp.int32)[None, :]).astype(
        jnp.int32
    )
    blocked = onehot.reshape(n_tp, rows * TOPK, experts)
    earlier = jnp.cumsum(blocked, axis=1) - blocked
    position = jnp.sum(earlier * blocked, axis=2).reshape(-1)
    entry = jnp.arange(tokens * TOPK, dtype=jnp.int32)
    slot = flat_expert * slots + entry // (rows * TOPK) * most + position
    table = jnp.full((total,), tokens, jnp.int32).at[slot].set(entry // TOPK)
    block_rows = lax.all_to_all(normal_cols, "tp", split_axis=0, concat_axis=1, tiled=True)
    mine = lax.dynamic_index_in_dim(
        table.reshape(n_sp, EXP_DEV, n_tp, most), lax.axis_index("tp"), 2, False
    )
    local = jnp.where(mine >= tokens, rows, mine - lax.axis_index("tp") * rows)
    padded_block = jnp.concatenate([block_rows, jnp.zeros((1, width), jnp.bfloat16)], axis=0)
    got = lax.all_to_all(padded_block[local], "sp", split_axis=0, concat_axis=0, tiled=True)
    arrived, whole = (
        lax.all_gather(got, "tp", axis=2, tiled=True),
        lax.all_gather(block_rows.reshape(1, 1, rows, width), "tp", axis=2, tiled=True),
    )
    normal = whole.reshape(tokens, width)
    gate = jnp.einsum("nesd,edh->nesh", arrived, expert_gate, preferred_element_type=jnp.float32)
    upper = jnp.einsum("nesd,edh->nesh", arrived, expert_up, preferred_element_type=jnp.float32)
    hidden = (jax.nn.silu(gate) * upper).astype(jnp.bfloat16)
    hidden_flat = hidden.reshape(n_sp * EXP_DEV * slots, hidden.shape[3])
    shared_hid = (
        jax.nn.silu(jnp.dot(normal, shared_gate, preferred_element_type=jnp.float32))
        * jnp.dot(normal, shared_up, preferred_element_type=jnp.float32)
    ).astype(jnp.bfloat16)
    expert_piece = lax.all_gather(hidden_flat, "tp", axis=1, tiled=True)
    shared_piece = lax.all_gather(shared_hid, "tp", axis=1, tiled=True)
    count = expert_piece.shape[1]
    expert_part = jnp.einsum(
        "nesh,ehd->nesd",
        expert_piece.reshape(n_sp, EXP_DEV, slots, count),
        expert_down,
        preferred_element_type=jnp.float32,
    )
    shared_part = jnp.dot(shared_piece, shared_down, preferred_element_type=jnp.float32)
    returned = lax.all_to_all(
        expert_part.astype(jnp.bfloat16), "sp", split_axis=0, concat_axis=0, tiled=True
    )
    picked = (
        returned.reshape(total, cols)[slot].astype(jnp.float32) * route_weight.reshape(-1)[:, None]
    )
    routed = jnp.sum(picked.reshape(tokens, TOPK, cols), axis=1)
    return (stream32 + shared_part + routed).astype(jnp.bfloat16)


MESH = pl.DeviceIdType.MESH
F32 = jnp.float32
BF16 = jnp.bfloat16


def silu_mul(gate, upper):
    return (gate / (1.0 + jnp.exp(-gate)) * upper).astype(BF16)


def mm(a, b):
    return jnp.dot(a, b, preferred_element_type=F32)


SPLIT = 2


def plan(n_z):
    last = n_z - 1
    orders = []
    for z in range(n_z):
        near = sorted((q for q in range(n_z) if q != z), key=lambda q: (abs(q - z), -q if z < n_z / 2 else q))
        orders.append(
            [(q, 0) for q in near] + [(q, 1) for q in reversed(near)] + [(z, 0), (z, 1)]
        )
    others = 2 * last
    base = SPLIT * n_z + 1

    def digit(item):
        return item[0] * SPLIT + item[1] + 1

    def pack(lists, slots):
        codes = []
        for k in range(slots):
            value = 0
            for step in sorted(lists, reverse=True):
                here = lists[step]
                value = value * base + (digit(here[k]) if k < len(here) else 0)
            codes.append(value)
        return codes

    lead, result = 2, []
    for z in range(n_z):
        order = orders[z]
        ends = z in (0, last)
        ahead = {i: [] for i in range(-lead, others + 2 - lead)}
        for k, item in enumerate(order):
            at = k - lead if ends or k >= others else k * 2 // 3 - lead
            ahead[at] = sorted(ahead[at] + [item], key=lambda other: abs(other[0] - z))
        close = {i: [] for i in range(1, others + 3)}
        for k, item in enumerate(order[:others]):
            end = 0 if item[0] > z else last
            at = max(k, orders[end].index(item) + abs(z - end))
            close[at + 1].append(item)
        result.append(
            (
                pack({k: [item] for k, item in enumerate(order)}, 1)
                + pack(ahead, 2)
                + pack(close, 2)
            )
        )
    return result, base


def layer_kernel(
    n_z,
    most,
    og_hbm,
    ig_hbm,
    ci_hbm,
    res_hbm,
    wo_hbm,
    docs_ref,
    taps_ref,
    mix_ref,
    ffn_ref,
    own_meta,
    wg_hbm,
    wu_hbm,
    wd_hbm,
    sg_hbm,
    su_hbm,
    sd_hbm,
    out_ref,
    og,
    ig,
    ci,
    res,
    wo,
    wg,
    wu,
    wd,
    sg,
    su,
    sd,
    ext,
    dext,
    hsend,
    hrecv,
    act,
    ssq,
    srow,
    scl,
    gsend,
    grecv,
    fg,
    tri,
    blk,
    meta,
    xs,
    hid,
    shid,
    ys,
    acc,
    outgo,
    sib,
    back,
    load_sem,
    halo_sem,
    sum_sem,
    fg_sem,
    giv_send,
    giv_recv,
    z_send,
    x_send,
    c_send,
    b_recv,
    m_send,
    m_recv,
    hid_send,
    hid_recv,
    sh_send,
    sh_recv,
    sib_send,
    sib_recv,
    back_send,
    back_recv,
):
    first = [
        pltpu.make_async_copy(src, dst, load_sem.at[n])
        for n, (src, dst) in enumerate(
            ((ig_hbm, ig), (ci_hbm, ci), (og_hbm, og), (wo_hbm, wo), (res_hbm, res))
        )
    ]
    later = [
        pltpu.make_async_copy(src, dst, load_sem.at[5 + n])
        for n, (src, dst) in enumerate(
            ((wg_hbm, wg), (wu_hbm, wu), (wd_hbm, wd), (sg_hbm, sg), (su_hbm, su), (sd_hbm, sd))
        )
    ]
    for load in first:
        load.start()
    s = lax.axis_index("sp")
    t = lax.axis_index("tp")
    z = s // 2
    c = s % 2
    tokens, chan = ig.shape
    cols = out_ref.shape[1]
    width = 2 * cols
    half_rows = tokens // SPLIT
    piece = half_rows // 2
    unit = wg.shape[2]
    pad = ext.shape[0] - tokens
    lo = z > 0
    hi = z < n_z - 1
    up, down = {"sp": s + 2}, {"sp": s - 2}
    other, peer = {"sp": s + 1 - 2 * c}, {"tp": 1 - t}
    after = {"sp": s + 1}
    before = {"sp": s - 1}
    targets = (up, down, peer, other)
    n_items = SPLIT * n_z

    def remote(src, dst, ssem, rsem, dev):
        return pltpu.make_async_remote_copy(
            src_ref=src,
            dst_ref=dst,
            send_sem=ssem,
            recv_sem=rsem,
            device_id=dev,
            device_id_type=MESH,
        )

    def chunk(zq, cq, h, half, q, ssem, dev):
        ref = blk.at[zq * 2 + cq, h, half, pl.ds(q * piece, piece)]
        return remote(ref, ref, ssem, b_recv.at[zq * 2 + cq, h, half, q], dev)

    def z_copy(way, zq, half, q):
        return chunk(zq, c, t, half, q, z_send.at[way, zq, half, q], targets[way])

    def x_copy(zq, half, q):
        return chunk(zq, c, t, half, q, x_send.at[zq, half, q], peer)

    def c_copy(zq, h, half, q):
        return chunk(zq, c, h, half, q, c_send.at[zq, h, half, q], other)

    def arrived(zq, cq, h, half, q):
        chunk(zq, cq, h, half, q, c_send.at[zq, h, half, q], other).wait_recv()

    def m_copy(way, zq, cq):
        b = zq * 2 + cq
        return remote(
            meta.at[b], meta.at[b], m_send.at[way, zq], m_recv.at[b], (up, down, other)[way]
        )

    def hid_copy(zq, half):
        return remote(
            hid.at[t, zq, half],
            hid.at[t, zq, half],
            hid_send.at[zq, half],
            hid_recv.at[zq, half],
            peer,
        )

    def sh_copy(half):
        return remote(
            shid.at[t, half], shid.at[t, half], sh_send.at[half], sh_recv.at[half], peer
        )

    def sib_copy(zq, half):
        return remote(
            outgo.at[zq, half],
            sib.at[zq, half],
            sib_send.at[zq, half],
            sib_recv.at[zq, half],
            other,
        )

    def back_copy(zq, half, q, to, dev):
        return remote(
            acc.at[zq, half, pl.ds(q * piece, piece)],
            back.at[to, half, pl.ds(q * piece, piece)],
            back_send.at[zq, half, q],
            back_recv.at[to, half, q],
            dev,
        )

    def halo_copy():
        return remote(hsend, hrecv, halo_sem.at[0], halo_sem.at[1], after)

    def sum_copy():
        return remote(srow.at[0], srow.at[1], sum_sem.at[0], sum_sem.at[1], peer)

    def fg_copy():
        return remote(fg.at[t], fg.at[t], fg_sem.at[0], fg_sem.at[1], peer)

    def giv_copy(r):
        return remote(gsend.at[r], grecv.at[r], giv_send.at[r], giv_recv.at[r], peer)

    barrier = pltpu.get_barrier_semaphore()
    cross_up = hi & (c == 1)
    cross_down = lo & (c == 0)
    for target, there in ((up, hi), (down, lo), (after, cross_up), (before, cross_down)):

        @pl.when(there)
        def _():
            pl.semaphore_signal(barrier, inc=1, device_id=target, device_id_type=MESH)

    for target in (peer, other):
        pl.semaphore_signal(barrier, inc=1, device_id=target, device_id_type=MESH)

    has_next = s < 2 * n_z - 1
    has_prev = s > 0
    first[0].wait()
    first[1].wait()

    tail = 16

    def product(rows):
        return (ig[rows, :].astype(F32) * ci[rows, :].astype(F32)).astype(BF16).astype(F32)

    end_rows = product(pl.ds(tokens - tail, tail))
    hsend[:, :chan] = end_rows[tail - 8 :]
    hsend[:, chan:] = docs_ref[tokens - 8 :, :]
    fg[t] = jnp.broadcast_to(ffn_ref[...], fg.shape[1:])
    arrivals = (
        2
        + lo.astype(jnp.int32)
        + hi.astype(jnp.int32)
        + cross_up.astype(jnp.int32)
        + cross_down.astype(jnp.int32)
    )
    pl.semaphore_wait(barrier, arrivals)

    @pl.when(has_next)
    def _():
        halo_copy().start()

    fg_copy().start()
    meta[z * 2 + c] = own_meta[...]

    @pl.when(hi)
    def _():
        m_copy(0, z, c).start()

    @pl.when(lo)
    def _():
        m_copy(1, z, c).start()

    m_copy(2, z, c).start()

    step_rows = 32

    @pl.loop(0, tokens // step_rows)
    def _(i):
        at = pl.multiple_of(i * step_rows, step_rows)
        ext[pl.ds(pad + at, step_rows), :] = product(pl.ds(at, step_rows))
        dext[pl.ds(pad + at, step_rows), :] = docs_ref[pl.ds(at, step_rows), :]

    n_tri = tri.shape[0]
    row_id = lax.broadcasted_iota(jnp.int32, (n_tri, n_tri), 0)
    col_id = lax.broadcasted_iota(jnp.int32, (n_tri, n_tri), 1)
    tri[...] = (row_id < col_id).astype(F32).astype(BF16)
    for load in first[2:]:
        load.wait()
    for load in later:
        load.start()

    @pl.when(has_prev)
    def _():
        halo_copy().wait_recv()
        ext[pad - 8 : pad, :] = hrecv[:, :chan]
        dext[pad - 8 : pad, :] = hrecv[:, chan:]

    @pl.when(jnp.logical_not(has_prev))
    def _():
        ext[pad - 8 : pad, :] = jnp.zeros((8, chan), F32)
        dext[pad - 8 : pad, :] = jnp.zeros((8, dext.shape[1]), F32)

    lanes = dext.shape[1]

    @pl.loop(0, tokens // step_rows)
    def _(i):
        at = pl.multiple_of(i * step_rows, step_rows)
        v = ext[pl.ds(pl.multiple_of(pad - 8 + at, 8), step_rows + 8), :]
        d = dext[pl.ds(pl.multiple_of(pad - 8 + at, 8), step_rows + 8), :]
        doc = d[8:]
        mixed = None
        for k in range(CONV_K):
            by = CONV_K - 1 - k
            if by:
                same = (pltpu.roll(d, by, 0)[8:] == doc).astype(F32)
                same = jnp.concatenate([same] * (chan // lanes), axis=1)
                term = taps_ref[k : k + 1, :] * pltpu.roll(v, by, 0)[8:] * same
            else:
                term = taps_ref[k : k + 1, :] * v[8:]
            mixed = term if mixed is None else mixed + term
        rows = pl.ds(at, step_rows)
        conv_out = og[rows, :].astype(F32) * mixed
        total = jnp.sum(conv_out * conv_out, axis=1, keepdims=True)
        ssq[rows, :] = jnp.broadcast_to(total, (step_rows, lanes))
        act[rows, :] = (conv_out * mix_ref[...]).astype(BF16)

    eye = lax.broadcasted_iota(jnp.int32, (lanes, lanes), 0) == lax.broadcasted_iota(
        jnp.int32, (lanes, lanes), 1
    )
    for k in range(tokens // lanes):
        part = ssq[k * lanes : (k + 1) * lanes, :]
        line = jnp.sum(jnp.where(eye, part, F32(0.0)), axis=0, keepdims=True)
        srow[0, :, k * lanes : (k + 1) * lanes] = jnp.broadcast_to(line, (8, lanes))
    sum_copy().start()

    n_chunks = 2 * SPLIT

    def out_cols(who):
        return pl.ds(pl.multiple_of(who * cols, cols), cols)

    for r in range(n_chunks):
        gsend[r] = mm(act[r * piece : (r + 1) * piece, :], wo[:, out_cols(1 - t)]).astype(BF16)
        giv_copy(r).start()

    sum_copy().wait_recv()
    for k in range(tokens // lanes):
        line = srow[1, 0:1, k * lanes : (k + 1) * lanes]
        theirs = jnp.sum(jnp.where(eye, line, F32(0.0)), axis=1, keepdims=True)
        whole = ssq[k * lanes : (k + 1) * lanes, :] + theirs
        scl[k * lanes : (k + 1) * lanes, :] = lax.rsqrt(whole / (2 * chan) + 1e-06)

    for r in range(n_chunks):
        half, q = divmod(r, 2)
        rows = slice(r * piece, (r + 1) * piece)
        kept = mm(act[rows, :], wo[:, out_cols(t)])
        giv_copy(r).wait_recv()
        proj = (kept + grecv[r].astype(F32)) * scl[rows, 0:1]
        blk[z * 2 + c, t, half, q * piece : (q + 1) * piece, :] = (
            res[rows, :].astype(F32) + proj
        ).astype(BF16)

        if half == 0:
            go_up, go_down = hi, lo
        else:
            go_up, go_down = hi & jnp.logical_not(lo), lo & jnp.logical_not(hi)

        @pl.when(go_up)
        def _():
            z_copy(0, z, half, q).start()

        @pl.when(go_down)
        def _():
            z_copy(1, z, half, q).start()

        c_copy(z, t, half, q).start()

    fg_copy().wait_recv()
    for load in later:
        load.wait()

    def picks(zq, cq, half):
        info = meta[zq * 2 + cq, half][:, :half_rows]
        mine = (lax.broadcasted_iota(jnp.int32, (8, half_rows), 0) + s * EXP_DEV).astype(F32)
        hot0 = info[0:1] == mine
        hot1 = info[1:2] == mine
        hot = hot0 | hot1
        earlier = mm(hot.astype(F32).astype(BF16), tri[...])
        position = jnp.where(hot, earlier, F32(-1.0))
        weight = jnp.where(hot0, info[2:3], F32(0.0)) + jnp.where(hot1, info[3:4], F32(0.0))
        place = lax.broadcasted_iota(jnp.int32, (most, half_rows), 0).astype(F32)
        chosen = [(position[e : e + 1] == place).astype(F32) for e in range(EXP_DEV)]
        return chosen, weight

    def norm_scale(parts):
        total = sum(jnp.sum(part * part, axis=1, keepdims=True) for part in parts)
        return lax.rsqrt(total / width + 1e-06)

    def normal_of(parts):
        scale = norm_scale(parts)
        return [(part * scale * fg[h, 0:1, :]).astype(BF16) for h, part in enumerate(parts)]

    def sides():
        return [(0, c), (1, 1 - c)]

    def hidden(zq, half):
        for p, cq in sides():
            chosen, _ = picks(zq, cq, half)
            sel = jnp.concatenate(chosen, axis=0).astype(BF16)
            got = normal_of([mm(sel, blk[zq * 2 + cq, h, half]) for h in range(2)])
            for h in range(2):
                for e in range(EXP_DEV):
                    xs[e, p * most : (p + 1) * most, h * cols : (h + 1) * cols] = got[h][
                        e * most : (e + 1) * most
                    ]
        for e in range(EXP_DEV):
            hid[t, zq, half, e] = silu_mul(mm(xs[e], wg[e]), mm(xs[e], wu[e]))

    def shared(half):
        whole = normal_of([blk[z * 2 + c, h, half].astype(F32) for h in range(2)])
        gate = mm(whole[0], sg[:cols, :]) + mm(whole[1], sg[cols:, :])
        upper = mm(whole[0], su[:cols, :]) + mm(whole[1], su[cols:, :])
        shid[t, half] = silu_mul(gate, upper)

    def results(zq, half):
        hid_copy(zq, half).wait_recv()
        for e in range(EXP_DEV):
            ys[e] = (
                mm(hid[0, zq, half, e], wd[e, :unit, :]) + mm(hid[1, zq, half, e], wd[e, unit:, :])
            ).astype(BF16)
        for p, cq in sides():
            chosen, weight = picks(zq, cq, half)
            parts = []
            for e in range(EXP_DEV):
                scale = jnp.sum(chosen[e] * weight[e : e + 1], axis=1, keepdims=True)
                part = ys[e, p * most : (p + 1) * most, :].astype(F32)
                parts.append((part * scale).astype(BF16))
            sel = jnp.concatenate(chosen, axis=0).astype(BF16)
            into = acc if p == 0 else outgo
            into[zq, half] = lax.dot_general(
                sel,
                jnp.concatenate(parts, axis=0),
                (((0,), (0,)), ((), ())),
                preferred_element_type=F32,
            ).astype(BF16)
        sib_copy(zq, half).start()

    def is_end(zq):
        return ((zq > z) & jnp.logical_not(lo)) | ((zq < z) & jnp.logical_not(hi))

    def combine(zq, half):
        sib_copy(zq, half).wait_recv()
        end = is_end(zq)
        for q in range(2):
            rows = slice(q * piece, (q + 1) * piece)

            @pl.when(end)
            def _():
                acc[zq, half, rows, :] = (
                    acc[zq, half, rows, :].astype(F32) + sib[zq, half, rows, :].astype(F32)
                ).astype(BF16)

            @pl.when(jnp.logical_not(end))
            def _():
                back_copy(zq, half, q, zq, up).wait_recv()
                acc[zq, half, rows, :] = (
                    acc[zq, half, rows, :].astype(F32)
                    + sib[zq, half, rows, :].astype(F32)
                    + back[zq, half, rows, :].astype(F32)
                ).astype(BF16)

            @pl.when(zq > z)
            def _():
                back_copy(zq, half, q, zq, up).start()

            @pl.when(zq < z - 1)
            def _():
                back_copy(zq, half, q, zq, down).start()

            @pl.when(zq == z - 1)
            def _():
                back_copy(zq, half, q, n_z, down).start()

    def pass_ahead(zq, half):
        @pl.when((zq != z) & (half == 0))
        def _():
            m_copy(2, zq, c).wait_recv()

            @pl.when((zq < z) & hi)
            def _():
                m_copy(0, zq, c).start()

            @pl.when((zq > z) & lo)
            def _():
                m_copy(1, zq, c).start()

            m_copy(2, zq, c).start()

        for q in range(2):

            @pl.when(zq != z)
            def _():
                arrived(zq, c, t, half, q)

                @pl.when((zq < z) & hi)
                def _():
                    z_copy(0, zq, half, q).start()

                @pl.when((zq > z) & lo)
                def _():
                    z_copy(1, zq, half, q).start()

                c_copy(zq, t, half, q).start()

            x_copy(zq, half, q).start()

        @pl.when((zq == z - 1) & (half == 1) & hi)
        def _():
            for q in range(2):
                z_copy(0, z, 1, q).start()

        @pl.when((zq == z + 1) & (half == 1) & lo)
        def _():
            for q in range(2):
                z_copy(1, z, 1, q).start()

    def pass_across(zq, half):
        for q in range(2):
            arrived(zq, c, 1 - t, half, q)
            c_copy(zq, 1 - t, half, q).start()

    def gathered(zq, half):
        @pl.when(half == 0)
        def _():
            m_copy(2, zq, 1 - c).wait_recv()

        for h in range(2):
            for q in range(2):
                arrived(zq, 1 - c, h, half, q)

    def item(code):
        return (code - 1) // SPLIT, (code - 1) % SPLIT

    tables, base = plan(n_z)
    codes = []
    for k in range(len(tables[0])):
        value = 0
        for zz in range(n_z):
            value = value + (z == zz).astype(jnp.int32) * tables[zz][k]
        codes.append(value)

    def turn(i, carry):
        now, ahead0, ahead1, close0, close1, prev = carry
        here = i >= 2
        cur = jnp.where(here, now % base, 0)

        @pl.when(cur > 0)
        def _():
            pass_across(*item(cur))

        @pl.when(prev > 0)
        def _():
            results(*item(prev))

        @pl.when(cur > 0)
        def _():
            zq, half = item(cur)
            gathered(zq, half)
            hidden(zq, half)
            hid_copy(zq, half).start()

            @pl.when(zq == z)
            def _():
                shared(half)
                sh_copy(half).start()

        @pl.loop(0, 2)
        def _(k):
            code = ahead0 % base * (1 - k) + ahead1 % base * k

            @pl.when(code > 0)
            def _():
                pass_ahead(*item(code))

        closing = i >= 3

        @pl.when(closing)
        def _():
            @pl.loop(0, 2)
            def _(k):
                code = close0 % base * (1 - k) + close1 % base * k

                @pl.when(code > 0)
                def _():
                    combine(*item(code))

        def shift(value, live):
            return jnp.where(live, value // base, value)

        return (
            shift(now, here),
            ahead0 // base,
            ahead1 // base,
            shift(close0, closing),
            shift(close1, closing),
            cur,
        )

    lax.fori_loop(0, n_items + 3, turn, tuple(codes) + (jnp.int32(0),))

    for half in range(SPLIT):
        sib_copy(z, half).wait_recv()
        sh_copy(half).wait_recv()
        for q in range(2):

            @pl.when(lo)
            def _():
                back_copy(z, half, q, z, up).wait_recv()

            @pl.when(hi)
            def _():
                back_copy(z, half, q, n_z, up).wait_recv()

            rows = slice(q * piece, (q + 1) * piece)
            fin = (
                blk[z * 2 + c, t, half, rows, :].astype(F32)
                + mm(shid[0, half, rows, :], sd[:unit, :])
                + mm(shid[1, half, rows, :], sd[unit:, :])
                + acc[z, half, rows, :].astype(F32)
                + sib[z, half, rows, :].astype(F32)
            )
            low = jnp.where(lo, back[z, half, rows, :].astype(F32), F32(0.0))
            high = jnp.where(hi, back[n_z, half, rows, :].astype(F32), F32(0.0))
            at = half * half_rows + q * piece
            out_ref[at : at + piece, :] = (fin + low + high).astype(BF16)

    @pl.when(has_next)
    def _():
        halo_copy().wait_send()

    fg_copy().wait_send()
    sum_copy().wait_send()
    for r in range(n_chunks):
        giv_copy(r).wait_send()
    for half in range(SPLIT):
        sh_copy(half).wait_send()

    @pl.loop(0, n_z)
    def _(zq):
        @pl.when(hi & (zq <= z))
        def _():
            m_copy(0, zq, c).wait_send()
            for half in range(SPLIT):
                for q in range(2):
                    z_copy(0, zq, half, q).wait_send()

        @pl.when(lo & (zq >= z))
        def _():
            m_copy(1, zq, c).wait_send()
            for half in range(SPLIT):
                for q in range(2):
                    z_copy(1, zq, half, q).wait_send()

        m_copy(2, zq, c).wait_send()
        for half in range(SPLIT):
            for q in range(2):
                x_copy(zq, half, q).wait_send()
                for h in range(2):
                    c_copy(zq, h, half, q).wait_send()

                @pl.when(zq != z)
                def _():
                    back_copy(zq, half, q, zq, up).wait_send()

            hid_copy(zq, half).wait_send()
            sib_copy(zq, half).wait_send()


def fast(
    out_gate,
    in_gate,
    conv_input,
    doc_ids,
    residual,
    conv_taps,
    mix_gain,
    out_weight,
    ffn_gain,
    routing,
    route_weight,
    expert_gate,
    expert_up,
    expert_down,
    shared_gate,
    shared_up,
    shared_down,
):
    tokens, cols = residual.shape
    chan, width = out_weight.shape
    n_tp, n_sp = lax.axis_size("tp"), lax.axis_size("sp")
    n_z = n_sp // 2
    rows = tokens // n_tp
    experts = n_sp * EXP_DEV
    most = max(1, 2 * rows * TOPK // experts)
    lanes = 128
    docs = jnp.broadcast_to(doc_ids.astype(F32)[:, None], (tokens, lanes))
    info = jnp.concatenate([routing.astype(F32), route_weight], axis=1)
    info = info.reshape(SPLIT, rows, 2 * TOPK).transpose(0, 2, 1)
    info = jnp.pad(info, ((0, 0), (0, 8 - 2 * TOPK), (0, -rows % lanes)), constant_values=-1.0)

    piece = rows // 2
    blocks = n_sp
    unit = expert_gate.shape[2]
    vm = pl.BlockSpec(memory_space=pltpu.VMEM)
    hbm = pl.BlockSpec(memory_space=pl.ANY)
    dma = pltpu.SemaphoreType.DMA
    return pl.pallas_call(
        functools.partial(layer_kernel, n_z, most),
        out_shape=jax.ShapeDtypeStruct((tokens, cols), BF16),
        in_specs=[hbm] * 5 + [vm] * 5 + [hbm] * 6,
        out_specs=vm,
        scratch_shapes=[
            pltpu.VMEM((tokens, chan), BF16),
            pltpu.VMEM((tokens, chan), BF16),
            pltpu.VMEM((tokens, chan), BF16),
            pltpu.VMEM((tokens, cols), BF16),
            pltpu.VMEM((chan, width), BF16),
            pltpu.VMEM(expert_gate.shape, BF16),
            pltpu.VMEM(expert_up.shape, BF16),
            pltpu.VMEM(expert_down.shape, BF16),
            pltpu.VMEM(shared_gate.shape, BF16),
            pltpu.VMEM(shared_up.shape, BF16),
            pltpu.VMEM(shared_down.shape, BF16),
            pltpu.VMEM((tokens + 16, chan), F32),
            pltpu.VMEM((tokens + 16, lanes), F32),
            pltpu.VMEM((8, chan + lanes), F32),
            pltpu.VMEM((8, chan + lanes), F32),
            pltpu.VMEM((tokens, chan), BF16),
            pltpu.VMEM((tokens, lanes), F32),
            pltpu.VMEM((2, 8, tokens), F32),
            pltpu.VMEM((tokens, lanes), F32),
            pltpu.VMEM((2 * SPLIT, piece, cols), BF16),
            pltpu.VMEM((2 * SPLIT, piece, cols), BF16),
            pltpu.VMEM((2, 8, cols), F32),
            pltpu.VMEM((rows, rows), BF16),
            pltpu.VMEM((blocks, 2, SPLIT, rows, cols), BF16),
            pltpu.VMEM((blocks,) + info.shape, F32),
            pltpu.VMEM((EXP_DEV, 2 * most, width), BF16),
            pltpu.VMEM((2, n_z, SPLIT, EXP_DEV, 2 * most, unit), BF16),
            pltpu.VMEM((2, SPLIT, rows, unit), BF16),
            pltpu.VMEM((EXP_DEV, 2 * most, cols), BF16),
            pltpu.VMEM((n_z, SPLIT, rows, cols), BF16),
            pltpu.VMEM((n_z, SPLIT, rows, cols), BF16),
            pltpu.VMEM((n_z, SPLIT, rows, cols), BF16),
            pltpu.VMEM((n_z + 1, SPLIT, rows, cols), BF16),
            dma((11,)),
            dma((2,)),
            dma((2,)),
            dma((2,)),
            dma((2 * SPLIT,)),
            dma((2 * SPLIT,)),
            dma((2, n_z, SPLIT, 2)),
            dma((n_z, SPLIT, 2)),
            dma((n_z, 2, SPLIT, 2)),
            dma((blocks, 2, SPLIT, 2)),
            dma((3, n_z)),
            dma((blocks,)),
            dma((n_z, SPLIT)),
            dma((n_z, SPLIT)),
            dma((SPLIT,)),
            dma((SPLIT,)),
            dma((n_z, SPLIT)),
            dma((n_z, SPLIT)),
            dma((n_z, SPLIT, 2)),
            dma((n_z + 1, SPLIT, 2)),
        ],
        compiler_params=pltpu.CompilerParams(
            collective_id=0, has_side_effects=True, vmem_limit_bytes=64 * 1024 * 1024 - 65536
        ),
    )(
        out_gate,
        in_gate,
        conv_input,
        residual,
        out_weight,
        docs,
        conv_taps,
        mix_gain[None, :],
        ffn_gain[None, :],
        info,
        expert_gate,
        expert_up,
        expert_down,
        shared_gate,
        shared_up,
        shared_down,
    )


def fits(mesh):
    return mesh.shape["tp"] == 2 and mesh.shape["sp"] in (4, 6, 8)


def solution(mesh):
    return jax.shard_map(
        fast if fits(mesh) else body,
        mesh=mesh,
        in_specs=(
            P(("grp", "sp"), "tp"),
            P(("grp", "sp"), "tp"),
            P(("grp", "sp"), "tp"),
            P(("grp", "sp")),
            P(("grp", "sp"), "tp"),
            P(None, "tp"),
            P("tp"),
            P("tp", None),
            P("tp"),
            P(("grp", "sp"), None),
            P(("grp", "sp"), None),
            P("sp", None, "tp"),
            P("sp", None, "tp"),
            P("sp", None, "tp"),
            P(None, "tp"),
            P(None, "tp"),
            P(None, "tp"),
        ),
        out_specs=P(("grp", "sp"), "tp"),
        check_vma=False,
    )
```

```python
import functools

import jax
import jax.numpy as jnp
from jax import lax
from jax.experimental import pallas as pl
from jax.experimental.pallas import tpu as pltpu
from jax.sharding import PartitionSpec as P

D_CONV = 1024
CONV_K = 3
TOPK = 2
EXP_DEV = 2


def from_behind(value, axis, steps):
    count = lax.axis_size(axis)
    first, last = (max(0, -steps), min(count, count - steps))
    return lax.ppermute(value, axis, [(source, source + steps) for source in range(first, last)])


def body(
    out_gate,
    in_gate,
    conv_input,
    doc_ids,
    residual,
    conv_taps,
    mix_gain,
    out_weight,
    ffn_gain,
    routing,
    route_weight,
    expert_gate,
    expert_up,
    expert_down,
    shared_gate,
    shared_up,
    shared_down,
):
    tokens = residual.shape[0]
    width = out_weight.shape[1]
    n_tp = lax.axis_size("tp")
    n_sp = lax.axis_size("sp")
    rows = tokens // n_tp
    experts = n_sp * EXP_DEV
    most = max(1, 2 * rows * TOPK // experts)
    slots = n_tp * most
    total = experts * slots
    cols = expert_down.shape[2]
    product = (in_gate.astype(jnp.float32) * conv_input.astype(jnp.float32)).astype(jnp.bfloat16)
    tail = (product[tokens - CONV_K + 1 :], doc_ids[tokens - CONV_K + 1 :].astype(jnp.bfloat16))
    prev_rows, prev_docs = from_behind((tail[0], tail[1]), "sp", 1)
    extended = jnp.concatenate([prev_rows, product], axis=0).astype(jnp.float32)
    ext_docs = jnp.concatenate([prev_docs.astype(jnp.int32), doc_ids])
    mixed = jnp.zeros(product.shape, jnp.float32)
    for k in range(CONV_K):
        keep = (ext_docs[k : k + tokens] == doc_ids)[:, None]
        mixed = mixed + jnp.where(keep, conv_taps[k] * extended[k : k + tokens], jnp.float32(0.0))
    conv_out = out_gate.astype(jnp.float32) * mixed
    squares = lax.psum(jnp.sum(conv_out * conv_out, axis=1), "tp")
    normed = (conv_out * lax.rsqrt(squares / D_CONV + 1e-06)[:, None] * mix_gain).astype(
        jnp.bfloat16
    )
    partial_value = jnp.dot(normed, out_weight, preferred_element_type=jnp.float32)
    proj = lax.psum_scatter(
        partial_value.astype(jnp.bfloat16), "tp", scatter_dimension=1, tiled=True
    ).astype(jnp.float32)
    stream = (residual.astype(jnp.float32) + proj).astype(jnp.bfloat16)
    stream32 = stream.astype(jnp.float32)
    stream_sq = lax.psum(jnp.sum(stream32 * stream32, axis=1), "tp")
    normal_cols = (stream32 * lax.rsqrt(stream_sq / width + 1e-06)[:, None] * ffn_gain).astype(
        jnp.bfloat16
    )
    flat_expert = routing.reshape(-1)
    onehot = (flat_expert[:, None] == jnp.arange(experts, dtype=jnp.int32)[None, :]).astype(
        jnp.int32
    )
    blocked = onehot.reshape(n_tp, rows * TOPK, experts)
    earlier = jnp.cumsum(blocked, axis=1) - blocked
    position = jnp.sum(earlier * blocked, axis=2).reshape(-1)
    entry = jnp.arange(tokens * TOPK, dtype=jnp.int32)
    slot = flat_expert * slots + entry // (rows * TOPK) * most + position
    table = jnp.full((total,), tokens, jnp.int32).at[slot].set(entry // TOPK)
    block_rows = lax.all_to_all(normal_cols, "tp", split_axis=0, concat_axis=1, tiled=True)
    mine = lax.dynamic_index_in_dim(
        table.reshape(n_sp, EXP_DEV, n_tp, most), lax.axis_index("tp"), 2, False
    )
    local = jnp.where(mine >= tokens, rows, mine - lax.axis_index("tp") * rows)
    padded_block = jnp.concatenate([block_rows, jnp.zeros((1, width), jnp.bfloat16)], axis=0)
    got = lax.all_to_all(padded_block[local], "sp", split_axis=0, concat_axis=0, tiled=True)
    arrived, whole = (
        lax.all_gather(got, "tp", axis=2, tiled=True),
        lax.all_gather(block_rows.reshape(1, 1, rows, width), "tp", axis=2, tiled=True),
    )
    normal = whole.reshape(tokens, width)
    gate = jnp.einsum("nesd,edh->nesh", arrived, expert_gate, preferred_element_type=jnp.float32)
    upper = jnp.einsum("nesd,edh->nesh", arrived, expert_up, preferred_element_type=jnp.float32)
    hidden = (jax.nn.silu(gate) * upper).astype(jnp.bfloat16)
    hidden_flat = hidden.reshape(n_sp * EXP_DEV * slots, hidden.shape[3])
    shared_hid = (
        jax.nn.silu(jnp.dot(normal, shared_gate, preferred_element_type=jnp.float32))
        * jnp.dot(normal, shared_up, preferred_element_type=jnp.float32)
    ).astype(jnp.bfloat16)
    expert_piece = lax.all_gather(hidden_flat, "tp", axis=1, tiled=True)
    shared_piece = lax.all_gather(shared_hid, "tp", axis=1, tiled=True)
    count = expert_piece.shape[1]
    expert_part = jnp.einsum(
        "nesh,ehd->nesd",
        expert_piece.reshape(n_sp, EXP_DEV, slots, count),
        expert_down,
        preferred_element_type=jnp.float32,
    )
    shared_part = jnp.dot(shared_piece, shared_down, preferred_element_type=jnp.float32)
    returned = lax.all_to_all(
        expert_part.astype(jnp.bfloat16), "sp", split_axis=0, concat_axis=0, tiled=True
    )
    picked = (
        returned.reshape(total, cols)[slot].astype(jnp.float32) * route_weight.reshape(-1)[:, None]
    )
    routed = jnp.sum(picked.reshape(tokens, TOPK, cols), axis=1)
    return (stream32 + shared_part + routed).astype(jnp.bfloat16)


MESH = pl.DeviceIdType.MESH
F32 = jnp.float32
BF16 = jnp.bfloat16


def silu_mul(gate, upper):
    return (gate / (1.0 + jnp.exp(-gate)) * upper).astype(BF16)


def mm(a, b):
    return jnp.dot(a, b, preferred_element_type=F32)


SPLIT = 2


FULL = ((0, 1), (0, 1))
HOP, START, DEPTH = 2.8, 6.0, 1.0
W = (8.4, 6.0, 3.8, -3.3, 5.9, 4.9, 4.7, -4.7, -0.8, 1.6, 5.9, 3.4, 5.6)
KINDS = ("stream", "land", "up", "down", "across", "hidden", "result", "combine")


def full_rows(n_z, source, target, half, q):
    return abs(source - target) == 1 and half * 2 + q in FULL[0 < target < n_z - 1]


def plan(n_z):
    wire, hop, near = 4.2, HOP, 1.6
    cost = dict(
        stream=0.35, land=0.1, up=0.1, down=0.1, across=0.1, hidden=1.7, result=1.35, combine=0.3
    )
    chunks = [(half, q) for half in range(SPLIT) for q in range(2)]
    zones = range(n_z)
    have, told, heard, summed, went = {}, {}, {}, {}, {}
    todo = {z: [] for z in zones}
    for z in zones:
        for k, (half, q) in enumerate(chunks):
            todo[z].append(("stream", z, 0, half, q))
            went[z, z, half, q] = START + wire * (k + 1) + hop
        for zq in zones:
            for half, q in chunks:
                if zq != z:
                    todo[z].append(("land", zq, 0, half, q))
                todo[z].append(("land", zq, 1, half, q))
                if zq <= z < n_z - 1:
                    todo[z].append(("up", zq, 0, half, q))
                if zq >= z > 0:
                    todo[z].append(("down", zq, 0, half, q))
                if not full_rows(n_z, zq, z, half, q):
                    todo[z].append(("across", zq, 0, half, q))
            for half in range(SPLIT):
                todo[z].append(("hidden", zq, 0, half, 0))
                todo[z].append(("result", zq, 0, half, 0))
                if zq != z:
                    todo[z] += [("combine", zq, 0, half, q) for q in range(2)]
        for half, q in chunks:
            if z < n_z - 1 and full_rows(n_z, z, z + 1, half, q):
                todo[z].append(("up", z, 1, half, q))
            if z > 0 and full_rows(n_z, z, z - 1, half, q):
                todo[z].append(("down", z, 1, half, q))
    arrive = {}
    link = {(z, way): 0.0 for z in zones for way in ("up", "down", "across")}
    for z in zones:
        link[z, "across"] = START + wire * len(chunks)
    core = {z: 0.0 for z in zones}
    never = 1e9

    def put(z, way, now, size):
        begin = max(now, link[z, way])
        link[z, way] = begin + wire * size
        return link[z, way] + hop

    def ready(z, event):
        kind, zq, h, half, q = event
        if kind == "stream":
            return went[z, z, half, q]
        if kind == "land":
            return arrive.get((z, zq, h, half, q), never)
        if kind in ("up", "down", "across"):
            return max(have.get((z, zq, h, half, q), never), link[z, kind] - DEPTH)
        if kind == "hidden":
            return max(have.get((z, zq, g, half, p), never) for g in range(2) for p in range(2)) + near
        if kind == "result":
            return heard.get((z, zq, half), never)
        before = z - 1 if zq > z else z + 1
        coming = summed.get((before, zq, half, q), never) if 0 <= before < n_z else 0.0
        return max(told.get((z, zq, half), never), coming)

    def rank(z, event):
        kind, zq, h, half, q = event
        away = abs(zq - z)
        if kind in ("stream", "land"):
            return (0, 0.0)
        if kind == "combine":
            return (1, W[12] * away + half)
        if kind in ("result", "hidden"):
            return (2, (kind == "hidden") * 1.0, W[11] * away)
        if kind == "across":
            return (3, W[away] + W[4] * half, q)
        return (3, (W[9] if h else W[5 + away]) + W[10] * half, q)

    order = {z: [] for z in zones}
    while any(todo.values()):
        best = None
        for z in zones:
            if not todo[z]:
                continue
            starts = [(max(core[z], ready(z, event)), event) for event in todo[z]]
            at = min(start for start, _ in starts)
            if best is None or at < best[0]:
                best = (at, z, starts)
        at, z, starts = best
        assert at < never
        event = min((e for start, e in starts if start <= at), key=lambda e: rank(z, e))
        kind, zq, h, half, q = event
        todo[z].remove(event)
        order[z].append(event)
        end = at + cost[kind] + (0.9 if kind == "hidden" and zq == z else 0.0)
        core[z] = end
        if kind in ("stream", "land"):
            have[z, zq, h, half, q] = end
        elif kind in ("up", "down"):
            arrive[z + (1 if kind == "up" else -1), zq, h, half, q] = put(z, kind, end, 1)
        elif kind == "across":
            arrive[z, zq, 1, half, q] = put(z, kind, end, 1)
        elif kind == "hidden":
            heard[z, zq, half] = put(z, "across", end, 1.0 if zq == z else 0.5)
        elif kind == "result":
            told[z, zq, half] = end + 2.2
        else:
            summed[z, zq, half, q] = put(z, "up" if zq > z else "down", end, 1)
    done = max(max(core.values()), max(summed.values()))
    return order, done


def encode(events):
    codes = [
        (((KINDS.index(kind) * 4 + zq) * 2 + h) * 2 + half) * 2 + q
        for kind, zq, h, half, q in events
    ]
    return [
        sum(code << (8 * k) for k, code in enumerate(codes[at : at + 3]))
        for at in range(0, len(codes), 3)
    ]


def layer_kernel(
    n_z,
    most,
    og_hbm,
    ig_hbm,
    ci_hbm,
    res_hbm,
    wo_hbm,
    docs_ref,
    taps_ref,
    mix_ref,
    ffn_ref,
    names_ref,
    share_ref,
    wg_hbm,
    wu_hbm,
    wd_hbm,
    sg_hbm,
    su_hbm,
    sd_hbm,
    out_ref,
    og,
    ig,
    ci,
    res,
    wo,
    wg,
    wu,
    wd,
    sg,
    su,
    sd,
    ext,
    dext,
    hsend,
    hrecv,
    act,
    ssq,
    srow,
    scl,
    gsend,
    grecv,
    fg,
    tri,
    blk,
    meta,
    xs,
    hid,
    shid,
    ys,
    acc,
    outgo,
    sib,
    back,
    load_sem,
    halo_sem,
    sum_sem,
    fg_sem,
    giv_send,
    giv_recv,
    z_send,
    x_send,
    c_send,
    b_recv,
    m_send,
    m_recv,
    hid_send,
    hid_recv,
    sh_send,
    sh_recv,
    sib_send,
    sib_recv,
    back_send,
    back_recv,
):
    first = [
        pltpu.make_async_copy(src, dst, load_sem.at[n])
        for n, (src, dst) in enumerate(
            ((ig_hbm, ig), (ci_hbm, ci), (og_hbm, og), (wo_hbm, wo), (res_hbm, res))
        )
    ]
    later = [
        pltpu.make_async_copy(src, dst, load_sem.at[5 + n])
        for n, (src, dst) in enumerate(
            ((wg_hbm, wg), (wu_hbm, wu), (wd_hbm, wd), (sg_hbm, sg), (su_hbm, su), (sd_hbm, sd))
        )
    ]
    for load in first:
        load.start()
    s = lax.axis_index("sp")
    t = lax.axis_index("tp")
    z = s // 2
    c = s % 2
    tokens, chan = ig.shape
    cols = out_ref.shape[1]
    width = 2 * cols
    half_rows = tokens // SPLIT
    piece = half_rows // 2
    unit = wg.shape[2]
    pad = ext.shape[0] - tokens
    lo = z > 0
    hi = z < n_z - 1
    up, down = {"sp": s + 2}, {"sp": s - 2}
    other, peer = {"sp": s + 1 - 2 * c}, {"tp": 1 - t}
    after = {"sp": s + 1}
    before = {"sp": s - 1}
    targets = (up, down, peer, other)

    def remote(src, dst, ssem, rsem, dev):
        return pltpu.make_async_remote_copy(
            src_ref=src,
            dst_ref=dst,
            send_sem=ssem,
            recv_sem=rsem,
            device_id=dev,
            device_id_type=MESH,
        )

    def chunk(zq, cq, h, half, q, ssem, dev):
        ref = blk.at[zq * 2 + cq, h, half, pl.ds(q * piece, piece)]
        return remote(ref, ref, ssem, b_recv.at[zq * 2 + cq, h, half, q], dev)

    def side(h):
        return t + h * (1 - 2 * t)

    def z_copy(way, zq, h, half, q):
        return chunk(
            zq, c, side(h), half, q, z_send.at[way, zq + h * (n_z - zq), half, q], targets[way]
        )

    def x_copy(zq, half, q):
        return chunk(zq, c, t, half, q, x_send.at[zq, half, q], peer)

    def c_copy(zq, h, half, q):
        return chunk(zq, c, h, half, q, c_send.at[zq, h, half, q], other)

    def arrived(zq, cq, h, half, q):
        chunk(zq, cq, h, half, q, c_send.at[zq, h, half, q], other).wait_recv()

    def m_copy(way, zq, cq, half):
        ref = meta.at[zq * 2 + cq, half]
        return remote(
            ref,
            ref,
            m_send.at[way, zq, half],
            m_recv.at[zq * 2 + cq, half],
            (up, down, other)[way],
        )

    def hid_copy(zq, half):
        return remote(
            hid.at[t, zq, half],
            hid.at[t, zq, half],
            hid_send.at[zq, half],
            hid_recv.at[zq, half],
            peer,
        )

    def sh_copy(half):
        return remote(
            shid.at[t, half], shid.at[t, half], sh_send.at[half], sh_recv.at[half], peer
        )

    def sib_copy(zq, half, q):
        rows = pl.ds(q * piece, piece)
        return remote(
            outgo.at[zq, half, rows],
            sib.at[zq, half, rows],
            sib_send.at[zq, half, q],
            sib_recv.at[zq, half, q],
            other,
        )

    def back_copy(zq, half, q, to, dev):
        return remote(
            acc.at[zq, half, pl.ds(q * piece, piece)],
            back.at[to, half, pl.ds(q * piece, piece)],
            back_send.at[zq, half, q],
            back_recv.at[to, half, q],
            dev,
        )

    def halo_copy():
        return remote(hsend, hrecv, halo_sem.at[0], halo_sem.at[1], after)

    def sum_copy():
        return remote(srow.at[0], srow.at[1], sum_sem.at[0], sum_sem.at[1], peer)

    def fg_copy():
        return remote(fg.at[t], fg.at[t], fg_sem.at[0], fg_sem.at[1], peer)

    def giv_copy(r):
        return remote(gsend.at[r], grecv.at[r], giv_send.at[r], giv_recv.at[r], peer)

    barrier = pltpu.get_barrier_semaphore()
    cross_up = hi & (c == 1)
    cross_down = lo & (c == 0)
    for target, there in ((up, hi), (down, lo), (after, cross_up), (before, cross_down)):

        @pl.when(there)
        def _():
            pl.semaphore_signal(barrier, inc=1, device_id=target, device_id_type=MESH)

    for target in (peer, other):
        pl.semaphore_signal(barrier, inc=1, device_id=target, device_id_type=MESH)

    has_next = s < 2 * n_z - 1
    has_prev = s > 0
    first[0].wait()
    first[1].wait()

    tail = 16

    def product(rows):
        return (ig[rows, :].astype(F32) * ci[rows, :].astype(F32)).astype(BF16).astype(F32)

    lanes = dext.shape[1]
    eye = lax.broadcasted_iota(jnp.int32, (lanes, lanes), 0) == lax.broadcasted_iota(
        jnp.int32, (lanes, lanes), 1
    )

    def upright(line):
        return jnp.sum(jnp.where(eye, line, F32(0.0)), axis=1, keepdims=True)

    docs = docs_ref[...].astype(F32)
    for k in range(tokens // lanes):
        column = upright(docs[:, k * lanes : (k + 1) * lanes])
        dext[pad + k * lanes : pad + (k + 1) * lanes, :] = jnp.broadcast_to(column, (lanes, lanes))
    end_rows = product(pl.ds(tokens - tail, tail))
    hsend[:, :chan] = end_rows[tail - 8 :]
    hsend[:, chan:] = dext[pad + tokens - 8 : pad + tokens, :]
    own = z * 2 + c
    names = names_ref[...].astype(F32)
    share = share_ref[...]
    for half in range(SPLIT):
        part = slice(half * half_rows, (half + 1) * half_rows)
        meta[own, half] = jnp.zeros(meta.shape[2:], F32)
        meta[own, half, 0:TOPK, :half_rows] = names[:, part]
        meta[own, half, TOPK : 2 * TOPK, :half_rows] = share[:, part]
    fg[t] = jnp.broadcast_to(ffn_ref[...], fg.shape[1:])
    arrivals = (
        2
        + lo.astype(jnp.int32)
        + hi.astype(jnp.int32)
        + cross_up.astype(jnp.int32)
        + cross_down.astype(jnp.int32)
    )
    pl.semaphore_wait(barrier, arrivals)

    @pl.when(has_next)
    def _():
        halo_copy().start()

    fg_copy().start()
    for half in range(SPLIT):
        m_copy(2, z, c, half).start()

    step_rows = 32

    @pl.loop(0, tokens // step_rows)
    def _(i):
        at = pl.multiple_of(i * step_rows, step_rows)
        ext[pl.ds(pad + at, step_rows), :] = product(pl.ds(at, step_rows))

    n_tri = tri.shape[0]
    row_id = lax.broadcasted_iota(jnp.int32, (n_tri, n_tri), 0)
    col_id = lax.broadcasted_iota(jnp.int32, (n_tri, n_tri), 1)
    tri[...] = (row_id < col_id).astype(F32).astype(BF16)
    for load in first[2:]:
        load.wait()
    for load in later:
        load.start()

    @pl.when(has_prev)
    def _():
        halo_copy().wait_recv()
        ext[pad - 8 : pad, :] = hrecv[:, :chan]
        dext[pad - 8 : pad, :] = hrecv[:, chan:]

    @pl.when(jnp.logical_not(has_prev))
    def _():
        ext[pad - 8 : pad, :] = jnp.zeros((8, chan), F32)
        dext[pad - 8 : pad, :] = jnp.zeros((8, dext.shape[1]), F32)

    @pl.loop(0, tokens // step_rows)
    def _(i):
        at = pl.multiple_of(i * step_rows, step_rows)
        v = ext[pl.ds(pl.multiple_of(pad - 8 + at, 8), step_rows + 8), :]
        d = dext[pl.ds(pl.multiple_of(pad - 8 + at, 8), step_rows + 8), :]
        doc = d[8:]
        mixed = None
        for k in range(CONV_K):
            by = CONV_K - 1 - k
            if by:
                same = (pltpu.roll(d, by, 0)[8:] == doc).astype(F32)
                same = jnp.concatenate([same] * (chan // lanes), axis=1)
                term = taps_ref[k : k + 1, :] * pltpu.roll(v, by, 0)[8:] * same
            else:
                term = taps_ref[k : k + 1, :] * v[8:]
            mixed = term if mixed is None else mixed + term
        rows = pl.ds(at, step_rows)
        conv_out = og[rows, :].astype(F32) * mixed
        total = jnp.sum(conv_out * conv_out, axis=1, keepdims=True)
        ssq[rows, :] = jnp.broadcast_to(total, (step_rows, lanes))
        act[rows, :] = (conv_out * mix_ref[...]).astype(BF16)

    for k in range(tokens // lanes):
        part = ssq[k * lanes : (k + 1) * lanes, :]
        line = jnp.sum(jnp.where(eye, part, F32(0.0)), axis=0, keepdims=True)
        srow[0, :, k * lanes : (k + 1) * lanes] = jnp.broadcast_to(line, (8, lanes))
    sum_copy().start()

    n_chunks = 2 * SPLIT

    def out_cols(who):
        return pl.ds(pl.multiple_of(who * cols, cols), cols)

    for r in range(n_chunks):
        gsend[r] = mm(act[r * piece : (r + 1) * piece, :], wo[:, out_cols(1 - t)]).astype(BF16)
        giv_copy(r).start()

    sum_copy().wait_recv()
    for k in range(tokens // lanes):
        line = srow[1, 0:1, k * lanes : (k + 1) * lanes]
        whole = ssq[k * lanes : (k + 1) * lanes, :] + upright(line)
        scl[k * lanes : (k + 1) * lanes, :] = lax.rsqrt(whole / (2 * chan) + 1e-06)

    fg_copy().wait_recv()
    for load in later:
        load.wait()

    def picks(zq, cq, half):
        info = meta[zq * 2 + cq, half][:, :half_rows]
        mine = (lax.broadcasted_iota(jnp.int32, (8, half_rows), 0) + s * EXP_DEV).astype(F32)
        hot0 = info[0:1] == mine
        hot1 = info[1:2] == mine
        hot = hot0 | hot1
        earlier = mm(hot.astype(F32).astype(BF16), tri[...])
        position = jnp.where(hot, earlier, F32(-1.0))
        weight = jnp.where(hot0, info[2:3], F32(0.0)) + jnp.where(hot1, info[3:4], F32(0.0))
        place = lax.broadcasted_iota(jnp.int32, (most, half_rows), 0).astype(F32)
        chosen = [(position[e : e + 1] == place).astype(F32) for e in range(EXP_DEV)]
        return chosen, weight

    def norm_scale(parts):
        total = sum(jnp.sum(part * part, axis=1, keepdims=True) for part in parts)
        return lax.rsqrt(total / width + 1e-06)

    def normal_of(parts):
        scale = norm_scale(parts)
        return [(part * scale * fg[h, 0:1, :]).astype(BF16) for h, part in enumerate(parts)]

    def sides():
        return [(0, c), (1, 1 - c)]

    def hidden(zq, half):
        for p, cq in sides():
            chosen, _ = picks(zq, cq, half)
            sel = jnp.concatenate(chosen, axis=0).astype(BF16)
            got = normal_of([mm(sel, blk[zq * 2 + cq, h, half]) for h in range(2)])
            for h in range(2):
                for e in range(EXP_DEV):
                    xs[e, p * most : (p + 1) * most, h * cols : (h + 1) * cols] = got[h][
                        e * most : (e + 1) * most
                    ]
        for e in range(EXP_DEV):
            hid[t, zq, half, e] = silu_mul(mm(xs[e], wg[e]), mm(xs[e], wu[e]))

    def shared(half):
        whole = normal_of([blk[z * 2 + c, h, half].astype(F32) for h in range(2)])
        gate = mm(whole[0], sg[:cols, :]) + mm(whole[1], sg[cols:, :])
        upper = mm(whole[0], su[:cols, :]) + mm(whole[1], su[cols:, :])
        shid[t, half] = silu_mul(gate, upper)

    def results(zq, half):
        hid_copy(zq, half).wait_recv()
        for e in range(EXP_DEV):
            ys[e] = (
                mm(hid[0, zq, half, e], wd[e, :unit, :]) + mm(hid[1, zq, half, e], wd[e, unit:, :])
            ).astype(BF16)
        for p, cq in sides():
            chosen, weight = picks(zq, cq, half)
            parts = []
            for e in range(EXP_DEV):
                scale = jnp.sum(chosen[e] * weight[e : e + 1], axis=1, keepdims=True)
                part = ys[e, p * most : (p + 1) * most, :].astype(F32)
                parts.append((part * scale).astype(BF16))
            sel = jnp.concatenate(chosen, axis=0).astype(BF16)
            into = acc if p == 0 else outgo
            into[zq, half] = lax.dot_general(
                sel,
                jnp.concatenate(parts, axis=0),
                (((0,), (0,)), ((), ())),
                preferred_element_type=F32,
            ).astype(BF16)
        for q in range(2):
            sib_copy(zq, half, q).start()

    def is_end(zq):
        return ((zq > z) & jnp.logical_not(lo)) | ((zq < z) & jnp.logical_not(hi))

    def strip(q):
        return pl.ds(pl.multiple_of(q * piece, piece), piece)

    def on_stream(zq, h, half, q):
        r = half * 2 + q
        rows = pl.ds(pl.multiple_of(r * piece, piece), piece)
        kept = mm(act[rows, :], wo[:, out_cols(t)])
        giv_copy(r).wait_recv()
        proj = (kept + grecv[r].astype(F32)) * scl[rows, 0:1]
        blk[z * 2 + c, t, half, strip(q), :] = (res[rows, :].astype(F32) + proj).astype(BF16)
        c_copy(z, t, half, q).start()

    def on_land(zq, h, half, q):
        @pl.when((h == 0) & (q == 0))
        def _():
            m_copy(2, zq, c, half).wait_recv()
            m_copy(2, zq, c, half).start()

        arrived(zq, c, side(h), half, q)
        c_copy(zq, side(h), half, q).start()

    def on_z(way):
        def send(zq, h, half, q):
            @pl.when((h == 0) & (q == 0))
            def _():
                m_copy(way, zq, c, half).start()

            z_copy(way, zq, h, half, q).start()

        return send

    def on_across(zq, h, half, q):
        x_copy(zq, half, q).start()

    def on_hidden(zq, h, half, q):
        m_copy(2, zq, 1 - c, half).wait_recv()
        for hh in range(2):
            for qq in range(2):
                arrived(zq, 1 - c, hh, half, qq)
        hidden(zq, half)
        hid_copy(zq, half).start()

        @pl.when(zq == z)
        def _():
            shared(half)
            sh_copy(half).start()

    def on_result(zq, h, half, q):
        results(zq, half)

    def on_combine(zq, h, half, q):
        rows = strip(q)
        sib_copy(zq, half, q).wait_recv()
        end = is_end(zq)

        @pl.when(end)
        def _():
            acc[zq, half, rows, :] = (
                acc[zq, half, rows, :].astype(F32) + sib[zq, half, rows, :].astype(F32)
            ).astype(BF16)

        @pl.when(jnp.logical_not(end))
        def _():
            back_copy(zq, half, q, zq, up).wait_recv()
            acc[zq, half, rows, :] = (
                acc[zq, half, rows, :].astype(F32)
                + sib[zq, half, rows, :].astype(F32)
                + back[zq, half, rows, :].astype(F32)
            ).astype(BF16)

        @pl.when(zq > z)
        def _():
            back_copy(zq, half, q, zq, up).start()

        @pl.when(zq < z - 1)
        def _():
            back_copy(zq, half, q, zq, down).start()

        @pl.when(zq == z - 1)
        def _():
            back_copy(zq, half, q, n_z, down).start()

    actions = (
        on_stream,
        on_land,
        on_z(0),
        on_z(1),
        on_across,
        on_hidden,
        on_result,
        on_combine,
    )
    order, _ = plan(n_z)
    groups = max(-(-len(order[zz]) // 3) for zz in range(n_z))
    tables = [
        encode(order[zz] + [("combine", zz, 0, 0, 0)] * (3 * groups - len(order[zz])))
        for zz in range(n_z)
    ]
    values = [
        sum((z == zz).astype(jnp.int32) * tables[zz][g] for zz in range(n_z)) for g in range(groups)
    ]

    @pl.loop(0, groups)
    def _(g):
        value = sum((g == k).astype(jnp.int32) * values[k] for k in range(groups))

        def turn(k, rest):
            code = rest % 256
            q, half, h = code % 2, code // 2 % 2, code // 4 % 2
            zq, kind = code // 8 % 4, code // 32
            for n, action in enumerate(actions):
                live = kind == n
                if action is on_combine:
                    live = live & (zq != z)

                @pl.when(live)
                def _():
                    action(zq, h, half, q)

            return rest // 256

        lax.fori_loop(0, 3, turn, value)

    for half in range(SPLIT):
        sh_copy(half).wait_recv()
        for q in range(2):
            sib_copy(z, half, q).wait_recv()

            @pl.when(lo)
            def _():
                back_copy(z, half, q, z, up).wait_recv()

            @pl.when(hi)
            def _():
                back_copy(z, half, q, n_z, up).wait_recv()

            rows = slice(q * piece, (q + 1) * piece)
            fin = (
                blk[z * 2 + c, t, half, rows, :].astype(F32)
                + mm(shid[0, half, rows, :], sd[:unit, :])
                + mm(shid[1, half, rows, :], sd[unit:, :])
                + acc[z, half, rows, :].astype(F32)
                + sib[z, half, rows, :].astype(F32)
            )
            low = jnp.where(lo, back[z, half, rows, :].astype(F32), F32(0.0))
            high = jnp.where(hi, back[n_z, half, rows, :].astype(F32), F32(0.0))
            at = half * half_rows + q * piece
            out_ref[at : at + piece, :] = (fin + low + high).astype(BF16)

    @pl.when(has_next)
    def _():
        halo_copy().wait_send()

    fg_copy().wait_send()
    sum_copy().wait_send()
    for r in range(n_chunks):
        giv_copy(r).wait_send()
    for half in range(SPLIT):
        sh_copy(half).wait_send()

    def listed(target, half, q):
        inner = (target > 0) & (target < n_z - 1)
        outer_in, inner_in = half * 2 + q in FULL[0], half * 2 + q in FULL[1]
        return (inner & inner_in) | (jnp.logical_not(inner) & outer_in)

    for half in range(SPLIT):
        for q in range(2):
            for way, there, target in ((0, hi, z + 1), (1, lo, z - 1)):

                @pl.when(there & listed(target, half, q))
                def _():
                    z_copy(way, z, 1, half, q).wait_send()

    @pl.loop(0, n_z)
    def _(zq):
        for way, there in ((0, hi & (zq <= z)), (1, lo & (zq >= z))):

            @pl.when(there)
            def _():
                for half in range(SPLIT):
                    m_copy(way, zq, c, half).wait_send()
                    for q in range(2):
                        z_copy(way, zq, 0, half, q).wait_send()

        near = (zq == z + 1) | (zq == z - 1)
        for half in range(SPLIT):
            m_copy(2, zq, c, half).wait_send()
            for q in range(2):

                @pl.when(jnp.logical_not(near & listed(z, half, q)))
                def _():
                    x_copy(zq, half, q).wait_send()

                for h in range(2):
                    c_copy(zq, h, half, q).wait_send()
                sib_copy(zq, half, q).wait_send()

                @pl.when(zq != z)
                def _():
                    back_copy(zq, half, q, zq, up).wait_send()

            hid_copy(zq, half).wait_send()


def fast(
    out_gate,
    in_gate,
    conv_input,
    doc_ids,
    residual,
    conv_taps,
    mix_gain,
    out_weight,
    ffn_gain,
    routing,
    route_weight,
    expert_gate,
    expert_up,
    expert_down,
    shared_gate,
    shared_up,
    shared_down,
):
    tokens, cols = residual.shape
    chan, width = out_weight.shape
    n_tp, n_sp = lax.axis_size("tp"), lax.axis_size("sp")
    n_z = n_sp // 2
    rows = tokens // n_tp
    experts = n_sp * EXP_DEV
    most = max(1, 2 * rows * TOPK // experts)
    lanes = 128
    piece = rows // 2
    blocks = n_sp
    unit = expert_gate.shape[2]
    vm = pl.BlockSpec(memory_space=pltpu.VMEM)
    hbm = pl.BlockSpec(memory_space=pl.ANY)
    dma = pltpu.SemaphoreType.DMA
    return pl.pallas_call(
        functools.partial(layer_kernel, n_z, most),
        out_shape=jax.ShapeDtypeStruct((tokens, cols), BF16),
        in_specs=[hbm] * 5 + [vm] * 6 + [hbm] * 6,
        out_specs=vm,
        scratch_shapes=[
            pltpu.VMEM((tokens, chan), BF16),
            pltpu.VMEM((tokens, chan), BF16),
            pltpu.VMEM((tokens, chan), BF16),
            pltpu.VMEM((tokens, cols), BF16),
            pltpu.VMEM((chan, width), BF16),
            pltpu.VMEM(expert_gate.shape, BF16),
            pltpu.VMEM(expert_up.shape, BF16),
            pltpu.VMEM(expert_down.shape, BF16),
            pltpu.VMEM(shared_gate.shape, BF16),
            pltpu.VMEM(shared_up.shape, BF16),
            pltpu.VMEM(shared_down.shape, BF16),
            pltpu.VMEM((tokens + 16, chan), F32),
            pltpu.VMEM((tokens + 16, lanes), F32),
            pltpu.VMEM((8, chan + lanes), F32),
            pltpu.VMEM((8, chan + lanes), F32),
            pltpu.VMEM((tokens, chan), BF16),
            pltpu.VMEM((tokens, lanes), F32),
            pltpu.VMEM((2, 8, tokens), F32),
            pltpu.VMEM((tokens, lanes), F32),
            pltpu.VMEM((2 * SPLIT, piece, cols), BF16),
            pltpu.VMEM((2 * SPLIT, piece, cols), BF16),
            pltpu.VMEM((2, 8, cols), F32),
            pltpu.VMEM((rows, rows), BF16),
            pltpu.VMEM((blocks, 2, SPLIT, rows, cols), BF16),
            pltpu.VMEM((blocks, SPLIT, 8, rows + -rows % lanes), F32),
            pltpu.VMEM((EXP_DEV, 2 * most, width), BF16),
            pltpu.VMEM((2, n_z, SPLIT, EXP_DEV, 2 * most, unit), BF16),
            pltpu.VMEM((2, SPLIT, rows, unit), BF16),
            pltpu.VMEM((EXP_DEV, 2 * most, cols), BF16),
            pltpu.VMEM((n_z, SPLIT, rows, cols), BF16),
            pltpu.VMEM((n_z, SPLIT, rows, cols), BF16),
            pltpu.VMEM((n_z, SPLIT, rows, cols), BF16),
            pltpu.VMEM((n_z + 1, SPLIT, rows, cols), BF16),
            dma((11,)),
            dma((2,)),
            dma((2,)),
            dma((2,)),
            dma((2 * SPLIT,)),
            dma((2 * SPLIT,)),
            dma((2, n_z + 1, SPLIT, 2)),
            dma((n_z, SPLIT, 2)),
            dma((n_z, 2, SPLIT, 2)),
            dma((blocks, 2, SPLIT, 2)),
            dma((3, n_z, SPLIT)),
            dma((blocks, SPLIT)),
            dma((n_z, SPLIT)),
            dma((n_z, SPLIT)),
            dma((SPLIT,)),
            dma((SPLIT,)),
            dma((n_z, SPLIT, 2)),
            dma((n_z, SPLIT, 2)),
            dma((n_z, SPLIT, 2)),
            dma((n_z + 1, SPLIT, 2)),
        ],
        compiler_params=pltpu.CompilerParams(
            collective_id=0, has_side_effects=True, vmem_limit_bytes=64 * 1024 * 1024 - 65536
        ),
    )(
        out_gate,
        in_gate,
        conv_input,
        residual,
        out_weight,
        doc_ids[None, :],
        conv_taps,
        mix_gain[None, :],
        ffn_gain[None, :],
        routing.T,
        route_weight.T,
        expert_gate,
        expert_up,
        expert_down,
        shared_gate,
        shared_up,
        shared_down,
    )


def fits(mesh):
    return mesh.shape["tp"] == 2 and mesh.shape["sp"] in (4, 6, 8)


def solution(mesh):
    return jax.shard_map(
        fast if fits(mesh) else body,
        mesh=mesh,
        in_specs=(
            P(("grp", "sp"), "tp"),
            P(("grp", "sp"), "tp"),
            P(("grp", "sp"), "tp"),
            P(("grp", "sp")),
            P(("grp", "sp"), "tp"),
            P(None, "tp"),
            P("tp"),
            P("tp", None),
            P("tp"),
            P(("grp", "sp"), None),
            P(("grp", "sp"), None),
            P("sp", None, "tp"),
            P("sp", None, "tp"),
            P("sp", None, "tp"),
            P(None, "tp"),
            P(None, "tp"),
            P(None, "tp"),
        ),
        out_specs=P(("grp", "sp"), "tp"),
        check_vma=False,
    )
```

```python
import functools

import jax
import jax.numpy as jnp
from jax import lax
from jax.experimental import pallas as pl
from jax.experimental.pallas import tpu as pltpu
from jax.sharding import PartitionSpec as P

D_CONV = 1024
CONV_K = 3
TOPK = 2
EXP_DEV = 2


def from_behind(value, axis, steps):
    count = lax.axis_size(axis)
    first, last = (max(0, -steps), min(count, count - steps))
    return lax.ppermute(value, axis, [(source, source + steps) for source in range(first, last)])


def body(
    out_gate,
    in_gate,
    conv_input,
    doc_ids,
    residual,
    conv_taps,
    mix_gain,
    out_weight,
    ffn_gain,
    routing,
    route_weight,
    expert_gate,
    expert_up,
    expert_down,
    shared_gate,
    shared_up,
    shared_down,
):
    tokens = residual.shape[0]
    width = out_weight.shape[1]
    n_tp = lax.axis_size("tp")
    n_sp = lax.axis_size("sp")
    rows = tokens // n_tp
    experts = n_sp * EXP_DEV
    most = max(1, 2 * rows * TOPK // experts)
    slots = n_tp * most
    total = experts * slots
    cols = expert_down.shape[2]
    product = (in_gate.astype(jnp.float32) * conv_input.astype(jnp.float32)).astype(jnp.bfloat16)
    tail = (product[tokens - CONV_K + 1 :], doc_ids[tokens - CONV_K + 1 :].astype(jnp.bfloat16))
    prev_rows, prev_docs = from_behind((tail[0], tail[1]), "sp", 1)
    extended = jnp.concatenate([prev_rows, product], axis=0).astype(jnp.float32)
    ext_docs = jnp.concatenate([prev_docs.astype(jnp.int32), doc_ids])
    mixed = jnp.zeros(product.shape, jnp.float32)
    for k in range(CONV_K):
        keep = (ext_docs[k : k + tokens] == doc_ids)[:, None]
        mixed = mixed + jnp.where(keep, conv_taps[k] * extended[k : k + tokens], jnp.float32(0.0))
    conv_out = out_gate.astype(jnp.float32) * mixed
    squares = lax.psum(jnp.sum(conv_out * conv_out, axis=1), "tp")
    normed = (conv_out * lax.rsqrt(squares / D_CONV + 1e-06)[:, None] * mix_gain).astype(
        jnp.bfloat16
    )
    partial_value = jnp.dot(normed, out_weight, preferred_element_type=jnp.float32)
    proj = lax.psum_scatter(
        partial_value.astype(jnp.bfloat16), "tp", scatter_dimension=1, tiled=True
    ).astype(jnp.float32)
    stream = (residual.astype(jnp.float32) + proj).astype(jnp.bfloat16)
    stream32 = stream.astype(jnp.float32)
    stream_sq = lax.psum(jnp.sum(stream32 * stream32, axis=1), "tp")
    normal_cols = (stream32 * lax.rsqrt(stream_sq / width + 1e-06)[:, None] * ffn_gain).astype(
        jnp.bfloat16
    )
    flat_expert = routing.reshape(-1)
    onehot = (flat_expert[:, None] == jnp.arange(experts, dtype=jnp.int32)[None, :]).astype(
        jnp.int32
    )
    blocked = onehot.reshape(n_tp, rows * TOPK, experts)
    earlier = jnp.cumsum(blocked, axis=1) - blocked
    position = jnp.sum(earlier * blocked, axis=2).reshape(-1)
    entry = jnp.arange(tokens * TOPK, dtype=jnp.int32)
    slot = flat_expert * slots + entry // (rows * TOPK) * most + position
    table = jnp.full((total,), tokens, jnp.int32).at[slot].set(entry // TOPK)
    block_rows = lax.all_to_all(normal_cols, "tp", split_axis=0, concat_axis=1, tiled=True)
    mine = lax.dynamic_index_in_dim(
        table.reshape(n_sp, EXP_DEV, n_tp, most), lax.axis_index("tp"), 2, False
    )
    local = jnp.where(mine >= tokens, rows, mine - lax.axis_index("tp") * rows)
    padded_block = jnp.concatenate([block_rows, jnp.zeros((1, width), jnp.bfloat16)], axis=0)
    got = lax.all_to_all(padded_block[local], "sp", split_axis=0, concat_axis=0, tiled=True)
    arrived, whole = (
        lax.all_gather(got, "tp", axis=2, tiled=True),
        lax.all_gather(block_rows.reshape(1, 1, rows, width), "tp", axis=2, tiled=True),
    )
    normal = whole.reshape(tokens, width)
    gate = jnp.einsum("nesd,edh->nesh", arrived, expert_gate, preferred_element_type=jnp.float32)
    upper = jnp.einsum("nesd,edh->nesh", arrived, expert_up, preferred_element_type=jnp.float32)
    hidden = (jax.nn.silu(gate) * upper).astype(jnp.bfloat16)
    hidden_flat = hidden.reshape(n_sp * EXP_DEV * slots, hidden.shape[3])
    shared_hid = (
        jax.nn.silu(jnp.dot(normal, shared_gate, preferred_element_type=jnp.float32))
        * jnp.dot(normal, shared_up, preferred_element_type=jnp.float32)
    ).astype(jnp.bfloat16)
    expert_piece = lax.all_gather(hidden_flat, "tp", axis=1, tiled=True)
    shared_piece = lax.all_gather(shared_hid, "tp", axis=1, tiled=True)
    count = expert_piece.shape[1]
    expert_part = jnp.einsum(
        "nesh,ehd->nesd",
        expert_piece.reshape(n_sp, EXP_DEV, slots, count),
        expert_down,
        preferred_element_type=jnp.float32,
    )
    shared_part = jnp.dot(shared_piece, shared_down, preferred_element_type=jnp.float32)
    returned = lax.all_to_all(
        expert_part.astype(jnp.bfloat16), "sp", split_axis=0, concat_axis=0, tiled=True
    )
    picked = (
        returned.reshape(total, cols)[slot].astype(jnp.float32) * route_weight.reshape(-1)[:, None]
    )
    routed = jnp.sum(picked.reshape(tokens, TOPK, cols), axis=1)
    return (stream32 + shared_part + routed).astype(jnp.bfloat16)


MESH = pl.DeviceIdType.MESH
F32 = jnp.float32
BF16 = jnp.bfloat16


def silu_mul(gate, upper):
    return (gate / (1.0 + jnp.exp(-gate)) * upper).astype(BF16)


def mm(a, b):
    return jnp.dot(a, b, preferred_element_type=F32)


SPLIT = 2


GIVEN = (1, 0, 2, 3)
HOP, START, WIRE, NEAR = 2.8, 4.5, 4.18, (1.4, 2.5)
COST, EXTRA = (0.45, 0.15, 0.15, 0.15, 0.15, 1.65, 1.3, 0.22), (0.9, 0.3)
FULL = ((0, 1), (0, 1))
ROWX = (4.4, 6.8, -4.4, 5.1, -5, 1.7, -0.6, -5.3)
ROWZ = (3.5, 5.9, -6, 3.6, -2.6, 0, -1.7, -4.6)
ROWF = (-5.4, -6.7)
COMB = (-3.8, -2, 3, -5.8, -4.1, 0.2, -0.3, 1)
WORK = (4.9, 1.9, 4.4, 2.3, 5, -3.8, 6.2, -1.2)
RANK, DEPTH = (0, 0, 1, 4, 0), (1, 1.5)
BASE = 257


KINDS = ("stream", "land", "up", "down", "across", "hidden", "result", "combine")


def full_rows(n_z, source, target, half, q):
    return abs(source - target) == 1 and half * 2 + q in FULL[0 < target < n_z - 1]


def plan(n_z):
    chunks = [(half, q) for half in range(SPLIT) for q in range(2)]
    zones = range(n_z)
    never = 1e9
    have, told, heard, summed, went, final, arrive = {}, {}, {}, {}, {}, {}, {}
    todo = {z: [] for z in zones}
    for z in zones:
        for k, (half, q) in enumerate(chunks):
            todo[z].append(("stream", z, 0, half, q))
            went[z, half, q] = START + WIRE * (GIVEN.index(k) + 1) + HOP
        for zq in zones:
            for half, q in chunks:
                if zq != z:
                    todo[z].append(("land", zq, 0, half, q))
                todo[z].append(("land", zq, 1, half, q))
                if zq <= z < n_z - 1:
                    todo[z].append(("up", zq, 0, half, q))
                if zq >= z > 0:
                    todo[z].append(("down", zq, 0, half, q))
                if not full_rows(n_z, zq, z, half, q):
                    todo[z].append(("across", zq, 0, half, q))
                todo[z].append(("combine", zq, 0, half, q))
            for half in range(SPLIT):
                todo[z].append(("hidden", zq, 0, half, 0))
                todo[z].append(("result", zq, 0, half, 0))
        for half, q in chunks:
            if z < n_z - 1 and full_rows(n_z, z, z + 1, half, q):
                todo[z].append(("up", z, 1, half, q))
            if z > 0 and full_rows(n_z, z, z - 1, half, q):
                todo[z].append(("down", z, 1, half, q))
    link = {(z, way): 0.0 for z in zones for way in ("up", "down", "across")}
    for z in zones:
        link[z, "across"] = START + WIRE * len(chunks)
    core = {z: START for z in zones}

    def put(z, way, now, size):
        link[z, way] = max(now, link[z, way]) + WIRE * size
        return link[z, way] + HOP

    def ready(z, event):
        kind, zq, h, half, q = event
        if kind == "stream":
            return went[z, half, q]
        if kind == "land":
            return arrive.get((z, zq, h, half, q), never)
        if kind in ("up", "down", "across"):
            depth = DEPTH[kind == "across"]
            return max(have.get((z, zq, h, half, q), never), link[z, kind] - depth)
        if kind == "hidden":
            parts = [have.get((z, zq, g, half, p), never) for g in range(2) for p in range(2)]
            return max(parts) + NEAR[0]
        if kind == "result":
            return heard.get((z, zq, half), never)
        at = told.get((z, zq, half), never)
        if zq >= z and z > 0:
            at = max(at, summed.get((z - 1, zq, half, q), never))
        if zq <= z and z < n_z - 1:
            at = max(at, summed.get((z + 1, zq, half, q), never))
        if zq == z and q > 0:
            at = max(at, final.get((z, half, q - 1), never))
        return at

    def rank(z, event):
        kind, zq, h, half, q = event
        away = abs(zq - z)
        if kind in ("stream", "land"):
            return (RANK[0], 0.0, q)
        if kind == "combine":
            return (RANK[1], COMB[away * 2 + half], q)
        if kind == "result":
            return (RANK[2], WORK[away * 2 + half], q)
        if kind == "hidden":
            return (RANK[3], WORK[away * 2 + half], q)
        if kind == "across":
            return (RANK[4], ROWX[away * 2 + half], q)
        return (RANK[4], ROWZ[away * 2 + half] if h == 0 else ROWF[half], q)

    order = {z: [] for z in zones}
    while any(todo.values()):
        best = None
        for z in zones:
            if not todo[z]:
                continue
            starts = [(max(core[z], ready(z, event)), event) for event in todo[z]]
            at = min(start for start, _ in starts)
            if best is None or at < best[0]:
                best = (at, z, starts)
        at, z, starts = best
        assert at < never
        event = min((e for start, e in starts if start <= at), key=lambda e: rank(z, e))
        kind, zq, h, half, q = event
        todo[z].remove(event)
        order[z].append(event)
        end = at + COST[KINDS.index(kind)]
        if zq == z:
            end = end + (EXTRA[0] if kind == "hidden" else EXTRA[1] if kind == "combine" else 0.0)
        core[z] = end
        if kind in ("stream", "land"):
            have[z, zq, h, half, q] = end
        elif kind in ("up", "down"):
            arrive[z + (1 if kind == "up" else -1), zq, h, half, q] = put(z, kind, end, 1.0)
        elif kind == "across":
            arrive[z, zq, 1, half, q] = put(z, kind, end, 1.0)
        elif kind == "hidden":
            heard[z, zq, half] = put(z, "across", end, 1.0 if zq == z else 0.5)
        elif kind == "result":
            told[z, zq, half] = end + NEAR[1]
        elif zq == z:
            final[z, half, q] = end
        else:
            summed[z, zq, half, q] = put(z, "up" if zq > z else "down", end, 1.0)
    return order, max(final.values())


def encode(events, slots):
    codes = [
        (((KINDS.index(kind) * 4 + zq) * 2 + h) * 2 + half) * 2 + q + 1
        for kind, zq, h, half, q in events
    ]
    codes += [0] * (slots - len(codes))
    return [sum(codes[at + k] * BASE**k for k in range(3)) for at in range(0, slots, 3)]


def layer_kernel(
    n_z,
    most,
    og_hbm,
    ig_hbm,
    ci_hbm,
    res_hbm,
    wo_hbm,
    docs_ref,
    taps_ref,
    mix_ref,
    ffn_ref,
    names_ref,
    share_ref,
    wg_hbm,
    wu_hbm,
    wd_hbm,
    sg_hbm,
    su_hbm,
    sd_hbm,
    out_hbm,
    og,
    ig,
    ci,
    res,
    wo,
    wg,
    wu,
    wd,
    sg,
    su,
    sd,
    ext,
    dext,
    hsend,
    hrecv,
    act,
    ssq,
    srow,
    gsend,
    grecv,
    fg,
    tri,
    blk,
    meta,
    xs,
    hid,
    shid,
    ys,
    acc,
    outgo,
    sib,
    back,
    done,
    load_sem,
    halo_sem,
    sum_sem,
    fg_sem,
    giv_send,
    giv_recv,
    z_send,
    x_send,
    c_send,
    b_recv,
    m_send,
    m_recv,
    hid_send,
    hid_recv,
    sh_send,
    sh_recv,
    sib_send,
    sib_recv,
    back_send,
    back_recv,
    out_sem,
):
    first = [
        pltpu.make_async_copy(src, dst, load_sem.at[n])
        for n, (src, dst) in enumerate(
            ((ig_hbm, ig), (ci_hbm, ci), (og_hbm, og), (wo_hbm, wo), (res_hbm, res))
        )
    ]
    later = [
        pltpu.make_async_copy(src, dst, load_sem.at[5 + n])
        for n, (src, dst) in enumerate(
            ((wg_hbm, wg), (wu_hbm, wu), (wd_hbm, wd), (sg_hbm, sg), (su_hbm, su), (sd_hbm, sd))
        )
    ]
    for load in first:
        load.start()
    s = lax.axis_index("sp")
    t = lax.axis_index("tp")
    z = s // 2
    c = s % 2
    tokens, chan = ig.shape
    cols = res.shape[1]
    width = 2 * cols
    half_rows = tokens // SPLIT
    piece = half_rows // 2
    unit = wg.shape[2]
    pad = ext.shape[0] - tokens
    lo = z > 0
    hi = z < n_z - 1
    up, down = {"sp": s + 2}, {"sp": s - 2}
    other, peer = {"sp": s + 1 - 2 * c}, {"tp": 1 - t}
    after = {"sp": s + 1}
    before = {"sp": s - 1}
    targets = (up, down, peer, other)

    def remote(src, dst, ssem, rsem, dev):
        return pltpu.make_async_remote_copy(
            src_ref=src,
            dst_ref=dst,
            send_sem=ssem,
            recv_sem=rsem,
            device_id=dev,
            device_id_type=MESH,
        )

    def chunk(zq, cq, h, half, q, ssem, dev):
        ref = blk.at[zq * 2 + cq, h, half, pl.ds(q * piece, piece)]
        return remote(ref, ref, ssem, b_recv.at[zq * 2 + cq, h, half, q], dev)

    def side(h):
        return t + h * (1 - 2 * t)

    def z_copy(way, zq, h, half, q):
        return chunk(
            zq, c, side(h), half, q, z_send.at[way, zq + h * (n_z - zq), half, q], targets[way]
        )

    def x_copy(zq, half, q):
        return chunk(zq, c, t, half, q, x_send.at[zq, half, q], peer)

    def c_copy(zq, h, half, q):
        return chunk(zq, c, h, half, q, c_send.at[zq, h, half, q], other)

    def arrived(zq, cq, h, half, q):
        chunk(zq, cq, h, half, q, c_send.at[zq, h, half, q], other).wait_recv()

    def m_copy(way, zq, cq, half):
        ref = meta.at[zq * 2 + cq, half]
        return remote(
            ref,
            ref,
            m_send.at[way, zq, half],
            m_recv.at[zq * 2 + cq, half],
            (up, down, other)[way],
        )

    def hid_copy(zq, half):
        return remote(
            hid.at[t, zq, half],
            hid.at[t, zq, half],
            hid_send.at[zq, half],
            hid_recv.at[zq, half],
            peer,
        )

    def sh_copy(half):
        return remote(
            shid.at[t, half], shid.at[t, half], sh_send.at[half], sh_recv.at[half], peer
        )

    def sib_copy(zq, half, q):
        rows = pl.ds(q * piece, piece)
        return remote(
            outgo.at[zq, half, rows],
            sib.at[zq, half, rows],
            sib_send.at[zq, half, q],
            sib_recv.at[zq, half, q],
            other,
        )

    def back_copy(zq, half, q, to, dev):
        return remote(
            acc.at[zq, half, pl.ds(q * piece, piece)],
            back.at[to, half, pl.ds(q * piece, piece)],
            back_send.at[zq, half, q],
            back_recv.at[to, half, q],
            dev,
        )

    def halo_copy():
        return remote(hsend, hrecv, halo_sem.at[0], halo_sem.at[1], after)

    def sum_copy(r):
        return remote(srow.at[0, r], srow.at[1, r], sum_sem.at[0, r], sum_sem.at[1, r], peer)

    def fg_copy():
        return remote(fg.at[t], fg.at[t], fg_sem.at[0], fg_sem.at[1], peer)

    def giv_copy(r):
        return remote(gsend.at[r], grecv.at[r], giv_send.at[r], giv_recv.at[r], peer)

    barrier = pltpu.get_barrier_semaphore()
    cross_up = hi & (c == 1)
    cross_down = lo & (c == 0)
    for target, there in ((up, hi), (down, lo), (after, cross_up), (before, cross_down)):

        @pl.when(there)
        def _():
            pl.semaphore_signal(barrier, inc=1, device_id=target, device_id_type=MESH)

    for target in (peer, other):
        pl.semaphore_signal(barrier, inc=1, device_id=target, device_id_type=MESH)

    has_next = s < 2 * n_z - 1
    has_prev = s > 0
    first[0].wait()
    first[1].wait()

    tail = 16

    def product(rows):
        return (ig[rows, :].astype(F32) * ci[rows, :].astype(F32)).astype(BF16).astype(F32)

    lanes = dext.shape[1]
    eye = lax.broadcasted_iota(jnp.int32, (lanes, lanes), 0) == lax.broadcasted_iota(
        jnp.int32, (lanes, lanes), 1
    )

    def upright(line):
        return jnp.sum(jnp.where(eye, line, F32(0.0)), axis=1, keepdims=True)

    docs = docs_ref[...].astype(F32)
    for k in range(tokens // lanes):
        column = upright(docs[:, k * lanes : (k + 1) * lanes])
        dext[pad + k * lanes : pad + (k + 1) * lanes, :] = jnp.broadcast_to(column, (lanes, lanes))
    end_rows = product(pl.ds(tokens - tail, tail))
    hsend[:, :chan] = end_rows[tail - 8 :]
    hsend[:, chan:] = dext[pad + tokens - 8 : pad + tokens, :]
    own = z * 2 + c
    names = names_ref[...].astype(F32)
    share = share_ref[...]
    for half in range(SPLIT):
        part = slice(half * half_rows, (half + 1) * half_rows)
        meta[own, half] = jnp.zeros(meta.shape[2:], F32)
        meta[own, half, 0:TOPK, :half_rows] = names[:, part]
        meta[own, half, TOPK : 2 * TOPK, :half_rows] = share[:, part]
    fg[t] = ffn_ref[...]
    step_rows = 32

    @pl.loop(0, tokens // step_rows)
    def _(i):
        at = pl.multiple_of(i * step_rows, step_rows)
        ext[pl.ds(pad + at, step_rows), :] = product(pl.ds(at, step_rows))

    n_tri = tri.shape[0]
    row_id = lax.broadcasted_iota(jnp.int32, (n_tri, n_tri), 0)
    col_id = lax.broadcasted_iota(jnp.int32, (n_tri, n_tri), 1)
    tri[...] = (row_id < col_id).astype(F32).astype(BF16)

    def convolve(r):
        @pl.loop(0, piece // step_rows)
        def _(i):
            at = pl.multiple_of(r * piece + i * step_rows, step_rows)
            v = ext[pl.ds(pl.multiple_of(pad - 8 + at, 8), step_rows + 8), :]
            d = dext[pl.ds(pl.multiple_of(pad - 8 + at, 8), step_rows + 8), :]
            doc = d[8:]
            mixed = None
            for k in range(CONV_K):
                by = CONV_K - 1 - k
                if by:
                    same = (pltpu.roll(d, by, 0)[8:] == doc).astype(F32)
                    same = jnp.concatenate([same] * (chan // lanes), axis=1)
                    term = taps_ref[k : k + 1, :] * pltpu.roll(v, by, 0)[8:] * same
                else:
                    term = taps_ref[k : k + 1, :] * v[8:]
                mixed = term if mixed is None else mixed + term
            rows = pl.ds(at, step_rows)
            conv_out = og[rows, :].astype(F32) * mixed
            total = jnp.sum(conv_out * conv_out, axis=1, keepdims=True)
            ssq[rows, :] = jnp.broadcast_to(total, (step_rows, lanes))
            act[rows, :] = (conv_out * mix_ref[...]).astype(BF16)

    n_chunks = 2 * SPLIT
    eye_piece = lax.broadcasted_iota(jnp.int32, (piece, lanes), 0) == lax.broadcasted_iota(
        jnp.int32, (piece, lanes), 1
    )

    def out_cols(who):
        return pl.ds(pl.multiple_of(who * cols, cols), cols)

    def sums(r):
        part = ssq[r * piece : (r + 1) * piece, :]
        line = jnp.sum(jnp.where(eye_piece, part, F32(0.0)), axis=0, keepdims=True)
        srow[0, r] = jnp.broadcast_to(line, srow.shape[2:])

    def give(r):
        gsend[r] = mm(act[r * piece : (r + 1) * piece, :], wo[:, out_cols(1 - t)]).astype(BF16)

    def send_given(r):
        sum_copy(r).start()
        giv_copy(r).start()

    first[2].wait()
    for r in GIVEN:
        if r:
            convolve(r)
            sums(r)
    first[3].wait()
    give(GIVEN[0])
    first[4].wait()
    arrivals = (
        2
        + lo.astype(jnp.int32)
        + hi.astype(jnp.int32)
        + cross_up.astype(jnp.int32)
        + cross_down.astype(jnp.int32)
    )
    pl.semaphore_wait(barrier, arrivals)

    @pl.when(has_next)
    def _():
        halo_copy().start()

    fg_copy().start()
    send_given(GIVEN[0])
    for half in range(SPLIT):
        m_copy(2, z, c, half).start()

    @pl.when(has_prev)
    def _():
        halo_copy().wait_recv()
        ext[pad - 8 : pad, :] = hrecv[:, :chan]
        dext[pad - 8 : pad, :] = hrecv[:, chan:]

    @pl.when(jnp.logical_not(has_prev))
    def _():
        ext[pad - 8 : pad, :] = jnp.zeros((8, chan), F32)
        dext[pad - 8 : pad, :] = jnp.zeros((8, lanes), F32)

    convolve(0)
    sums(0)
    for r in GIVEN[1:]:
        give(r)
        send_given(r)
    fg_copy().wait_recv()

    def picks(zq, cq, half):
        info = meta[zq * 2 + cq, half][:, :half_rows]
        mine = (lax.broadcasted_iota(jnp.int32, (8, half_rows), 0) + s * EXP_DEV).astype(F32)
        hot0 = info[0:1] == mine
        hot1 = info[1:2] == mine
        hot = hot0 | hot1
        earlier = mm(hot.astype(F32).astype(BF16), tri[...])
        position = jnp.where(hot, earlier, F32(-1.0))
        weight = jnp.where(hot0, info[2:3], F32(0.0)) + jnp.where(hot1, info[3:4], F32(0.0))
        place = lax.broadcasted_iota(jnp.int32, (most, half_rows), 0).astype(F32)
        chosen = [(position[e : e + 1] == place).astype(F32) for e in range(EXP_DEV)]
        return chosen, weight

    def norm_scale(parts):
        total = sum(jnp.sum(part * part, axis=1, keepdims=True) for part in parts)
        return lax.rsqrt(total / width + 1e-06)

    def normal_of(parts):
        scale = norm_scale(parts)
        return [(part * scale * fg[h, 0:1, :]).astype(BF16) for h, part in enumerate(parts)]

    def sides():
        return [(0, c), (1, 1 - c)]

    def hidden(zq, half):
        for p, cq in sides():
            chosen, _ = picks(zq, cq, half)
            sel = jnp.concatenate(chosen, axis=0).astype(BF16)
            got = normal_of([mm(sel, blk[zq * 2 + cq, h, half]) for h in range(2)])
            for h in range(2):
                for e in range(EXP_DEV):
                    xs[e, p * most : (p + 1) * most, h * cols : (h + 1) * cols] = got[h][
                        e * most : (e + 1) * most
                    ]
        for e in range(EXP_DEV):
            hid[t, zq, half, e] = silu_mul(mm(xs[e], wg[e]), mm(xs[e], wu[e]))

    def shared(half):
        whole = normal_of([blk[z * 2 + c, h, half].astype(F32) for h in range(2)])
        gate = mm(whole[0], sg[:cols, :]) + mm(whole[1], sg[cols:, :])
        upper = mm(whole[0], su[:cols, :]) + mm(whole[1], su[cols:, :])
        shid[t, half] = silu_mul(gate, upper)

    def results(zq, half):
        hid_copy(zq, half).wait_recv()
        for e in range(EXP_DEV):
            ys[e] = (
                mm(hid[0, zq, half, e], wd[e, :unit, :]) + mm(hid[1, zq, half, e], wd[e, unit:, :])
            ).astype(BF16)
        for p, cq in sides():
            chosen, weight = picks(zq, cq, half)
            parts = []
            for e in range(EXP_DEV):
                scale = jnp.sum(chosen[e] * weight[e : e + 1], axis=1, keepdims=True)
                part = ys[e, p * most : (p + 1) * most, :].astype(F32)
                parts.append((part * scale).astype(BF16))
            sel = jnp.concatenate(chosen, axis=0).astype(BF16)
            into = acc if p == 0 else outgo
            into[zq, half] = lax.dot_general(
                sel,
                jnp.concatenate(parts, axis=0),
                (((0,), (0,)), ((), ())),
                preferred_element_type=F32,
            ).astype(BF16)
        for q in range(2):
            sib_copy(zq, half, q).start()

    def is_end(zq):
        return ((zq > z) & jnp.logical_not(lo)) | ((zq < z) & jnp.logical_not(hi))

    def strip(q):
        return pl.ds(pl.multiple_of(q * piece, piece), piece)

    def on_stream(zq, h, half, q):
        r = half * 2 + q
        rows = pl.ds(pl.multiple_of(r * piece, piece), piece)
        kept = mm(act[rows, :], wo[:, out_cols(t)])
        sum_copy(r).wait_recv()
        line = srow[1, r, 0:1, :]
        theirs = jnp.sum(jnp.where(eye_piece, line, F32(0.0)), axis=1, keepdims=True)
        scale = lax.rsqrt((ssq[rows, 0:1] + theirs) / (2 * chan) + 1e-06)
        giv_copy(r).wait_recv()
        proj = (kept + grecv[r].astype(F32)) * scale
        blk[z * 2 + c, t, half, strip(q), :] = (res[rows, :].astype(F32) + proj).astype(BF16)
        c_copy(z, t, half, q).start()

        @pl.when(r == GIVEN[0])
        def _():
            for load in later:
                load.start()

        @pl.when(r == GIVEN[-1])
        def _():
            for load in later:
                load.wait()

    def on_land(zq, h, half, q):
        @pl.when((h == 0) & (q == 0))
        def _():
            m_copy(2, zq, c, half).wait_recv()
            m_copy(2, zq, c, half).start()

        arrived(zq, c, side(h), half, q)
        c_copy(zq, side(h), half, q).start()

    def on_z(way):
        def send(zq, h, half, q):
            @pl.when((h == 0) & (q == 0))
            def _():
                m_copy(way, zq, c, half).start()

            z_copy(way, zq, h, half, q).start()

        return send

    def on_across(zq, h, half, q):
        x_copy(zq, half, q).start()

    def on_hidden(zq, h, half, q):
        m_copy(2, zq, 1 - c, half).wait_recv()
        for hh in range(2):
            for qq in range(2):
                arrived(zq, 1 - c, hh, half, qq)
        hidden(zq, half)
        hid_copy(zq, half).start()

        @pl.when(zq == z)
        def _():
            shared(half)
            sh_copy(half).start()

    def on_result(zq, h, half, q):
        results(zq, half)

    def out_copy(half, q):
        return pltpu.make_async_copy(
            done.at[half, pl.ds(q * piece, piece)],
            out_hbm.at[pl.ds(half * half_rows + q * piece, piece)],
            out_sem.at[half, q],
        )

    def finish(half, q):
        rows = strip(q)

        @pl.when(q == 0)
        def _():
            sh_copy(half).wait_recv()

        fin = (
            blk[z * 2 + c, t, half, rows, :].astype(F32)
            + mm(shid[0, half, rows, :], sd[:unit, :])
            + mm(shid[1, half, rows, :], sd[unit:, :])
            + acc[z, half, rows, :].astype(F32)
            + sib[z, half, rows, :].astype(F32)
        )

        @pl.when(lo)
        def _():
            back_copy(z, half, q, z, up).wait_recv()

        @pl.when(hi)
        def _():
            back_copy(z, half, q, n_z, up).wait_recv()

        low = jnp.where(lo, back[z, half, rows, :].astype(F32), F32(0.0))
        high = jnp.where(hi, back[n_z, half, rows, :].astype(F32), F32(0.0))
        done[half, rows, :] = (fin + low + high).astype(BF16)
        out_copy(half, q).start()

    def on_combine(zq, h, half, q):
        rows = strip(q)
        sib_copy(zq, half, q).wait_recv()

        @pl.when(zq == z)
        def _():
            finish(half, q)

        @pl.when(zq != z)
        def _():
            @pl.when(is_end(zq))
            def _():
                acc[zq, half, rows, :] = (
                    acc[zq, half, rows, :].astype(F32) + sib[zq, half, rows, :].astype(F32)
                ).astype(BF16)

            @pl.when(jnp.logical_not(is_end(zq)))
            def _():
                back_copy(zq, half, q, zq, up).wait_recv()
                acc[zq, half, rows, :] = (
                    acc[zq, half, rows, :].astype(F32)
                    + sib[zq, half, rows, :].astype(F32)
                    + back[zq, half, rows, :].astype(F32)
                ).astype(BF16)

            @pl.when(zq > z)
            def _():
                back_copy(zq, half, q, zq, up).start()

            @pl.when(zq < z - 1)
            def _():
                back_copy(zq, half, q, zq, down).start()

            @pl.when(zq == z - 1)
            def _():
                back_copy(zq, half, q, n_z, down).start()

    actions = (
        on_stream,
        on_land,
        on_z(0),
        on_z(1),
        on_across,
        on_hidden,
        on_result,
        on_combine,
    )
    order, _ = plan(n_z)
    groups = max(-(-len(order[zz]) // 3) for zz in range(n_z))
    tables = [encode(order[zz], 3 * groups) for zz in range(n_z)]
    values = [
        sum((z == zz).astype(jnp.int32) * tables[zz][g] for zz in range(n_z)) for g in range(groups)
    ]

    @pl.loop(0, groups)
    def _(g):
        value = sum((g == k).astype(jnp.int32) * values[k] for k in range(groups))

        def turn(k, rest):
            mark = rest % BASE + 31
            q, half, h = mark % 2, mark // 2 % 2, mark // 4 % 2
            zq, kind = mark // 8 % 4, mark // 32
            for n, action in enumerate(actions):
                @pl.when(kind == n + 1)
                def _():
                    action(zq, h, half, q)

            return rest // BASE

        lax.fori_loop(0, 3, turn, value)

    @pl.when(has_next)
    def _():
        halo_copy().wait_send()

    fg_copy().wait_send()
    for r in range(n_chunks):
        sum_copy(r).wait_send()
        giv_copy(r).wait_send()
    for half in range(SPLIT):
        sh_copy(half).wait_send()

    for half in range(SPLIT):
        for q in range(2):
            out_copy(half, q).wait()

    def listed(target, half, q):
        inner = (target > 0) & (target < n_z - 1)
        outer_in, inner_in = half * 2 + q in FULL[0], half * 2 + q in FULL[1]
        return (inner & inner_in) | (jnp.logical_not(inner) & outer_in)

    for half in range(SPLIT):
        for q in range(2):
            for way, there, target in ((0, hi, z + 1), (1, lo, z - 1)):

                @pl.when(there & listed(target, half, q))
                def _():
                    z_copy(way, z, 1, half, q).wait_send()

    @pl.loop(0, n_z)
    def _(zq):
        for way, there in ((0, hi & (zq <= z)), (1, lo & (zq >= z))):

            @pl.when(there)
            def _():
                for half in range(SPLIT):
                    m_copy(way, zq, c, half).wait_send()
                    for q in range(2):
                        z_copy(way, zq, 0, half, q).wait_send()

        near = (zq == z + 1) | (zq == z - 1)
        for half in range(SPLIT):
            m_copy(2, zq, c, half).wait_send()
            for q in range(2):

                @pl.when(jnp.logical_not(near & listed(z, half, q)))
                def _():
                    x_copy(zq, half, q).wait_send()

                for h in range(2):
                    c_copy(zq, h, half, q).wait_send()
                sib_copy(zq, half, q).wait_send()

                @pl.when(zq != z)
                def _():
                    back_copy(zq, half, q, zq, up).wait_send()

            hid_copy(zq, half).wait_send()


def fast(
    out_gate,
    in_gate,
    conv_input,
    doc_ids,
    residual,
    conv_taps,
    mix_gain,
    out_weight,
    ffn_gain,
    routing,
    route_weight,
    expert_gate,
    expert_up,
    expert_down,
    shared_gate,
    shared_up,
    shared_down,
):
    tokens, cols = residual.shape
    chan, width = out_weight.shape
    n_tp, n_sp = lax.axis_size("tp"), lax.axis_size("sp")
    n_z = n_sp // 2
    rows = tokens // n_tp
    experts = n_sp * EXP_DEV
    most = max(1, 2 * rows * TOPK // experts)
    lanes = 128
    piece = rows // 2
    blocks = n_sp
    unit = expert_gate.shape[2]
    vm = pl.BlockSpec(memory_space=pltpu.VMEM)
    hbm = pl.BlockSpec(memory_space=pl.ANY)
    dma = pltpu.SemaphoreType.DMA
    return pl.pallas_call(
        functools.partial(layer_kernel, n_z, most),
        out_shape=jax.ShapeDtypeStruct((tokens, cols), BF16),
        in_specs=[hbm] * 5 + [vm] * 6 + [hbm] * 6,
        out_specs=hbm,
        scratch_shapes=[
            pltpu.VMEM((tokens, chan), BF16),
            pltpu.VMEM((tokens, chan), BF16),
            pltpu.VMEM((tokens, chan), BF16),
            pltpu.VMEM((tokens, cols), BF16),
            pltpu.VMEM((chan, width), BF16),
            pltpu.VMEM(expert_gate.shape, BF16),
            pltpu.VMEM(expert_up.shape, BF16),
            pltpu.VMEM(expert_down.shape, BF16),
            pltpu.VMEM(shared_gate.shape, BF16),
            pltpu.VMEM(shared_up.shape, BF16),
            pltpu.VMEM(shared_down.shape, BF16),
            pltpu.VMEM((tokens + 16, chan), F32),
            pltpu.VMEM((tokens + 16, lanes), F32),
            pltpu.VMEM((8, chan + lanes), F32),
            pltpu.VMEM((8, chan + lanes), F32),
            pltpu.VMEM((tokens, chan), BF16),
            pltpu.VMEM((tokens, lanes), F32),
            pltpu.VMEM((2, 2 * SPLIT, 8, lanes), F32),
            pltpu.VMEM((2 * SPLIT, piece, cols), BF16),
            pltpu.VMEM((2 * SPLIT, piece, cols), BF16),
            pltpu.VMEM((2, 1, cols), F32),
            pltpu.VMEM((rows, rows), BF16),
            pltpu.VMEM((blocks, 2, SPLIT, rows, cols), BF16),
            pltpu.VMEM((blocks, SPLIT, 8, rows + -rows % lanes), F32),
            pltpu.VMEM((EXP_DEV, 2 * most, width), BF16),
            pltpu.VMEM((2, n_z, SPLIT, EXP_DEV, 2 * most, unit), BF16),
            pltpu.VMEM((2, SPLIT, rows, unit), BF16),
            pltpu.VMEM((EXP_DEV, 2 * most, cols), BF16),
            pltpu.VMEM((n_z, SPLIT, rows, cols), BF16),
            pltpu.VMEM((n_z, SPLIT, rows, cols), BF16),
            pltpu.VMEM((n_z, SPLIT, rows, cols), BF16),
            pltpu.VMEM((n_z + 1, SPLIT, rows, cols), BF16),
            pltpu.VMEM((SPLIT, rows, cols), BF16),
            dma((11,)),
            dma((2,)),
            dma((2, 2 * SPLIT)),
            dma((2,)),
            dma((2 * SPLIT,)),
            dma((2 * SPLIT,)),
            dma((2, n_z + 1, SPLIT, 2)),
            dma((n_z, SPLIT, 2)),
            dma((n_z, 2, SPLIT, 2)),
            dma((blocks, 2, SPLIT, 2)),
            dma((3, n_z, SPLIT)),
            dma((blocks, SPLIT)),
            dma((n_z, SPLIT)),
            dma((n_z, SPLIT)),
            dma((SPLIT,)),
            dma((SPLIT,)),
            dma((n_z, SPLIT, 2)),
            dma((n_z, SPLIT, 2)),
            dma((n_z, SPLIT, 2)),
            dma((n_z + 1, SPLIT, 2)),
            dma((SPLIT, 2)),
        ],
        compiler_params=pltpu.CompilerParams(
            collective_id=0, has_side_effects=True, vmem_limit_bytes=64 * 1024 * 1024 - 65536
        ),
    )(
        out_gate,
        in_gate,
        conv_input,
        residual,
        out_weight,
        doc_ids[None, :],
        conv_taps,
        mix_gain[None, :],
        ffn_gain[None, :],
        routing.T,
        route_weight.T,
        expert_gate,
        expert_up,
        expert_down,
        shared_gate,
        shared_up,
        shared_down,
    )


def fits(mesh):
    return mesh.shape["tp"] == 2 and mesh.shape["sp"] in (4, 6, 8)


def solution(mesh):
    return jax.shard_map(
        fast if fits(mesh) else body,
        mesh=mesh,
        in_specs=(
            P(("grp", "sp"), "tp"),
            P(("grp", "sp"), "tp"),
            P(("grp", "sp"), "tp"),
            P(("grp", "sp")),
            P(("grp", "sp"), "tp"),
            P(None, "tp"),
            P("tp"),
            P("tp", None),
            P("tp"),
            P(("grp", "sp"), None),
            P(("grp", "sp"), None),
            P("sp", None, "tp"),
            P("sp", None, "tp"),
            P("sp", None, "tp"),
            P(None, "tp"),
            P(None, "tp"),
            P(None, "tp"),
        ),
        out_specs=P(("grp", "sp"), "tp"),
        check_vma=False,
    )
```

```python
import functools

import jax
import jax.numpy as jnp
from jax import lax
from jax.experimental import pallas as pl
from jax.experimental.pallas import tpu as pltpu
from jax.sharding import PartitionSpec as P

D_CONV = 1024
CONV_K = 3
TOPK = 2
EXP_DEV = 2


def from_behind(value, axis, steps):
    count = lax.axis_size(axis)
    first, last = (max(0, -steps), min(count, count - steps))
    return lax.ppermute(value, axis, [(source, source + steps) for source in range(first, last)])


def body(
    out_gate,
    in_gate,
    conv_input,
    doc_ids,
    residual,
    conv_taps,
    mix_gain,
    out_weight,
    ffn_gain,
    routing,
    route_weight,
    expert_gate,
    expert_up,
    expert_down,
    shared_gate,
    shared_up,
    shared_down,
):
    tokens = residual.shape[0]
    width = out_weight.shape[1]
    n_tp = lax.axis_size("tp")
    n_sp = lax.axis_size("sp")
    rows = tokens // n_tp
    experts = n_sp * EXP_DEV
    most = max(1, 2 * rows * TOPK // experts)
    slots = n_tp * most
    total = experts * slots
    cols = expert_down.shape[2]
    product = (in_gate.astype(jnp.float32) * conv_input.astype(jnp.float32)).astype(jnp.bfloat16)
    tail = (product[tokens - CONV_K + 1 :], doc_ids[tokens - CONV_K + 1 :].astype(jnp.bfloat16))
    prev_rows, prev_docs = from_behind((tail[0], tail[1]), "sp", 1)
    extended = jnp.concatenate([prev_rows, product], axis=0).astype(jnp.float32)
    ext_docs = jnp.concatenate([prev_docs.astype(jnp.int32), doc_ids])
    mixed = jnp.zeros(product.shape, jnp.float32)
    for k in range(CONV_K):
        keep = (ext_docs[k : k + tokens] == doc_ids)[:, None]
        mixed = mixed + jnp.where(keep, conv_taps[k] * extended[k : k + tokens], jnp.float32(0.0))
    conv_out = out_gate.astype(jnp.float32) * mixed
    squares = lax.psum(jnp.sum(conv_out * conv_out, axis=1), "tp")
    normed = (conv_out * lax.rsqrt(squares / D_CONV + 1e-06)[:, None] * mix_gain).astype(
        jnp.bfloat16
    )
    partial_value = jnp.dot(normed, out_weight, preferred_element_type=jnp.float32)
    proj = lax.psum_scatter(
        partial_value.astype(jnp.bfloat16), "tp", scatter_dimension=1, tiled=True
    ).astype(jnp.float32)
    stream = (residual.astype(jnp.float32) + proj).astype(jnp.bfloat16)
    stream32 = stream.astype(jnp.float32)
    stream_sq = lax.psum(jnp.sum(stream32 * stream32, axis=1), "tp")
    normal_cols = (stream32 * lax.rsqrt(stream_sq / width + 1e-06)[:, None] * ffn_gain).astype(
        jnp.bfloat16
    )
    flat_expert = routing.reshape(-1)
    onehot = (flat_expert[:, None] == jnp.arange(experts, dtype=jnp.int32)[None, :]).astype(
        jnp.int32
    )
    blocked = onehot.reshape(n_tp, rows * TOPK, experts)
    earlier = jnp.cumsum(blocked, axis=1) - blocked
    position = jnp.sum(earlier * blocked, axis=2).reshape(-1)
    entry = jnp.arange(tokens * TOPK, dtype=jnp.int32)
    slot = flat_expert * slots + entry // (rows * TOPK) * most + position
    table = jnp.full((total,), tokens, jnp.int32).at[slot].set(entry // TOPK)
    block_rows = lax.all_to_all(normal_cols, "tp", split_axis=0, concat_axis=1, tiled=True)
    mine = lax.dynamic_index_in_dim(
        table.reshape(n_sp, EXP_DEV, n_tp, most), lax.axis_index("tp"), 2, False
    )
    local = jnp.where(mine >= tokens, rows, mine - lax.axis_index("tp") * rows)
    padded_block = jnp.concatenate([block_rows, jnp.zeros((1, width), jnp.bfloat16)], axis=0)
    got = lax.all_to_all(padded_block[local], "sp", split_axis=0, concat_axis=0, tiled=True)
    arrived, whole = (
        lax.all_gather(got, "tp", axis=2, tiled=True),
        lax.all_gather(block_rows.reshape(1, 1, rows, width), "tp", axis=2, tiled=True),
    )
    normal = whole.reshape(tokens, width)
    gate = jnp.einsum("nesd,edh->nesh", arrived, expert_gate, preferred_element_type=jnp.float32)
    upper = jnp.einsum("nesd,edh->nesh", arrived, expert_up, preferred_element_type=jnp.float32)
    hidden = (jax.nn.silu(gate) * upper).astype(jnp.bfloat16)
    hidden_flat = hidden.reshape(n_sp * EXP_DEV * slots, hidden.shape[3])
    shared_hid = (
        jax.nn.silu(jnp.dot(normal, shared_gate, preferred_element_type=jnp.float32))
        * jnp.dot(normal, shared_up, preferred_element_type=jnp.float32)
    ).astype(jnp.bfloat16)
    expert_piece = lax.all_gather(hidden_flat, "tp", axis=1, tiled=True)
    shared_piece = lax.all_gather(shared_hid, "tp", axis=1, tiled=True)
    count = expert_piece.shape[1]
    expert_part = jnp.einsum(
        "nesh,ehd->nesd",
        expert_piece.reshape(n_sp, EXP_DEV, slots, count),
        expert_down,
        preferred_element_type=jnp.float32,
    )
    shared_part = jnp.dot(shared_piece, shared_down, preferred_element_type=jnp.float32)
    returned = lax.all_to_all(
        expert_part.astype(jnp.bfloat16), "sp", split_axis=0, concat_axis=0, tiled=True
    )
    picked = (
        returned.reshape(total, cols)[slot].astype(jnp.float32) * route_weight.reshape(-1)[:, None]
    )
    routed = jnp.sum(picked.reshape(tokens, TOPK, cols), axis=1)
    return (stream32 + shared_part + routed).astype(jnp.bfloat16)


MESH = pl.DeviceIdType.MESH
F32 = jnp.float32
BF16 = jnp.bfloat16


def silu_mul(gate, upper):
    return (gate / (1.0 + jnp.exp(-gate)) * upper).astype(BF16)


def mm(a, b):
    return jnp.dot(a, b, preferred_element_type=F32)


SPLIT = 2


GIVEN = (1, 0, 2, 3)
HOP, START, WIRE, NEAR = 2.8, 4.5, 4.18, (1.4, 2.5)
COST, EXTRA = (0.45, 0.15, 0.15, 0.15, 0.15, 1.65, 1.3, 0.22), (0.9, 0.3)
FULL = ((0, 2, 3), (0,), (1, 2, 3))
ROWX = (3.2, 7.8, -0.1, 7, 2.4, 1.9, -0.8, -4.5, -6.9, -1.3, -4.6, -1.2, -3.6, -2.7, -3.5, -1.3)
ROWZ = (5.3, -4.7, 3.6, 4.1, 6.5, 4, 5.6, -2.5, -3.8, 5.1, 3.9, -2.9, -5.3, 4.7, -3.6, 0.2)
ROWF = (-0.1, -5.8, 4.7, 4.9)
COMB = (5, -4.9, -3.1, 0.6, -2, -2.4, 5.5, -0.2, -1.5, -3.6, -4.8, 1.4, -0.4, 7.5, -2.3, -2.3)
WORK = (-3.4, 3.1, -3.1, 1.5, 1.1, -1.8, 5.4, -5.7, -0.1, 1.1, -4, 2.1, -4.3, 1.7, -0.5, 1)
RANK = (4, 0, 0, 0, 4)
DEPTH = (1, 2)
BASE = 257


KINDS = ("stream", "land", "up", "down", "across", "hidden", "result", "combine")


def inner(n_z, z):
    return int(0 < z < n_z - 1)


def full_rows(n_z, source, target, half, q):
    kind = inner(n_z, target) * (1 + inner(n_z, source))
    return abs(source - target) == 1 and half * 2 + q in FULL[kind]


def plan(n_z):
    chunks = [(half, q) for half in range(SPLIT) for q in range(2)]
    zones = range(n_z)
    never = 1e9
    have, told, heard, summed, went, final, arrive = {}, {}, {}, {}, {}, {}, {}
    todo = {z: [] for z in zones}
    for z in zones:
        for k, (half, q) in enumerate(chunks):
            todo[z].append(("stream", z, 0, half, q))
            went[z, half, q] = START + WIRE * (GIVEN.index(k) + 1) + HOP
        for zq in zones:
            for half, q in chunks:
                if zq != z:
                    todo[z].append(("land", zq, 0, half, q))
                todo[z].append(("land", zq, 1, half, q))
                if zq <= z < n_z - 1:
                    todo[z].append(("up", zq, 0, half, q))
                if zq >= z > 0:
                    todo[z].append(("down", zq, 0, half, q))
                if not full_rows(n_z, zq, z, half, q):
                    todo[z].append(("across", zq, 0, half, q))
                todo[z].append(("combine", zq, 0, half, q))
            for half in range(SPLIT):
                todo[z].append(("hidden", zq, 0, half, 0))
                todo[z].append(("result", zq, 0, half, 0))
        for half, q in chunks:
            if z < n_z - 1 and full_rows(n_z, z, z + 1, half, q):
                todo[z].append(("up", z, 1, half, q))
            if z > 0 and full_rows(n_z, z, z - 1, half, q):
                todo[z].append(("down", z, 1, half, q))
    link = {(z, way): 0.0 for z in zones for way in ("up", "down", "across")}
    for z in zones:
        link[z, "across"] = START + WIRE * len(chunks)
    core = {z: START for z in zones}

    def put(z, way, now, size):
        link[z, way] = max(now, link[z, way]) + WIRE * size
        return link[z, way] + HOP

    def ready(z, event):
        kind, zq, h, half, q = event
        if kind == "stream":
            return went[z, half, q]
        if kind == "land":
            return arrive.get((z, zq, h, half, q), never)
        if kind in ("up", "down", "across"):
            depth = DEPTH[kind == "across"]
            return max(have.get((z, zq, h, half, q), never), link[z, kind] - depth)
        if kind == "hidden":
            parts = [have.get((z, zq, g, half, p), never) for g in range(2) for p in range(2)]
            return max(parts) + NEAR[0]
        if kind == "result":
            return heard.get((z, zq, half), never)
        at = told.get((z, zq, half), never)
        if zq >= z and z > 0:
            at = max(at, summed.get((z - 1, zq, half, q), never))
        if zq <= z and z < n_z - 1:
            at = max(at, summed.get((z + 1, zq, half, q), never))
        if zq == z and q > 0:
            at = max(at, final.get((z, half, q - 1), never))
        return at

    def rank(z, event):
        kind, zq, h, half, q = event
        place = (inner(n_z, z) * 4 + abs(zq - z)) * 2 + half
        if kind in ("stream", "land"):
            return (RANK[0], 0.0, q)
        if kind == "combine":
            return (RANK[1], COMB[place], q)
        if kind == "result":
            return (RANK[2], WORK[place], q)
        if kind == "hidden":
            return (RANK[3], WORK[place], q)
        if kind == "across":
            return (RANK[4], ROWX[place], q)
        return (RANK[4], ROWZ[place] if h == 0 else ROWF[inner(n_z, z) * 2 + half], q)

    order = {z: [] for z in zones}
    while any(todo.values()):
        best = None
        for z in zones:
            if not todo[z]:
                continue
            starts = [(max(core[z], ready(z, event)), event) for event in todo[z]]
            at = min(start for start, _ in starts)
            if best is None or at < best[0]:
                best = (at, z, starts)
        at, z, starts = best
        assert at < never
        event = min((e for start, e in starts if start <= at), key=lambda e: rank(z, e))
        kind, zq, h, half, q = event
        todo[z].remove(event)
        order[z].append(event)
        end = at + COST[KINDS.index(kind)]
        if zq == z:
            end = end + (EXTRA[0] if kind == "hidden" else EXTRA[1] if kind == "combine" else 0.0)
        core[z] = end
        if kind in ("stream", "land"):
            have[z, zq, h, half, q] = end
        elif kind in ("up", "down"):
            arrive[z + (1 if kind == "up" else -1), zq, h, half, q] = put(z, kind, end, 1.0)
        elif kind == "across":
            arrive[z, zq, 1, half, q] = put(z, kind, end, 1.0)
        elif kind == "hidden":
            heard[z, zq, half] = put(z, "across", end, 1.0 if zq == z else 0.5)
        elif kind == "result":
            told[z, zq, half] = end + NEAR[1]
        elif zq == z:
            final[z, half, q] = end
        else:
            summed[z, zq, half, q] = put(z, "up" if zq > z else "down", end, 1.0)
    return order, max(final.values())


def encode(events, slots):
    codes = [
        (((KINDS.index(kind) * 4 + zq) * 2 + h) * 2 + half) * 2 + q + 1
        for kind, zq, h, half, q in events
    ]
    codes += [0] * (slots - len(codes))
    return [sum(codes[at + k] * BASE**k for k in range(3)) for at in range(0, slots, 3)]


def layer_kernel(
    n_z,
    most,
    og_hbm,
    ig_hbm,
    ci_hbm,
    res_hbm,
    wo_hbm,
    docs_ref,
    taps_ref,
    mix_ref,
    ffn_ref,
    names_ref,
    share_ref,
    wg_hbm,
    wu_hbm,
    wd_hbm,
    sg_hbm,
    su_hbm,
    sd_hbm,
    out_hbm,
    og,
    ig,
    ci,
    res,
    wo,
    wg,
    wu,
    wd,
    sg,
    su,
    sd,
    ext,
    dext,
    hsend,
    hrecv,
    act,
    ssq,
    srow,
    gsend,
    grecv,
    fg,
    tri,
    blk,
    meta,
    xs,
    hid,
    shid,
    ys,
    acc,
    outgo,
    sib,
    back,
    done,
    load_sem,
    halo_sem,
    sum_sem,
    fg_sem,
    giv_recv,
    z_send,
    x_send,
    c_send,
    b_recv,
    s_recv,
    m_send,
    m_recv,
    hid_send,
    hid_recv,
    sh_send,
    sh_recv,
    sib_send,
    sib_recv,
    back_send,
    back_recv,
    out_sem,
):
    first = [
        pltpu.make_async_copy(src, dst, load_sem.at[n])
        for n, (src, dst) in enumerate(
            ((ig_hbm, ig), (ci_hbm, ci), (og_hbm, og), (wo_hbm, wo), (res_hbm, res))
        )
    ]
    later = [
        pltpu.make_async_copy(src, dst, load_sem.at[5 + n])
        for n, (src, dst) in enumerate(
            ((wg_hbm, wg), (wu_hbm, wu), (wd_hbm, wd), (sg_hbm, sg), (su_hbm, su), (sd_hbm, sd))
        )
    ]
    for load in first:
        load.start()
    s = lax.axis_index("sp")
    t = lax.axis_index("tp")
    z = s // 2
    c = s % 2
    tokens, chan = ig.shape
    cols = res.shape[1]
    width = 2 * cols
    half_rows = tokens // SPLIT
    n_chunks = 2 * SPLIT
    piece = half_rows // 2
    unit = wg.shape[2]
    pad = ext.shape[0] - tokens
    lo = z > 0
    hi = z < n_z - 1
    up, down = {"sp": s + 2}, {"sp": s - 2}
    other, peer = {"sp": s + 1 - 2 * c}, {"tp": 1 - t}
    after = {"sp": s + 1}
    before = {"sp": s - 1}
    targets = (up, down, peer, other)

    def remote(src, dst, ssem, rsem, dev):
        return pltpu.make_async_remote_copy(
            src_ref=src,
            dst_ref=dst,
            send_sem=ssem,
            recv_sem=rsem,
            device_id=dev,
            device_id_type=MESH,
        )

    def chunk(zq, h, half, q, ssem, rsem, dev):
        ref = blk.at[zq * 2 + c, half, h, pl.ds(q * piece, piece)]
        return remote(ref, ref, ssem, rsem, dev)

    def side(h):
        return t + h * (1 - 2 * t)

    def z_copy(way, zq, h, half, q):
        row = (zq + way) * (1 - h) + (n_z + 1 + way) * h
        return chunk(
            zq,
            side(h),
            half,
            q,
            z_send.at[row, half, q],
            b_recv.at[zq, side(h), half, q],
            targets[way],
        )

    def x_copy(zq, half, q):
        return chunk(zq, t, half, q, x_send.at[zq, half, q], b_recv.at[zq, t, half, q], peer)

    def c_copy(zq, h, half, q):
        return chunk(zq, h, half, q, c_send.at[zq, h, half, q], s_recv.at[zq, half], other)

    def near_by(zq, half):
        ref = blk.at[zq * 2 + 1 - c, half]
        return remote(ref, ref, c_send.at[0, 0, 0, 0], s_recv.at[zq, half], other)

    def arrived(zq, h, half, q):
        chunk(zq, h, half, q, x_send.at[zq, half, q], b_recv.at[zq, h, half, q], peer).wait_recv()

    def m_copy(way, zq, cq, half):
        ref = meta.at[zq * 2 + cq, half]
        row = zq + (0, 1, n_z + 1)[way]
        ssem = m_send.at[row, half]
        return remote(ref, ref, ssem, m_recv.at[zq * 2 + cq, half], (up, down, other)[way])

    def hid_copy(zq, half):
        return remote(
            hid.at[t, zq, half],
            hid.at[t, zq, half],
            hid_send.at[zq, half],
            hid_recv.at[zq, half],
            peer,
        )

    def sh_copy(half):
        return remote(
            shid.at[t, half], shid.at[t, half], sh_send.at[half], sh_recv.at[half], peer
        )

    def sib_copy(zq, half, q):
        rows = pl.ds(q * piece, piece)
        return remote(
            outgo.at[zq, half, rows],
            sib.at[zq, half, rows],
            sib_send.at[zq, half, q],
            sib_recv.at[zq, half, q],
            other,
        )

    def back_copy(zq, half, q, to, dev):
        return remote(
            acc.at[zq, half, pl.ds(q * piece, piece)],
            back.at[to, half, pl.ds(q * piece, piece)],
            back_send.at[zq, half, q],
            back_recv.at[to, half, q],
            dev,
        )

    def halo_copy():
        return remote(hsend, hrecv, halo_sem.at[0], halo_sem.at[1], after)

    def sum_copy(r):
        return remote(srow.at[0, r], srow.at[1, r], sum_sem.at[n_chunks + r], sum_sem.at[r], peer)

    def fg_copy():
        return remote(fg.at[t], fg.at[t], fg_sem.at[0], fg_sem.at[1], peer)

    def giv_copy(r):
        return remote(gsend.at[r], grecv.at[r], giv_recv.at[n_chunks + r], giv_recv.at[r], peer)

    barrier = pltpu.get_barrier_semaphore()
    cross_up = hi & (c == 1)
    cross_down = lo & (c == 0)
    for target, there in ((up, hi), (down, lo), (after, cross_up), (before, cross_down)):

        @pl.when(there)
        def _():
            pl.semaphore_signal(barrier, inc=1, device_id=target, device_id_type=MESH)

    for target in (peer, other):
        pl.semaphore_signal(barrier, inc=1, device_id=target, device_id_type=MESH)

    has_next = s < 2 * n_z - 1
    has_prev = s > 0
    first[0].wait()
    first[1].wait()

    tail = 16

    def product(rows):
        return (ig[rows, :].astype(F32) * ci[rows, :].astype(F32)).astype(BF16).astype(F32)

    lanes = dext.shape[1]
    eye = lax.broadcasted_iota(jnp.int32, (lanes, lanes), 0) == lax.broadcasted_iota(
        jnp.int32, (lanes, lanes), 1
    )

    def upright(line):
        return jnp.sum(jnp.where(eye, line, F32(0.0)), axis=1, keepdims=True)

    docs = docs_ref[...].astype(F32)
    for k in range(tokens // lanes):
        column = upright(docs[k : k + 1, :])
        dext[pad + k * lanes : pad + (k + 1) * lanes, :] = jnp.broadcast_to(column, (lanes, lanes))
    end_rows = product(pl.ds(tokens - tail, tail))
    hsend[:, :chan] = end_rows[tail - 8 :]
    hsend[:, chan:] = dext[pad + tokens - 8 : pad + tokens, :]
    own = z * 2 + c
    names = names_ref[...].astype(F32)
    share = share_ref[...]
    for half in range(SPLIT):
        part = slice(half * half_rows, (half + 1) * half_rows)
        meta[own, half] = jnp.zeros(meta.shape[2:], F32)
        meta[own, half, 0:TOPK, :half_rows] = names[:, part]
        meta[own, half, TOPK : 2 * TOPK, :half_rows] = share[:, part]
    fg[t] = ffn_ref[...]
    step_rows = 32

    @pl.loop(0, tokens // step_rows)
    def _(i):
        at = pl.multiple_of(i * step_rows, step_rows)
        ext[pl.ds(pad + at, step_rows), :] = product(pl.ds(at, step_rows))

    n_tri = tri.shape[0]
    row_id = lax.broadcasted_iota(jnp.int32, (n_tri, n_tri), 0)
    col_id = lax.broadcasted_iota(jnp.int32, (n_tri, n_tri), 1)
    tri[...] = (row_id < col_id).astype(F32).astype(BF16)

    def convolve(r):
        @pl.loop(0, piece // step_rows)
        def _(i):
            at = pl.multiple_of(r * piece + i * step_rows, step_rows)
            v = ext[pl.ds(pl.multiple_of(pad - 8 + at, 8), step_rows + 8), :]
            d = dext[pl.ds(pl.multiple_of(pad - 8 + at, 8), step_rows + 8), :]
            doc = d[8:]
            mixed = None
            for k in range(CONV_K):
                by = CONV_K - 1 - k
                if by:
                    same = (pltpu.roll(d, by, 0)[8:] == doc).astype(F32)
                    same = jnp.concatenate([same] * (chan // lanes), axis=1)
                    term = taps_ref[k : k + 1, :] * pltpu.roll(v, by, 0)[8:] * same
                else:
                    term = taps_ref[k : k + 1, :] * v[8:]
                mixed = term if mixed is None else mixed + term
            rows = pl.ds(at, step_rows)
            conv_out = og[rows, :].astype(F32) * mixed
            total = jnp.sum(conv_out * conv_out, axis=1, keepdims=True)
            ssq[rows, :] = jnp.broadcast_to(total, (step_rows, lanes))
            act[rows, :] = (conv_out * mix_ref[...]).astype(BF16)

    eye_piece = lax.broadcasted_iota(jnp.int32, (piece, lanes), 0) == lax.broadcasted_iota(
        jnp.int32, (piece, lanes), 1
    )

    def out_cols(who):
        return pl.ds(pl.multiple_of(who * cols, cols), cols)

    def sums(r):
        part = ssq[r * piece : (r + 1) * piece, :]
        line = jnp.sum(jnp.where(eye_piece, part, F32(0.0)), axis=0, keepdims=True)
        srow[0, r] = jnp.broadcast_to(line, srow.shape[2:])

    def give(r):
        gsend[r] = mm(act[r * piece : (r + 1) * piece, :], wo[:, out_cols(1 - t)]).astype(BF16)

    def send_given(r):
        sum_copy(r).start()
        giv_copy(r).start()

    first[2].wait()
    for r in GIVEN:
        if r:
            convolve(r)
            sums(r)
    first[3].wait()
    give(GIVEN[0])
    first[4].wait()
    arrivals = (
        2
        + lo.astype(jnp.int32)
        + hi.astype(jnp.int32)
        + cross_up.astype(jnp.int32)
        + cross_down.astype(jnp.int32)
    )
    pl.semaphore_wait(barrier, arrivals)

    @pl.when(has_next)
    def _():
        halo_copy().start()

    fg_copy().start()
    send_given(GIVEN[0])
    for half in range(SPLIT):
        m_copy(2, z, c, half).start()

    @pl.when(has_prev)
    def _():
        halo_copy().wait_recv()
        ext[pad - 8 : pad, :] = hrecv[:, :chan]
        dext[pad - 8 : pad, :] = hrecv[:, chan:]

    @pl.when(jnp.logical_not(has_prev))
    def _():
        ext[pad - 8 : pad, :] = jnp.zeros((8, chan), F32)
        dext[pad - 8 : pad, :] = jnp.zeros((8, lanes), F32)

    convolve(0)
    sums(0)
    for r in GIVEN[1:]:
        give(r)
        send_given(r)
    fg_copy().wait_recv()

    def picks(zq, cq, half):
        info = meta[zq * 2 + cq, half][:, :half_rows]
        mine = (lax.broadcasted_iota(jnp.int32, (8, half_rows), 0) + s * EXP_DEV).astype(F32)
        hot0 = info[0:1] == mine
        hot1 = info[1:2] == mine
        hot = hot0 | hot1
        earlier = mm(hot.astype(F32).astype(BF16), tri[...])
        position = jnp.where(hot, earlier, F32(-1.0))
        weight = jnp.where(hot0, info[2:3], F32(0.0)) + jnp.where(hot1, info[3:4], F32(0.0))
        place = lax.broadcasted_iota(jnp.int32, (most, half_rows), 0).astype(F32)
        chosen = [(position[e : e + 1] == place).astype(F32) for e in range(EXP_DEV)]
        return chosen, weight

    def norm_scale(parts):
        total = sum(jnp.sum(part * part, axis=1, keepdims=True) for part in parts)
        return lax.rsqrt(total / width + 1e-06)

    def normal_of(parts):
        scale = norm_scale(parts)
        return [(part * scale * fg[h, 0:1, :]).astype(BF16) for h, part in enumerate(parts)]

    def sides():
        return [(0, c), (1, 1 - c)]

    def hidden(zq, half):
        for p, cq in sides():
            chosen, _ = picks(zq, cq, half)
            sel = jnp.concatenate(chosen, axis=0).astype(BF16)
            got = normal_of([mm(sel, blk[zq * 2 + cq, half, h]) for h in range(2)])
            for h in range(2):
                for e in range(EXP_DEV):
                    xs[e, p * most : (p + 1) * most, h * cols : (h + 1) * cols] = got[h][
                        e * most : (e + 1) * most
                    ]
        for e in range(EXP_DEV):
            hid[t, zq, half, e] = silu_mul(mm(xs[e], wg[e]), mm(xs[e], wu[e]))

    def shared(half):
        whole = normal_of([blk[z * 2 + c, half, h].astype(F32) for h in range(2)])
        gate = mm(whole[0], sg[:cols, :]) + mm(whole[1], sg[cols:, :])
        upper = mm(whole[0], su[:cols, :]) + mm(whole[1], su[cols:, :])
        shid[t, half] = silu_mul(gate, upper)

    def results(zq, half):
        hid_copy(zq, half).wait_recv()
        for e in range(EXP_DEV):
            ys[e] = (
                mm(hid[0, zq, half, e], wd[e, :unit, :]) + mm(hid[1, zq, half, e], wd[e, unit:, :])
            ).astype(BF16)
        for p, cq in sides():
            chosen, weight = picks(zq, cq, half)
            parts = []
            for e in range(EXP_DEV):
                scale = jnp.sum(chosen[e] * weight[e : e + 1], axis=1, keepdims=True)
                part = ys[e, p * most : (p + 1) * most, :].astype(F32)
                parts.append((part * scale).astype(BF16))
            sel = jnp.concatenate(chosen, axis=0).astype(BF16)
            into = acc if p == 0 else outgo
            into[zq, half] = lax.dot_general(
                sel,
                jnp.concatenate(parts, axis=0),
                (((0,), (0,)), ((), ())),
                preferred_element_type=F32,
            ).astype(BF16)
        for q in range(2):
            sib_copy(zq, half, q).start()

    def is_end(zq):
        return ((zq > z) & jnp.logical_not(lo)) | ((zq < z) & jnp.logical_not(hi))

    def strip(q):
        return pl.ds(pl.multiple_of(q * piece, piece), piece)

    def on_stream(zq, h, half, q):
        r = half * 2 + q
        rows = pl.ds(pl.multiple_of(r * piece, piece), piece)
        kept = mm(act[rows, :], wo[:, out_cols(t)])
        sum_copy(r).wait_recv()
        line = srow[1, r, 0:1, :]
        theirs = jnp.sum(jnp.where(eye_piece, line, F32(0.0)), axis=1, keepdims=True)
        scale = lax.rsqrt((ssq[rows, 0:1] + theirs) / (2 * chan) + 1e-06)
        giv_copy(r).wait_recv()
        proj = (kept + grecv[r].astype(F32)) * scale
        blk[z * 2 + c, half, t, strip(q), :] = (res[rows, :].astype(F32) + proj).astype(BF16)
        c_copy(z, t, half, q).start()

        @pl.when(r == GIVEN[0])
        def _():
            for load in later:
                load.start()

        @pl.when(r == GIVEN[-1])
        def _():
            for load in later:
                load.wait()

    def on_land(zq, h, half, q):
        @pl.when((h == 0) & (q == 0))
        def _():
            m_copy(2, zq, c, half).wait_recv()
            m_copy(2, zq, c, half).start()

        arrived(zq, side(h), half, q)
        c_copy(zq, side(h), half, q).start()

    def on_z(way):
        def send(zq, h, half, q):
            @pl.when((h == 0) & (q == 0))
            def _():
                m_copy(way, zq, c, half).start()

            z_copy(way, zq, h, half, q).start()

        return send

    def on_across(zq, h, half, q):
        x_copy(zq, half, q).start()

    def on_hidden(zq, h, half, q):
        m_copy(2, zq, 1 - c, half).wait_recv()
        near_by(zq, half).wait_recv()
        hidden(zq, half)
        hid_copy(zq, half).start()

        @pl.when(zq == z)
        def _():
            shared(half)
            sh_copy(half).start()

    def on_result(zq, h, half, q):
        results(zq, half)

    def out_copy(half, q):
        return pltpu.make_async_copy(
            done.at[half, pl.ds(q * piece, piece)],
            out_hbm.at[pl.ds(half * half_rows + q * piece, piece)],
            out_sem.at[half, q],
        )

    def finish(half, q):
        rows = strip(q)

        @pl.when(q == 0)
        def _():
            sh_copy(half).wait_recv()

        fin = (
            blk[z * 2 + c, half, t, rows, :].astype(F32)
            + mm(shid[0, half, rows, :], sd[:unit, :])
            + mm(shid[1, half, rows, :], sd[unit:, :])
            + acc[z, half, rows, :].astype(F32)
            + sib[z, half, rows, :].astype(F32)
        )

        @pl.when(lo)
        def _():
            back_copy(z, half, q, z, up).wait_recv()

        @pl.when(hi)
        def _():
            back_copy(z, half, q, n_z, up).wait_recv()

        low = jnp.where(lo, back[z, half, rows, :].astype(F32), F32(0.0))
        high = jnp.where(hi, back[n_z, half, rows, :].astype(F32), F32(0.0))
        done[half, rows, :] = (fin + low + high).astype(BF16)
        out_copy(half, q).start()

    def on_combine(zq, h, half, q):
        rows = strip(q)
        sib_copy(zq, half, q).wait_recv()

        @pl.when(zq == z)
        def _():
            finish(half, q)

        @pl.when(zq != z)
        def _():
            @pl.when(is_end(zq))
            def _():
                acc[zq, half, rows, :] = (
                    acc[zq, half, rows, :].astype(F32) + sib[zq, half, rows, :].astype(F32)
                ).astype(BF16)

            @pl.when(jnp.logical_not(is_end(zq)))
            def _():
                back_copy(zq, half, q, zq, up).wait_recv()
                acc[zq, half, rows, :] = (
                    acc[zq, half, rows, :].astype(F32)
                    + sib[zq, half, rows, :].astype(F32)
                    + back[zq, half, rows, :].astype(F32)
                ).astype(BF16)

            @pl.when(zq > z)
            def _():
                back_copy(zq, half, q, zq, up).start()

            @pl.when(zq < z - 1)
            def _():
                back_copy(zq, half, q, zq, down).start()

            @pl.when(zq == z - 1)
            def _():
                back_copy(zq, half, q, n_z, down).start()

    actions = (
        on_stream,
        on_land,
        on_z(0),
        on_z(1),
        on_across,
        on_hidden,
        on_result,
        on_combine,
    )
    order, _ = plan(n_z)
    groups = [-(-len(order[zz]) // 3) for zz in range(n_z)]
    tables = [encode(order[zz], 3 * max(groups)) for zz in range(n_z)]

    def of_zone(numbers):
        return sum((z == zz).astype(jnp.int32) * numbers[zz] for zz in range(n_z))

    def act_on(value):
        def turn(k, rest):
            mark = rest % BASE + 31
            q, half, h = mark % 2, mark // 2 % 2, mark // 4 % 2
            zq, kind = mark // 8 % 4, mark // 32
            for n, action in enumerate(actions):
                @pl.when(kind == n + 1)
                def _():
                    action(zq, h, half, q)

            return rest // BASE

        lax.fori_loop(0, 3, turn, value)

    span = 8
    values = [of_zone([table[g] for table in tables]) for g in range(max(groups))]
    values += [jnp.int32(0)] * (-len(values) % span)

    def among(k, options):
        return sum((k == n).astype(jnp.int32) * option for n, option in enumerate(options))

    count = of_zone(groups)

    @pl.loop(0, len(values) // span)
    def _(page):
        lines = [among(page, values[n::span]) for n in range(span)]

        def line(n, carry):
            act_on(among(n, lines))
            return carry

        lax.fori_loop(0, jnp.clip(count - page * span, 0, span), line, 0)

    @pl.when(has_next)
    def _():
        halo_copy().wait_send()

    fg_copy().wait_send()
    for r in range(n_chunks):
        sum_copy(r).wait_send()
        giv_copy(r).wait_send()
    for half in range(SPLIT):
        sh_copy(half).wait_send()

    for half in range(SPLIT):
        for q in range(2):
            out_copy(half, q).wait()

    def listed(source, target, half, q):
        inside = [(one > 0) & (one < n_z - 1) for one in (source, target)]
        to_end, from_end, both = [half * 2 + q in kind for kind in FULL]
        return (
            (jnp.logical_not(inside[1]) & to_end)
            | (inside[1] & jnp.logical_not(inside[0]) & from_end)
            | (inside[1] & inside[0] & both)
        )

    for half in range(SPLIT):
        for q in range(2):
            for way, there, target in ((0, hi, z + 1), (1, lo, z - 1)):

                @pl.when(there & listed(z, target, half, q))
                def _():
                    z_copy(way, z, 1, half, q).wait_send()

    @pl.loop(0, n_z)
    def _(zq):
        for way, there in ((0, hi & (zq <= z)), (1, lo & (zq >= z))):

            @pl.when(there)
            def _():
                for half in range(SPLIT):
                    m_copy(way, zq, c, half).wait_send()
                    for q in range(2):
                        z_copy(way, zq, 0, half, q).wait_send()

        near = (zq == z + 1) | (zq == z - 1)
        for half in range(SPLIT):
            m_copy(2, zq, c, half).wait_send()
            hid_copy(zq, half).wait_send()
            for q in range(2):
                sib_copy(zq, half, q).wait_send()
                for h in range(2):
                    c_copy(zq, h, half, q).wait_send()

                @pl.when(zq != z)
                def _():
                    back_copy(zq, half, q, zq, up).wait_send()

                @pl.when(jnp.logical_not(near & listed(zq, z, half, q)))
                def _():
                    x_copy(zq, half, q).wait_send()


def fast(
    out_gate,
    in_gate,
    conv_input,
    doc_ids,
    residual,
    conv_taps,
    mix_gain,
    out_weight,
    ffn_gain,
    routing,
    route_weight,
    expert_gate,
    expert_up,
    expert_down,
    shared_gate,
    shared_up,
    shared_down,
):
    tokens, cols = residual.shape
    chan, width = out_weight.shape
    n_tp, n_sp = lax.axis_size("tp"), lax.axis_size("sp")
    n_z = n_sp // 2
    rows = tokens // n_tp
    experts = n_sp * EXP_DEV
    most = max(1, 2 * rows * TOPK // experts)
    lanes = 128
    piece = rows // 2
    blocks = n_sp
    unit = expert_gate.shape[2]
    vm = pl.BlockSpec(memory_space=pltpu.VMEM)
    hbm = pl.BlockSpec(memory_space=pl.ANY)
    dma = pltpu.SemaphoreType.DMA
    return pl.pallas_call(
        functools.partial(layer_kernel, n_z, most),
        out_shape=jax.ShapeDtypeStruct((tokens, cols), BF16),
        in_specs=[hbm] * 5 + [vm] * 6 + [hbm] * 6,
        out_specs=hbm,
        scratch_shapes=[
            pltpu.VMEM((tokens, chan), BF16),
            pltpu.VMEM((tokens, chan), BF16),
            pltpu.VMEM((tokens, chan), BF16),
            pltpu.VMEM((tokens, cols), BF16),
            pltpu.VMEM((chan, width), BF16),
            pltpu.VMEM(expert_gate.shape, BF16),
            pltpu.VMEM(expert_up.shape, BF16),
            pltpu.VMEM(expert_down.shape, BF16),
            pltpu.VMEM(shared_gate.shape, BF16),
            pltpu.VMEM(shared_up.shape, BF16),
            pltpu.VMEM(shared_down.shape, BF16),
            pltpu.VMEM((tokens + 16, chan), F32),
            pltpu.VMEM((tokens + 16, lanes), F32),
            pltpu.VMEM((8, chan + lanes), F32),
            pltpu.VMEM((8, chan + lanes), F32),
            pltpu.VMEM((tokens, chan), BF16),
            pltpu.VMEM((tokens, lanes), F32),
            pltpu.VMEM((2, 2 * SPLIT, 8, lanes), F32),
            pltpu.VMEM((2 * SPLIT, piece, cols), BF16),
            pltpu.VMEM((2 * SPLIT, piece, cols), BF16),
            pltpu.VMEM((2, 1, cols), F32),
            pltpu.VMEM((rows, rows), BF16),
            pltpu.VMEM((blocks, SPLIT, 2, rows, cols), BF16),
            pltpu.VMEM((blocks, SPLIT, 8, rows + -rows % lanes), F32),
            pltpu.VMEM((EXP_DEV, 2 * most, width), BF16),
            pltpu.VMEM((2, n_z, SPLIT, EXP_DEV, 2 * most, unit), BF16),
            pltpu.VMEM((2, SPLIT, rows, unit), BF16),
            pltpu.VMEM((EXP_DEV, 2 * most, cols), BF16),
            pltpu.VMEM((n_z, SPLIT, rows, cols), BF16),
            pltpu.VMEM((n_z, SPLIT, rows, cols), BF16),
            pltpu.VMEM((n_z, SPLIT, rows, cols), BF16),
            pltpu.VMEM((n_z + 1, SPLIT, rows, cols), BF16),
            pltpu.VMEM((SPLIT, rows, cols), BF16),
            dma((11,)),
            dma((2,)),
            dma((4 * SPLIT,)),
            dma((2,)),
            dma((4 * SPLIT,)),
            dma((n_z + 3, SPLIT, 2)),
            dma((n_z, SPLIT, 2)),
            dma((n_z, 2, SPLIT, 2)),
            dma((n_z, 2, SPLIT, 2)),
            dma((n_z, SPLIT)),
            dma((2 * n_z + 1, SPLIT)),
            dma((blocks, SPLIT)),
            dma((n_z, SPLIT)),
            dma((n_z, SPLIT)),
            dma((SPLIT,)),
            dma((SPLIT,)),
            dma((n_z, SPLIT, 2)),
            dma((n_z, SPLIT, 2)),
            dma((n_z, SPLIT, 2)),
            dma((n_z + 1, SPLIT, 2)),
            dma((SPLIT, 2)),
        ],
        compiler_params=pltpu.CompilerParams(
            collective_id=0, has_side_effects=True, vmem_limit_bytes=64 * 1024 * 1024 - 65536
        ),
    )(
        out_gate,
        in_gate,
        conv_input,
        residual,
        out_weight,
        doc_ids.reshape(tokens // lanes, lanes),
        conv_taps,
        mix_gain[None, :],
        ffn_gain[None, :],
        routing.T,
        route_weight.T,
        expert_gate,
        expert_up,
        expert_down,
        shared_gate,
        shared_up,
        shared_down,
    )


def fits(mesh):
    return mesh.shape["tp"] == 2 and mesh.shape["sp"] in (4, 6, 8)


def solution(mesh):
    return jax.shard_map(
        fast if fits(mesh) else body,
        mesh=mesh,
        in_specs=(
            P(("grp", "sp"), "tp"),
            P(("grp", "sp"), "tp"),
            P(("grp", "sp"), "tp"),
            P(("grp", "sp")),
            P(("grp", "sp"), "tp"),
            P(None, "tp"),
            P("tp"),
            P("tp", None),
            P("tp"),
            P(("grp", "sp"), None),
            P(("grp", "sp"), None),
            P("sp", None, "tp"),
            P("sp", None, "tp"),
            P("sp", None, "tp"),
            P(None, "tp"),
            P(None, "tp"),
            P(None, "tp"),
        ),
        out_specs=P(("grp", "sp"), "tp"),
        check_vma=False,
    )
```

```python
import functools

import jax
import jax.numpy as jnp
from jax import lax
from jax.experimental import pallas as pl
from jax.experimental.pallas import tpu as pltpu
from jax.sharding import PartitionSpec as P

D_CONV = 1024
CONV_K = 3
TOPK = 2
EXP_DEV = 2


def from_behind(value, axis, steps):
    count = lax.axis_size(axis)
    first, last = (max(0, -steps), min(count, count - steps))
    return lax.ppermute(value, axis, [(source, source + steps) for source in range(first, last)])


def body(
    out_gate,
    in_gate,
    conv_input,
    doc_ids,
    residual,
    conv_taps,
    mix_gain,
    out_weight,
    ffn_gain,
    routing,
    route_weight,
    expert_gate,
    expert_up,
    expert_down,
    shared_gate,
    shared_up,
    shared_down,
):
    tokens = residual.shape[0]
    width = out_weight.shape[1]
    n_tp = lax.axis_size("tp")
    n_sp = lax.axis_size("sp")
    rows = tokens // n_tp
    experts = n_sp * EXP_DEV
    most = max(1, 2 * rows * TOPK // experts)
    slots = n_tp * most
    total = experts * slots
    cols = expert_down.shape[2]
    product = (in_gate.astype(jnp.float32) * conv_input.astype(jnp.float32)).astype(jnp.bfloat16)
    tail = (product[tokens - CONV_K + 1 :], doc_ids[tokens - CONV_K + 1 :].astype(jnp.bfloat16))
    prev_rows, prev_docs = from_behind((tail[0], tail[1]), "sp", 1)
    extended = jnp.concatenate([prev_rows, product], axis=0).astype(jnp.float32)
    ext_docs = jnp.concatenate([prev_docs.astype(jnp.int32), doc_ids])
    mixed = jnp.zeros(product.shape, jnp.float32)
    for k in range(CONV_K):
        keep = (ext_docs[k : k + tokens] == doc_ids)[:, None]
        mixed = mixed + jnp.where(keep, conv_taps[k] * extended[k : k + tokens], jnp.float32(0.0))
    conv_out = out_gate.astype(jnp.float32) * mixed
    squares = lax.psum(jnp.sum(conv_out * conv_out, axis=1), "tp")
    normed = (conv_out * lax.rsqrt(squares / D_CONV + 1e-06)[:, None] * mix_gain).astype(
        jnp.bfloat16
    )
    partial_value = jnp.dot(normed, out_weight, preferred_element_type=jnp.float32)
    proj = lax.psum_scatter(
        partial_value.astype(jnp.bfloat16), "tp", scatter_dimension=1, tiled=True
    ).astype(jnp.float32)
    stream = (residual.astype(jnp.float32) + proj).astype(jnp.bfloat16)
    stream32 = stream.astype(jnp.float32)
    stream_sq = lax.psum(jnp.sum(stream32 * stream32, axis=1), "tp")
    normal_cols = (stream32 * lax.rsqrt(stream_sq / width + 1e-06)[:, None] * ffn_gain).astype(
        jnp.bfloat16
    )
    flat_expert = routing.reshape(-1)
    onehot = (flat_expert[:, None] == jnp.arange(experts, dtype=jnp.int32)[None, :]).astype(
        jnp.int32
    )
    blocked = onehot.reshape(n_tp, rows * TOPK, experts)
    earlier = jnp.cumsum(blocked, axis=1) - blocked
    position = jnp.sum(earlier * blocked, axis=2).reshape(-1)
    entry = jnp.arange(tokens * TOPK, dtype=jnp.int32)
    slot = flat_expert * slots + entry // (rows * TOPK) * most + position
    table = jnp.full((total,), tokens, jnp.int32).at[slot].set(entry // TOPK)
    block_rows = lax.all_to_all(normal_cols, "tp", split_axis=0, concat_axis=1, tiled=True)
    mine = lax.dynamic_index_in_dim(
        table.reshape(n_sp, EXP_DEV, n_tp, most), lax.axis_index("tp"), 2, False
    )
    local = jnp.where(mine >= tokens, rows, mine - lax.axis_index("tp") * rows)
    padded_block = jnp.concatenate([block_rows, jnp.zeros((1, width), jnp.bfloat16)], axis=0)
    got = lax.all_to_all(padded_block[local], "sp", split_axis=0, concat_axis=0, tiled=True)
    arrived, whole = (
        lax.all_gather(got, "tp", axis=2, tiled=True),
        lax.all_gather(block_rows.reshape(1, 1, rows, width), "tp", axis=2, tiled=True),
    )
    normal = whole.reshape(tokens, width)
    gate = jnp.einsum("nesd,edh->nesh", arrived, expert_gate, preferred_element_type=jnp.float32)
    upper = jnp.einsum("nesd,edh->nesh", arrived, expert_up, preferred_element_type=jnp.float32)
    hidden = (jax.nn.silu(gate) * upper).astype(jnp.bfloat16)
    hidden_flat = hidden.reshape(n_sp * EXP_DEV * slots, hidden.shape[3])
    shared_hid = (
        jax.nn.silu(jnp.dot(normal, shared_gate, preferred_element_type=jnp.float32))
        * jnp.dot(normal, shared_up, preferred_element_type=jnp.float32)
    ).astype(jnp.bfloat16)
    expert_piece = lax.all_gather(hidden_flat, "tp", axis=1, tiled=True)
    shared_piece = lax.all_gather(shared_hid, "tp", axis=1, tiled=True)
    count = expert_piece.shape[1]
    expert_part = jnp.einsum(
        "nesh,ehd->nesd",
        expert_piece.reshape(n_sp, EXP_DEV, slots, count),
        expert_down,
        preferred_element_type=jnp.float32,
    )
    shared_part = jnp.dot(shared_piece, shared_down, preferred_element_type=jnp.float32)
    returned = lax.all_to_all(
        expert_part.astype(jnp.bfloat16), "sp", split_axis=0, concat_axis=0, tiled=True
    )
    picked = (
        returned.reshape(total, cols)[slot].astype(jnp.float32) * route_weight.reshape(-1)[:, None]
    )
    routed = jnp.sum(picked.reshape(tokens, TOPK, cols), axis=1)
    return (stream32 + shared_part + routed).astype(jnp.bfloat16)


MESH = pl.DeviceIdType.MESH
F32 = jnp.float32
BF16 = jnp.bfloat16


def silu_mul(gate, upper):
    return (gate / (1.0 + jnp.exp(-gate)) * upper).astype(BF16)


def mm(a, b):
    return jnp.dot(a, b, preferred_element_type=F32)


SPLIT = 2


GIVEN = (1, 0, 2, 3)
HOP, START, WIRE, NEAR = 2.8, 4.5, 4.18, (1.4, 2.5)
COST, EXTRA = (0.45, 0.15, 0.15, 0.15, 0.15, 1.65, 1.3, 0.22), (0.9, 0.3)
FULL = ((0, 2, 3), (0,), (1, 2, 3))
ROWX = (3.2, 7.8, -0.1, 7, 2.4, 1.9, -0.8, -4.5, -6.9, -1.3, -4.6, -1.2, -3.6, -2.7, -3.5, -1.3)
ROWZ = (5.3, -4.7, 3.6, 4.1, 6.5, 4, 5.6, -2.5, -3.8, 5.1, 3.9, -2.9, -5.3, 4.7, -3.6, 0.2)
ROWF = (-0.1, -5.8, 4.7, 4.9)
COMB = (5, -4.9, -3.1, 0.6, -2, -2.4, 5.5, -0.2, -1.5, -3.6, -4.8, 1.4, -0.4, 7.5, -2.3, -2.3)
WORK = (-3.4, 3.1, -3.1, 1.5, 1.1, -1.8, 5.4, -5.7, -0.1, 1.1, -4, 2.1, -4.3, 1.7, -0.5, 1)
RANK = (4, 0, 0, 0, 4)
DEPTH = (1, 2)
BASE = 257


KINDS = ("stream", "land", "up", "down", "across", "hidden", "result", "combine")


def inner(n_z, z):
    return int(0 < z < n_z - 1)


def full_rows(n_z, source, target, half, q):
    kind = inner(n_z, target) * (1 + inner(n_z, source))
    return abs(source - target) == 1 and half * 2 + q in FULL[kind]


def plan(n_z):
    chunks = [(half, q) for half in range(SPLIT) for q in range(2)]
    zones = range(n_z)
    never = 1e9
    have, told, heard, summed, went, final, arrive = {}, {}, {}, {}, {}, {}, {}
    todo = {z: [] for z in zones}
    for z in zones:
        for k, (half, q) in enumerate(chunks):
            todo[z].append(("stream", z, 0, half, q))
            went[z, half, q] = START + WIRE * (GIVEN.index(k) + 1) + HOP
        for zq in zones:
            for half, q in chunks:
                if zq != z:
                    todo[z].append(("land", zq, 0, half, q))
                todo[z].append(("land", zq, 1, half, q))
                if zq <= z < n_z - 1:
                    todo[z].append(("up", zq, 0, half, q))
                if zq >= z > 0:
                    todo[z].append(("down", zq, 0, half, q))
                if not full_rows(n_z, zq, z, half, q):
                    todo[z].append(("across", zq, 0, half, q))
                todo[z].append(("combine", zq, 0, half, q))
            for half in range(SPLIT):
                todo[z].append(("hidden", zq, 0, half, 0))
                todo[z].append(("result", zq, 0, half, 0))
        for half, q in chunks:
            if z < n_z - 1 and full_rows(n_z, z, z + 1, half, q):
                todo[z].append(("up", z, 1, half, q))
            if z > 0 and full_rows(n_z, z, z - 1, half, q):
                todo[z].append(("down", z, 1, half, q))
    link = {(z, way): 0.0 for z in zones for way in ("up", "down", "across")}
    for z in zones:
        link[z, "across"] = START + WIRE * len(chunks)
    core = {z: START for z in zones}

    def put(z, way, now, size):
        link[z, way] = max(now, link[z, way]) + WIRE * size
        return link[z, way] + HOP

    def ready(z, event):
        kind, zq, h, half, q = event
        if kind == "stream":
            return went[z, half, q]
        if kind == "land":
            return arrive.get((z, zq, h, half, q), never)
        if kind in ("up", "down", "across"):
            depth = DEPTH[kind == "across"]
            return max(have.get((z, zq, h, half, q), never), link[z, kind] - depth)
        if kind == "hidden":
            parts = [have.get((z, zq, g, half, p), never) for g in range(2) for p in range(2)]
            return max(parts) + NEAR[0]
        if kind == "result":
            return heard.get((z, zq, half), never)
        at = told.get((z, zq, half), never)
        if zq >= z and z > 0:
            at = max(at, summed.get((z - 1, zq, half, q), never))
        if zq <= z and z < n_z - 1:
            at = max(at, summed.get((z + 1, zq, half, q), never))
        if zq == z and q > 0:
            at = max(at, final.get((z, half, q - 1), never))
        return at

    def rank(z, event):
        kind, zq, h, half, q = event
        place = (inner(n_z, z) * 4 + abs(zq - z)) * 2 + half
        if kind in ("stream", "land"):
            return (RANK[0], 0.0, q)
        if kind == "combine":
            return (RANK[1], COMB[place], q)
        if kind == "result":
            return (RANK[2], WORK[place], q)
        if kind == "hidden":
            return (RANK[3], WORK[place], q)
        if kind == "across":
            return (RANK[4], ROWX[place], q)
        return (RANK[4], ROWZ[place] if h == 0 else ROWF[inner(n_z, z) * 2 + half], q)

    order = {z: [] for z in zones}
    while any(todo.values()):
        best = None
        for z in zones:
            if not todo[z]:
                continue
            starts = [(max(core[z], ready(z, event)), event) for event in todo[z]]
            at = min(start for start, _ in starts)
            if best is None or at < best[0]:
                best = (at, z, starts)
        at, z, starts = best
        assert at < never
        event = min((e for start, e in starts if start <= at), key=lambda e: rank(z, e))
        kind, zq, h, half, q = event
        todo[z].remove(event)
        order[z].append(event)
        end = at + COST[KINDS.index(kind)]
        if zq == z:
            end = end + (EXTRA[0] if kind == "hidden" else EXTRA[1] if kind == "combine" else 0.0)
        core[z] = end
        if kind in ("stream", "land"):
            have[z, zq, h, half, q] = end
        elif kind in ("up", "down"):
            arrive[z + (1 if kind == "up" else -1), zq, h, half, q] = put(z, kind, end, 1.0)
        elif kind == "across":
            arrive[z, zq, 1, half, q] = put(z, kind, end, 1.0)
        elif kind == "hidden":
            heard[z, zq, half] = put(z, "across", end, 1.0 if zq == z else 0.5)
        elif kind == "result":
            told[z, zq, half] = end + NEAR[1]
        elif zq == z:
            final[z, half, q] = end
        else:
            summed[z, zq, half, q] = put(z, "up" if zq > z else "down", end, 1.0)
    return order, max(final.values())


def encode(events, slots):
    codes = [
        (((KINDS.index(kind) * 4 + zq) * 2 + h) * 2 + half) * 2 + q + 1
        for kind, zq, h, half, q in events
    ]
    codes += [0] * (slots - len(codes))
    return [sum(codes[at + k] * BASE**k for k in range(3)) for at in range(0, slots, 3)]


def layer_kernel(
    n_z,
    most,
    og_hbm,
    ig_hbm,
    ci_hbm,
    res_hbm,
    wo_hbm,
    docs_ref,
    taps_ref,
    mix_ref,
    ffn_ref,
    names_ref,
    share_ref,
    wg_hbm,
    wu_hbm,
    wd_hbm,
    sg_hbm,
    su_hbm,
    sd_hbm,
    out_hbm,
    og,
    ig,
    ci,
    res,
    wo,
    wg,
    wu,
    wd,
    sg,
    su,
    sd,
    ext,
    dext,
    hsend,
    hrecv,
    act,
    ssq,
    srow,
    gsend,
    grecv,
    fg,
    tri,
    blk,
    meta,
    xs,
    hid,
    shid,
    ys,
    acc,
    outgo,
    sib,
    back,
    done,
    load_sem,
    halo_sem,
    sum_sem,
    fg_sem,
    giv_recv,
    z_send,
    x_send,
    c_send,
    b_recv,
    s_recv,
    m_send,
    m_recv,
    hid_send,
    hid_recv,
    sh_send,
    sh_recv,
    sib_send,
    sib_recv,
    back_send,
    back_recv,
    out_sem,
):
    first = [
        pltpu.make_async_copy(src, dst, load_sem.at[n])
        for n, (src, dst) in enumerate(
            ((ig_hbm, ig), (ci_hbm, ci), (og_hbm, og), (wo_hbm, wo), (res_hbm, res))
        )
    ]
    later = [
        pltpu.make_async_copy(src, dst, load_sem.at[5 + n])
        for n, (src, dst) in enumerate(
            ((wg_hbm, wg), (wu_hbm, wu), (wd_hbm, wd), (sg_hbm, sg), (su_hbm, su), (sd_hbm, sd))
        )
    ]
    for load in first:
        load.start()
    s = lax.axis_index("sp")
    t = lax.axis_index("tp")
    z = s // 2
    c = s % 2
    tokens, chan = ig.shape
    cols = res.shape[1]
    width = 2 * cols
    half_rows = tokens // SPLIT
    n_chunks = 2 * SPLIT
    piece = half_rows // 2
    unit = wg.shape[2]
    pad = ext.shape[0] - tokens
    lo = z > 0
    hi = z < n_z - 1
    up, down = {"sp": s + 2}, {"sp": s - 2}
    other, peer = {"sp": s + 1 - 2 * c}, {"tp": 1 - t}
    after = {"sp": s + 1}
    before = {"sp": s - 1}
    targets = (up, down, peer, other)

    def remote(src, dst, ssem, rsem, dev):
        return pltpu.make_async_remote_copy(
            src_ref=src,
            dst_ref=dst,
            send_sem=ssem,
            recv_sem=rsem,
            device_id=dev,
            device_id_type=MESH,
        )

    def chunk(zq, h, half, q, ssem, rsem, dev):
        ref = blk.at[zq * 2 + c, half, h, pl.ds(q * piece, piece)]
        return remote(ref, ref, ssem, rsem, dev)

    def side(h):
        return t + h * (1 - 2 * t)

    def z_copy(way, zq, h, half, q):
        ssem = z_send.at[way, zq + h * (n_z - zq + half * 2 + q)]
        return chunk(
            zq, side(h), half, q, ssem, b_recv.at[zq, side(h), half, q], targets[way]
        )

    def z_sent(way, zq):
        ref = blk.at[0]
        return remote(ref.at[0], ref.at[0], z_send.at[way, zq], b_recv.at[0, 0, 0, 0], targets[way])

    def x_copy(zq, half, q):
        return chunk(zq, t, half, q, x_send.at[zq, half, q], b_recv.at[zq, t, half, q], peer)

    def c_copy(zq, h, half, q):
        return chunk(zq, h, half, q, c_send.at[0], s_recv.at[zq, half], other)

    def c_all():
        ref = blk.at[pl.ds(0, n_z)]
        return remote(ref, ref, c_send.at[0], s_recv.at[0, 0], other)

    def near_by(zq, half):
        ref = blk.at[zq * 2 + 1 - c, half]
        return remote(ref, ref, c_send.at[0], s_recv.at[zq, half], other)

    def arrived(zq, h, half, q):
        chunk(zq, h, half, q, c_send.at[0], b_recv.at[zq, h, half, q], other).wait_recv()

    def m_copy(way, zq, cq, half):
        ref = meta.at[zq * 2 + cq, half]
        ssem = m_send.at[way * n_z + zq * (way < 2)]
        return remote(ref, ref, ssem, m_recv.at[zq * 2 + cq, half], (up, down, other)[way])

    def m_sent(way, zq):
        ref = meta.at[0] if way < 2 else meta.at[pl.ds(0, n_z)]
        return remote(
            ref, ref, m_send.at[way * n_z + zq], m_recv.at[0, 0], (up, down, other)[way]
        )

    def hid_copy(zq, half):
        return remote(
            hid.at[t, zq, half],
            hid.at[t, zq, half],
            hid_send.at[0],
            hid_recv.at[zq, half],
            peer,
        )

    def sh_copy(half):
        return remote(
            shid.at[t, half], shid.at[t, half], sh_send.at[half], sh_recv.at[half], peer
        )

    def sib_copy(zq, half, q):
        rows = pl.ds(q * piece, piece)
        return remote(
            outgo.at[zq, half, rows],
            sib.at[zq, half, rows],
            sib_send.at[0],
            sib_recv.at[zq, half, q],
            other,
        )

    def back_copy(zq, half, q, to, dev):
        return remote(
            acc.at[zq, half, pl.ds(q * piece, piece)],
            back.at[to, half, pl.ds(q * piece, piece)],
            back_send.at[0],
            back_recv.at[to, half, q],
            dev,
        )

    def halo_copy():
        return remote(hsend, hrecv, halo_sem.at[0], halo_sem.at[1], after)

    def sum_copy(r):
        return remote(srow.at[0, r], srow.at[1, r], sum_sem.at[n_chunks], sum_sem.at[r], peer)

    def fg_copy():
        return remote(fg.at[t], fg.at[t], fg_sem.at[0], fg_sem.at[1], peer)

    def giv_copy(r):
        return remote(gsend.at[r], grecv.at[r], giv_recv.at[n_chunks], giv_recv.at[r], peer)

    barrier = pltpu.get_barrier_semaphore()
    cross_up = hi & (c == 1)
    cross_down = lo & (c == 0)
    for target, there in ((up, hi), (down, lo), (after, cross_up), (before, cross_down)):

        @pl.when(there)
        def _():
            pl.semaphore_signal(barrier, inc=1, device_id=target, device_id_type=MESH)

    for target in (peer, other):
        pl.semaphore_signal(barrier, inc=1, device_id=target, device_id_type=MESH)

    has_next = s < 2 * n_z - 1
    has_prev = s > 0
    first[0].wait()
    first[1].wait()

    tail = 16

    def product(rows):
        return (ig[rows, :].astype(F32) * ci[rows, :].astype(F32)).astype(BF16).astype(F32)

    lanes = dext.shape[1]
    eye = lax.broadcasted_iota(jnp.int32, (lanes, lanes), 0) == lax.broadcasted_iota(
        jnp.int32, (lanes, lanes), 1
    )

    def upright(line):
        return jnp.sum(jnp.where(eye, line, F32(0.0)), axis=1, keepdims=True)

    docs = docs_ref[...].astype(F32)
    for k in range(tokens // lanes):
        column = upright(docs[k : k + 1, :])
        dext[pad + k * lanes : pad + (k + 1) * lanes, :] = jnp.broadcast_to(column, (lanes, lanes))
    end_rows = product(pl.ds(tokens - tail, tail))
    hsend[:, :chan] = end_rows[tail - 8 :]
    hsend[:, chan:] = dext[pad + tokens - 8 : pad + tokens, :]
    own = z * 2 + c
    names = names_ref[...].astype(F32)
    share = share_ref[...]
    for half in range(SPLIT):
        part = slice(half * half_rows, (half + 1) * half_rows)
        meta[own, half] = jnp.zeros(meta.shape[2:], F32)
        meta[own, half, 0:TOPK, :half_rows] = names[:, part]
        meta[own, half, TOPK : 2 * TOPK, :half_rows] = share[:, part]
    fg[t] = ffn_ref[...]
    step_rows = 32

    @pl.loop(0, tokens // step_rows)
    def _(i):
        at = pl.multiple_of(i * step_rows, step_rows)
        ext[pl.ds(pad + at, step_rows), :] = product(pl.ds(at, step_rows))

    n_tri = tri.shape[0]
    row_id = lax.broadcasted_iota(jnp.int32, (n_tri, n_tri), 0)
    col_id = lax.broadcasted_iota(jnp.int32, (n_tri, n_tri), 1)
    tri[...] = (row_id < col_id).astype(F32).astype(BF16)

    def convolve(r):
        @pl.loop(0, piece // step_rows)
        def _(i):
            at = pl.multiple_of(r * piece + i * step_rows, step_rows)
            v = ext[pl.ds(pl.multiple_of(pad - 8 + at, 8), step_rows + 8), :]
            d = dext[pl.ds(pl.multiple_of(pad - 8 + at, 8), step_rows + 8), :]
            doc = d[8:]
            mixed = None
            for k in range(CONV_K):
                by = CONV_K - 1 - k
                if by:
                    same = (pltpu.roll(d, by, 0)[8:] == doc).astype(F32)
                    same = jnp.concatenate([same] * (chan // lanes), axis=1)
                    term = taps_ref[k : k + 1, :] * pltpu.roll(v, by, 0)[8:] * same
                else:
                    term = taps_ref[k : k + 1, :] * v[8:]
                mixed = term if mixed is None else mixed + term
            rows = pl.ds(at, step_rows)
            conv_out = og[rows, :].astype(F32) * mixed
            total = jnp.sum(conv_out * conv_out, axis=1, keepdims=True)
            ssq[rows, :] = jnp.broadcast_to(total, (step_rows, lanes))
            act[rows, :] = (conv_out * mix_ref[...]).astype(BF16)

    eye_piece = lax.broadcasted_iota(jnp.int32, (piece, lanes), 0) == lax.broadcasted_iota(
        jnp.int32, (piece, lanes), 1
    )

    def out_cols(who):
        return pl.ds(pl.multiple_of(who * cols, cols), cols)

    def sums(r):
        part = ssq[r * piece : (r + 1) * piece, :]
        line = jnp.sum(jnp.where(eye_piece, part, F32(0.0)), axis=0, keepdims=True)
        srow[0, r] = jnp.broadcast_to(line, srow.shape[2:])

    def give(r):
        gsend[r] = mm(act[r * piece : (r + 1) * piece, :], wo[:, out_cols(1 - t)]).astype(BF16)

    def send_given(r):
        sum_copy(r).start()
        giv_copy(r).start()

    first[2].wait()
    for r in GIVEN:
        if r:
            convolve(r)
            sums(r)
    first[3].wait()
    give(GIVEN[0])
    first[4].wait()
    arrivals = (
        2
        + lo.astype(jnp.int32)
        + hi.astype(jnp.int32)
        + cross_up.astype(jnp.int32)
        + cross_down.astype(jnp.int32)
    )
    pl.semaphore_wait(barrier, arrivals)

    @pl.when(has_next)
    def _():
        halo_copy().start()

    fg_copy().start()
    send_given(GIVEN[0])
    for half in range(SPLIT):
        m_copy(2, z, c, half).start()

    @pl.when(has_prev)
    def _():
        halo_copy().wait_recv()
        ext[pad - 8 : pad, :] = hrecv[:, :chan]
        dext[pad - 8 : pad, :] = hrecv[:, chan:]

    @pl.when(jnp.logical_not(has_prev))
    def _():
        ext[pad - 8 : pad, :] = jnp.zeros((8, chan), F32)
        dext[pad - 8 : pad, :] = jnp.zeros((8, lanes), F32)

    convolve(0)
    sums(0)
    for r in GIVEN[1:]:
        give(r)
        send_given(r)
    fg_copy().wait_recv()

    def picks(zq, cq, half):
        info = meta[zq * 2 + cq, half][:, :half_rows]
        mine = (lax.broadcasted_iota(jnp.int32, (8, half_rows), 0) + s * EXP_DEV).astype(F32)
        hot0 = info[0:1] == mine
        hot1 = info[1:2] == mine
        hot = hot0 | hot1
        earlier = mm(hot.astype(F32).astype(BF16), tri[...])
        position = jnp.where(hot, earlier, F32(-1.0))
        weight = jnp.where(hot0, info[2:3], F32(0.0)) + jnp.where(hot1, info[3:4], F32(0.0))
        place = lax.broadcasted_iota(jnp.int32, (most, half_rows), 0).astype(F32)
        chosen = [(position[e : e + 1] == place).astype(F32) for e in range(EXP_DEV)]
        return chosen, weight

    def norm_scale(parts):
        total = sum(jnp.sum(part * part, axis=1, keepdims=True) for part in parts)
        return lax.rsqrt(total / width + 1e-06)

    def normal_of(parts):
        scale = norm_scale(parts)
        return [(part * scale * fg[h, 0:1, :]).astype(BF16) for h, part in enumerate(parts)]

    def sides():
        return [(0, c), (1, 1 - c)]

    def hidden(zq, half):
        for p, cq in sides():
            chosen, _ = picks(zq, cq, half)
            sel = jnp.concatenate(chosen, axis=0).astype(BF16)
            got = normal_of([mm(sel, blk[zq * 2 + cq, half, h]) for h in range(2)])
            for h in range(2):
                for e in range(EXP_DEV):
                    xs[e, p * most : (p + 1) * most, h * cols : (h + 1) * cols] = got[h][
                        e * most : (e + 1) * most
                    ]
        for e in range(EXP_DEV):
            hid[t, zq, half, e] = silu_mul(mm(xs[e], wg[e]), mm(xs[e], wu[e]))

    def shared(half):
        whole = normal_of([blk[z * 2 + c, half, h].astype(F32) for h in range(2)])
        gate = mm(whole[0], sg[:cols, :]) + mm(whole[1], sg[cols:, :])
        upper = mm(whole[0], su[:cols, :]) + mm(whole[1], su[cols:, :])
        shid[t, half] = silu_mul(gate, upper)

    def results(zq, half):
        hid_copy(zq, half).wait_recv()
        for e in range(EXP_DEV):
            ys[e] = (
                mm(hid[0, zq, half, e], wd[e, :unit, :]) + mm(hid[1, zq, half, e], wd[e, unit:, :])
            ).astype(BF16)
        for p, cq in sides():
            chosen, weight = picks(zq, cq, half)
            parts = []
            for e in range(EXP_DEV):
                scale = jnp.sum(chosen[e] * weight[e : e + 1], axis=1, keepdims=True)
                part = ys[e, p * most : (p + 1) * most, :].astype(F32)
                parts.append((part * scale).astype(BF16))
            sel = jnp.concatenate(chosen, axis=0).astype(BF16)
            into = acc if p == 0 else outgo
            into[zq, half] = lax.dot_general(
                sel,
                jnp.concatenate(parts, axis=0),
                (((0,), (0,)), ((), ())),
                preferred_element_type=F32,
            ).astype(BF16)
        for q in range(2):
            sib_copy(zq, half, q).start()

    def is_end(zq):
        return ((zq > z) & jnp.logical_not(lo)) | ((zq < z) & jnp.logical_not(hi))

    def strip(q):
        return pl.ds(pl.multiple_of(q * piece, piece), piece)

    def on_stream(zq, h, half, q):
        r = half * 2 + q
        rows = pl.ds(pl.multiple_of(r * piece, piece), piece)
        kept = mm(act[rows, :], wo[:, out_cols(t)])
        sum_copy(r).wait_recv()
        line = srow[1, r, 0:1, :]
        theirs = jnp.sum(jnp.where(eye_piece, line, F32(0.0)), axis=1, keepdims=True)
        scale = lax.rsqrt((ssq[rows, 0:1] + theirs) / (2 * chan) + 1e-06)
        giv_copy(r).wait_recv()
        proj = (kept + grecv[r].astype(F32)) * scale
        blk[z * 2 + c, half, t, strip(q), :] = (res[rows, :].astype(F32) + proj).astype(BF16)
        c_copy(z, t, half, q).start()

        @pl.when(r == GIVEN[0])
        def _():
            for load in later:
                load.start()

        @pl.when(r == GIVEN[-1])
        def _():
            for load in later:
                load.wait()

    def on_land(zq, h, half, q):
        @pl.when((h == 0) & (q == 0))
        def _():
            m_copy(2, zq, c, half).wait_recv()
            m_copy(2, zq, c, half).start()

        arrived(zq, side(h), half, q)
        c_copy(zq, side(h), half, q).start()

    def on_z(way):
        def send(zq, h, half, q):
            @pl.when((h == 0) & (q == 0))
            def _():
                m_copy(way, zq, c, half).start()

            z_copy(way, zq, h, half, q).start()

        return send

    def on_across(zq, h, half, q):
        x_copy(zq, half, q).start()

    def on_hidden(zq, h, half, q):
        m_copy(2, zq, 1 - c, half).wait_recv()
        near_by(zq, half).wait_recv()
        hidden(zq, half)
        hid_copy(zq, half).start()

        @pl.when(zq == z)
        def _():
            shared(half)
            sh_copy(half).start()

    def on_result(zq, h, half, q):
        results(zq, half)

    def out_copy(half, q):
        return pltpu.make_async_copy(
            done.at[half, pl.ds(q * piece, piece)],
            out_hbm.at[pl.ds(half * half_rows + q * piece, piece)],
            out_sem.at[half, q],
        )

    def finish(half, q):
        rows = strip(q)

        @pl.when(q == 0)
        def _():
            sh_copy(half).wait_recv()

        fin = (
            blk[z * 2 + c, half, t, rows, :].astype(F32)
            + mm(shid[0, half, rows, :], sd[:unit, :])
            + mm(shid[1, half, rows, :], sd[unit:, :])
            + acc[z, half, rows, :].astype(F32)
            + sib[z, half, rows, :].astype(F32)
        )

        @pl.when(lo)
        def _():
            back_copy(z, half, q, z, up).wait_recv()

        @pl.when(hi)
        def _():
            back_copy(z, half, q, n_z, up).wait_recv()

        low = jnp.where(lo, back[z, half, rows, :].astype(F32), F32(0.0))
        high = jnp.where(hi, back[n_z, half, rows, :].astype(F32), F32(0.0))
        done[half, rows, :] = (fin + low + high).astype(BF16)
        out_copy(half, q).start()

    def on_combine(zq, h, half, q):
        rows = strip(q)
        sib_copy(zq, half, q).wait_recv()

        @pl.when(zq == z)
        def _():
            finish(half, q)

        @pl.when(zq != z)
        def _():
            @pl.when(is_end(zq))
            def _():
                acc[zq, half, rows, :] = (
                    acc[zq, half, rows, :].astype(F32) + sib[zq, half, rows, :].astype(F32)
                ).astype(BF16)

            @pl.when(jnp.logical_not(is_end(zq)))
            def _():
                back_copy(zq, half, q, zq, up).wait_recv()
                acc[zq, half, rows, :] = (
                    acc[zq, half, rows, :].astype(F32)
                    + sib[zq, half, rows, :].astype(F32)
                    + back[zq, half, rows, :].astype(F32)
                ).astype(BF16)

            @pl.when(zq > z)
            def _():
                back_copy(zq, half, q, zq, up).start()

            @pl.when(zq < z - 1)
            def _():
                back_copy(zq, half, q, zq, down).start()

            @pl.when(zq == z - 1)
            def _():
                back_copy(zq, half, q, n_z, down).start()

    actions = (
        on_stream,
        on_land,
        on_z(0),
        on_z(1),
        on_across,
        on_hidden,
        on_result,
        on_combine,
    )
    order, _ = plan(n_z)
    groups = [-(-len(order[zz]) // 3) for zz in range(n_z)]
    tables = [encode(order[zz], 3 * max(groups)) for zz in range(n_z)]

    def of_zone(numbers):
        return sum((z == zz).astype(jnp.int32) * numbers[zz] for zz in range(n_z))

    def act_on(value):
        def turn(k, rest):
            mark = rest % BASE + 31
            q, half, h = mark % 2, mark // 2 % 2, mark // 4 % 2
            zq, kind = mark // 8 % 4, mark // 32
            for n, action in enumerate(actions):
                @pl.when(kind == n + 1)
                def _():
                    action(zq, h, half, q)

            return rest // BASE

        lax.fori_loop(0, 3, turn, value)

    span = 8
    values = [of_zone([table[g] for table in tables]) for g in range(max(groups))]
    values += [jnp.int32(0)] * (-len(values) % span)

    def among(k, options):
        return sum((k == n).astype(jnp.int32) * option for n, option in enumerate(options))

    count = of_zone(groups)

    @pl.loop(0, len(values) // span)
    def _(page):
        lines = [among(page, values[n::span]) for n in range(span)]

        def line(n, carry):
            act_on(among(n, lines))
            return carry

        lax.fori_loop(0, jnp.clip(count - page * span, 0, span), line, 0)

    @pl.when(has_next)
    def _():
        halo_copy().wait_send()

    fg_copy().wait_send()
    remote(srow.at[0], srow.at[0], sum_sem.at[n_chunks], sum_sem.at[0], peer).wait_send()
    remote(gsend, gsend, giv_recv.at[n_chunks], giv_recv.at[0], peer).wait_send()
    for half in range(SPLIT):
        sh_copy(half).wait_send()
    c_all().wait_send()
    m_sent(2, 0).wait_send()
    remote(hid.at[t], hid.at[t], hid_send.at[0], hid_recv.at[0, 0], peer).wait_send()
    remote(outgo, outgo, sib_send.at[0], sib_recv.at[0, 0, 0], other).wait_send()
    sent = acc.at[pl.ds(0, n_z - 1)]
    remote(sent, sent, back_send.at[0], back_recv.at[0, 0, 0], up).wait_send()

    for half in range(SPLIT):
        for q in range(2):
            out_copy(half, q).wait()

    def listed(source, target, half, q):
        inside = [(one > 0) & (one < n_z - 1) for one in (source, target)]
        to_end, from_end, both = [half * 2 + q in kind for kind in FULL]
        return (
            (jnp.logical_not(inside[1]) & to_end)
            | (inside[1] & jnp.logical_not(inside[0]) & from_end)
            | (inside[1] & inside[0] & both)
        )

    for half in range(SPLIT):
        for q in range(2):
            for way, there, target in ((0, hi, z + 1), (1, lo, z - 1)):

                @pl.when(there & listed(z, target, half, q))
                def _():
                    z_copy(way, z, 1, half, q).wait_send()

    @pl.loop(0, n_z)
    def _(zq):
        for way, there in ((0, hi & (zq <= z)), (1, lo & (zq >= z))):

            @pl.when(there)
            def _():
                m_sent(way, zq).wait_send()
                z_sent(way, zq).wait_send()

        near = (zq == z + 1) | (zq == z - 1)
        for half in range(SPLIT):
            for q in range(2):

                @pl.when(jnp.logical_not(near & listed(zq, z, half, q)))
                def _():
                    x_copy(zq, half, q).wait_send()


def fast(
    out_gate,
    in_gate,
    conv_input,
    doc_ids,
    residual,
    conv_taps,
    mix_gain,
    out_weight,
    ffn_gain,
    routing,
    route_weight,
    expert_gate,
    expert_up,
    expert_down,
    shared_gate,
    shared_up,
    shared_down,
):
    tokens, cols = residual.shape
    chan, width = out_weight.shape
    n_tp, n_sp = lax.axis_size("tp"), lax.axis_size("sp")
    n_z = n_sp // 2
    rows = tokens // n_tp
    experts = n_sp * EXP_DEV
    most = max(1, 2 * rows * TOPK // experts)
    lanes = 128
    piece = rows // 2
    blocks = n_sp
    unit = expert_gate.shape[2]
    vm = pl.BlockSpec(memory_space=pltpu.VMEM)
    hbm = pl.BlockSpec(memory_space=pl.ANY)
    dma = pltpu.SemaphoreType.DMA
    return pl.pallas_call(
        functools.partial(layer_kernel, n_z, most),
        out_shape=jax.ShapeDtypeStruct((tokens, cols), BF16),
        in_specs=[hbm] * 5 + [vm] * 6 + [hbm] * 6,
        out_specs=hbm,
        scratch_shapes=[
            pltpu.VMEM((tokens, chan), BF16),
            pltpu.VMEM((tokens, chan), BF16),
            pltpu.VMEM((tokens, chan), BF16),
            pltpu.VMEM((tokens, cols), BF16),
            pltpu.VMEM((chan, width), BF16),
            pltpu.VMEM(expert_gate.shape, BF16),
            pltpu.VMEM(expert_up.shape, BF16),
            pltpu.VMEM(expert_down.shape, BF16),
            pltpu.VMEM(shared_gate.shape, BF16),
            pltpu.VMEM(shared_up.shape, BF16),
            pltpu.VMEM(shared_down.shape, BF16),
            pltpu.VMEM((tokens + 16, chan), F32),
            pltpu.VMEM((tokens + 16, lanes), F32),
            pltpu.VMEM((8, chan + lanes), F32),
            pltpu.VMEM((8, chan + lanes), F32),
            pltpu.VMEM((tokens, chan), BF16),
            pltpu.VMEM((tokens, lanes), F32),
            pltpu.VMEM((2, 2 * SPLIT, 8, lanes), F32),
            pltpu.VMEM((2 * SPLIT, piece, cols), BF16),
            pltpu.VMEM((2 * SPLIT, piece, cols), BF16),
            pltpu.VMEM((2, 1, cols), F32),
            pltpu.VMEM((rows, rows), BF16),
            pltpu.VMEM((blocks, SPLIT, 2, rows, cols), BF16),
            pltpu.VMEM((blocks, SPLIT, 8, rows + -rows % lanes), F32),
            pltpu.VMEM((EXP_DEV, 2 * most, width), BF16),
            pltpu.VMEM((2, n_z, SPLIT, EXP_DEV, 2 * most, unit), BF16),
            pltpu.VMEM((2, SPLIT, rows, unit), BF16),
            pltpu.VMEM((EXP_DEV, 2 * most, cols), BF16),
            pltpu.VMEM((n_z, SPLIT, rows, cols), BF16),
            pltpu.VMEM((n_z, SPLIT, rows, cols), BF16),
            pltpu.VMEM((n_z, SPLIT, rows, cols), BF16),
            pltpu.VMEM((n_z + 1, SPLIT, rows, cols), BF16),
            pltpu.VMEM((SPLIT, rows, cols), BF16),
            dma((11,)),
            dma((2,)),
            dma((2 * SPLIT + 1,)),
            dma((2,)),
            dma((2 * SPLIT + 1,)),
            dma((2, n_z + 2 * SPLIT)),
            dma((n_z, SPLIT, 2)),
            dma((1,)),
            dma((n_z, 2, SPLIT, 2)),
            dma((n_z, SPLIT)),
            dma((2 * n_z + 1,)),
            dma((blocks, SPLIT)),
            dma((1,)),
            dma((n_z, SPLIT)),
            dma((SPLIT,)),
            dma((SPLIT,)),
            dma((1,)),
            dma((n_z, SPLIT, 2)),
            dma((1,)),
            dma((n_z + 1, SPLIT, 2)),
            dma((SPLIT, 2)),
        ],
        compiler_params=pltpu.CompilerParams(
            collective_id=0, has_side_effects=True, vmem_limit_bytes=64 * 1024 * 1024 - 65536
        ),
    )(
        out_gate,
        in_gate,
        conv_input,
        residual,
        out_weight,
        doc_ids.reshape(tokens // lanes, lanes),
        conv_taps,
        mix_gain[None, :],
        ffn_gain[None, :],
        routing.T,
        route_weight.T,
        expert_gate,
        expert_up,
        expert_down,
        shared_gate,
        shared_up,
        shared_down,
    )


def fits(mesh):
    return mesh.shape["tp"] == 2 and mesh.shape["sp"] in (4, 6, 8)


def solution(mesh):
    return jax.shard_map(
        fast if fits(mesh) else body,
        mesh=mesh,
        in_specs=(
            P(("grp", "sp"), "tp"),
            P(("grp", "sp"), "tp"),
            P(("grp", "sp"), "tp"),
            P(("grp", "sp")),
            P(("grp", "sp"), "tp"),
            P(None, "tp"),
            P("tp"),
            P("tp", None),
            P("tp"),
            P(("grp", "sp"), None),
            P(("grp", "sp"), None),
            P("sp", None, "tp"),
            P("sp", None, "tp"),
            P("sp", None, "tp"),
            P(None, "tp"),
            P(None, "tp"),
            P(None, "tp"),
        ),
        out_specs=P(("grp", "sp"), "tp"),
        check_vma=False,
    )
```

```python
import functools

import jax
import jax.numpy as jnp
from jax import lax
from jax.experimental import pallas as pl
from jax.experimental.pallas import tpu as pltpu
from jax.sharding import PartitionSpec as P

D_CONV = 1024
CONV_K = 3
TOPK = 2
EXP_DEV = 2


def from_behind(value, axis, steps):
    count = lax.axis_size(axis)
    first, last = (max(0, -steps), min(count, count - steps))
    return lax.ppermute(value, axis, [(source, source + steps) for source in range(first, last)])


def body(
    out_gate,
    in_gate,
    conv_input,
    doc_ids,
    residual,
    conv_taps,
    mix_gain,
    out_weight,
    ffn_gain,
    routing,
    route_weight,
    expert_gate,
    expert_up,
    expert_down,
    shared_gate,
    shared_up,
    shared_down,
):
    tokens = residual.shape[0]
    width = out_weight.shape[1]
    n_tp = lax.axis_size("tp")
    n_sp = lax.axis_size("sp")
    rows = tokens // n_tp
    experts = n_sp * EXP_DEV
    most = max(1, 2 * rows * TOPK // experts)
    slots = n_tp * most
    total = experts * slots
    cols = expert_down.shape[2]
    product = (in_gate.astype(jnp.float32) * conv_input.astype(jnp.float32)).astype(jnp.bfloat16)
    tail = (product[tokens - CONV_K + 1 :], doc_ids[tokens - CONV_K + 1 :].astype(jnp.bfloat16))
    prev_rows, prev_docs = from_behind((tail[0], tail[1]), "sp", 1)
    extended = jnp.concatenate([prev_rows, product], axis=0).astype(jnp.float32)
    ext_docs = jnp.concatenate([prev_docs.astype(jnp.int32), doc_ids])
    mixed = jnp.zeros(product.shape, jnp.float32)
    for k in range(CONV_K):
        keep = (ext_docs[k : k + tokens] == doc_ids)[:, None]
        mixed = mixed + jnp.where(keep, conv_taps[k] * extended[k : k + tokens], jnp.float32(0.0))
    conv_out = out_gate.astype(jnp.float32) * mixed
    squares = lax.psum(jnp.sum(conv_out * conv_out, axis=1), "tp")
    normed = (conv_out * lax.rsqrt(squares / D_CONV + 1e-06)[:, None] * mix_gain).astype(
        jnp.bfloat16
    )
    partial_value = jnp.dot(normed, out_weight, preferred_element_type=jnp.float32)
    proj = lax.psum_scatter(
        partial_value.astype(jnp.bfloat16), "tp", scatter_dimension=1, tiled=True
    ).astype(jnp.float32)
    stream = (residual.astype(jnp.float32) + proj).astype(jnp.bfloat16)
    stream32 = stream.astype(jnp.float32)
    stream_sq = lax.psum(jnp.sum(stream32 * stream32, axis=1), "tp")
    normal_cols = (stream32 * lax.rsqrt(stream_sq / width + 1e-06)[:, None] * ffn_gain).astype(
        jnp.bfloat16
    )
    flat_expert = routing.reshape(-1)
    onehot = (flat_expert[:, None] == jnp.arange(experts, dtype=jnp.int32)[None, :]).astype(
        jnp.int32
    )
    blocked = onehot.reshape(n_tp, rows * TOPK, experts)
    earlier = jnp.cumsum(blocked, axis=1) - blocked
    position = jnp.sum(earlier * blocked, axis=2).reshape(-1)
    entry = jnp.arange(tokens * TOPK, dtype=jnp.int32)
    slot = flat_expert * slots + entry // (rows * TOPK) * most + position
    table = jnp.full((total,), tokens, jnp.int32).at[slot].set(entry // TOPK)
    block_rows = lax.all_to_all(normal_cols, "tp", split_axis=0, concat_axis=1, tiled=True)
    mine = lax.dynamic_index_in_dim(
        table.reshape(n_sp, EXP_DEV, n_tp, most), lax.axis_index("tp"), 2, False
    )
    local = jnp.where(mine >= tokens, rows, mine - lax.axis_index("tp") * rows)
    padded_block = jnp.concatenate([block_rows, jnp.zeros((1, width), jnp.bfloat16)], axis=0)
    got = lax.all_to_all(padded_block[local], "sp", split_axis=0, concat_axis=0, tiled=True)
    arrived, whole = (
        lax.all_gather(got, "tp", axis=2, tiled=True),
        lax.all_gather(block_rows.reshape(1, 1, rows, width), "tp", axis=2, tiled=True),
    )
    normal = whole.reshape(tokens, width)
    gate = jnp.einsum("nesd,edh->nesh", arrived, expert_gate, preferred_element_type=jnp.float32)
    upper = jnp.einsum("nesd,edh->nesh", arrived, expert_up, preferred_element_type=jnp.float32)
    hidden = (jax.nn.silu(gate) * upper).astype(jnp.bfloat16)
    hidden_flat = hidden.reshape(n_sp * EXP_DEV * slots, hidden.shape[3])
    shared_hid = (
        jax.nn.silu(jnp.dot(normal, shared_gate, preferred_element_type=jnp.float32))
        * jnp.dot(normal, shared_up, preferred_element_type=jnp.float32)
    ).astype(jnp.bfloat16)
    expert_piece = lax.all_gather(hidden_flat, "tp", axis=1, tiled=True)
    shared_piece = lax.all_gather(shared_hid, "tp", axis=1, tiled=True)
    count = expert_piece.shape[1]
    expert_part = jnp.einsum(
        "nesh,ehd->nesd",
        expert_piece.reshape(n_sp, EXP_DEV, slots, count),
        expert_down,
        preferred_element_type=jnp.float32,
    )
    shared_part = jnp.dot(shared_piece, shared_down, preferred_element_type=jnp.float32)
    returned = lax.all_to_all(
        expert_part.astype(jnp.bfloat16), "sp", split_axis=0, concat_axis=0, tiled=True
    )
    picked = (
        returned.reshape(total, cols)[slot].astype(jnp.float32) * route_weight.reshape(-1)[:, None]
    )
    routed = jnp.sum(picked.reshape(tokens, TOPK, cols), axis=1)
    return (stream32 + shared_part + routed).astype(jnp.bfloat16)


MESH = pl.DeviceIdType.MESH
F32 = jnp.float32
BF16 = jnp.bfloat16


def silu_mul(gate, upper):
    return (gate / (1.0 + jnp.exp(-gate)) * upper).astype(BF16)


def mm(a, b):
    return jnp.dot(a, b, preferred_element_type=F32)


SPLIT = 2


GIVEN = (1, 0, 2, 3)
HOP, START, WIRE, NEAR = 2.8, 4.0, 4.18, (1.4, 2.5)
COST, EXTRA = (0.45, 0.15, 0.15, 0.15, 0.15, 1.65, 1.3, 0.2), (0.9, 0.15)
FULL = ((1, 2, 3), (0,), (1, 2, 3))
ROWX = (2.8, 4.5, -2, 6, -4.8, 0.1, 0.2, -4.4, -7.7, 3.3, -10, 3.7, -0.2, 0.7, 5.9, -0.4)
ROWZ = (0.5, -2.7, 0.5, -2.4, -4.1, -0.1, 2.8, -6.3, 4.6, 2.6, 2.3, 1.4, 0.3, -0.9, -3, 4.4)
ROWF = (1.3, 3, -5.7, 3.9)
COMB = (1.7, 3.6, 3.6, -1.7, 5.9, 5.1, -0.3, -0.2, -6, -1.4, -3.2, -5.6, -1, 1.9, 2, 3.1)
WORK = (6.6, -4.2, -3.5, 5.1, 1.1, 4.1, -1.4, 2.4, -4.3, 4.5, 1.2, -5.4, 2.4, -4.2, -3.7, 5.7)
RANK = (3, 4, 3, 4, 4)
DEPTH = (0.5, 2)
BASE = 257


KINDS = ("stream", "land", "up", "down", "across", "hidden", "result", "combine")


def inner(n_z, z):
    return int(0 < z < n_z - 1)


def full_rows(n_z, source, target, half, q):
    kind = inner(n_z, target) * (1 + inner(n_z, source))
    return abs(source - target) == 1 and half * 2 + q in FULL[kind]


def plan(n_z):
    chunks = [(half, q) for half in range(SPLIT) for q in range(2)]
    zones = range(n_z)
    never = 1e9
    have, told, heard, summed, went, begun, final, arrive = {}, {}, {}, {}, {}, {}, {}, {}
    todo = {z: [] for z in zones}
    for z in zones:
        for k, (half, q) in enumerate(chunks):
            todo[z].append(("stream", z, 0, half, q))
            went[z, half, q] = START + WIRE * (GIVEN.index(k) + 1) + HOP
        for zq in zones:
            for half, q in chunks:
                if zq != z:
                    todo[z].append(("land", zq, 0, half, q))
                todo[z].append(("land", zq, 1, half, q))
                if zq <= z < n_z - 1:
                    todo[z].append(("up", zq, 0, half, q))
                if zq >= z > 0:
                    todo[z].append(("down", zq, 0, half, q))
                if not full_rows(n_z, zq, z, half, q):
                    todo[z].append(("across", zq, 0, half, q))
                todo[z] += [("combine", zq, h, half, q) for h in range(2)]
            for half in range(SPLIT):
                todo[z].append(("hidden", zq, 0, half, 0))
                todo[z].append(("result", zq, 0, half, 0))
        for half, q in chunks:
            if z < n_z - 1 and full_rows(n_z, z, z + 1, half, q):
                todo[z].append(("up", z, 1, half, q))
            if z > 0 and full_rows(n_z, z, z - 1, half, q):
                todo[z].append(("down", z, 1, half, q))
    link = {(z, way): 0.0 for z in zones for way in ("up", "down", "across")}
    for z in zones:
        link[z, "across"] = START + WIRE * len(chunks)
    core = {z: START for z in zones}

    def put(z, way, now, size):
        link[z, way] = max(now, link[z, way]) + WIRE * size
        return link[z, way] + HOP

    def ready(z, event):
        kind, zq, h, half, q = event
        if kind == "stream":
            return went[z, half, q]
        if kind == "land":
            return arrive.get((z, zq, h, half, q), never)
        if kind in ("up", "down", "across"):
            depth = DEPTH[kind == "across"]
            return max(have.get((z, zq, h, half, q), never), link[z, kind] - depth)
        if kind == "hidden":
            parts = [have.get((z, zq, g, half, p), never) for g in range(2) for p in range(2)]
            return max(parts) + NEAR[0]
        if kind == "result":
            return heard.get((z, zq, half), never)
        at = told.get((z, zq, half), never)
        if zq >= z and z > 0:
            at = max(at, summed.get((z - 1, zq, h, half, q), never))
        if zq <= z and z < n_z - 1:
            at = max(at, summed.get((z + 1, zq, h, half, q), never))
        if h > 0:
            at = max(at, begun.get((z, zq, half, q), never))
        if zq == z and q > 0:
            at = max(at, begun.get((z, zq, half, 0), never))
        return at

    def rank(z, event):
        kind, zq, h, half, q = event
        place = (inner(n_z, z) * 4 + abs(zq - z)) * 2 + half
        if kind in ("stream", "land"):
            return (RANK[0], 0.0, q)
        if kind == "combine":
            return (RANK[1], COMB[place], q)
        if kind == "result":
            return (RANK[2], WORK[place], q)
        if kind == "hidden":
            return (RANK[3], WORK[place], q)
        if kind == "across":
            return (RANK[4], ROWX[place], q)
        return (RANK[4], ROWZ[place] if h == 0 else ROWF[inner(n_z, z) * 2 + half], q)

    order = {z: [] for z in zones}
    while any(todo.values()):
        best = None
        for z in zones:
            if not todo[z]:
                continue
            starts = [(max(core[z], ready(z, event)), event) for event in todo[z]]
            at = min(start for start, _ in starts)
            if best is None or at < best[0]:
                best = (at, z, starts)
        at, z, starts = best
        assert at < never
        event = min((e for start, e in starts if start <= at), key=lambda e: rank(z, e))
        kind, zq, h, half, q = event
        todo[z].remove(event)
        order[z].append(event)
        end = at + COST[KINDS.index(kind)]
        if zq == z:
            end = end + (EXTRA[0] if kind == "hidden" else EXTRA[1] if kind == "combine" else 0.0)
        core[z] = end
        if kind in ("stream", "land"):
            have[z, zq, h, half, q] = end
        elif kind in ("up", "down"):
            arrive[z + (1 if kind == "up" else -1), zq, h, half, q] = put(z, kind, end, 1.0)
        elif kind == "across":
            arrive[z, zq, 1, half, q] = put(z, kind, end, 1.0)
        elif kind == "hidden":
            heard[z, zq, half] = put(z, "across", end, 1.0 if zq == z else 0.5)
        elif kind == "result":
            told[z, zq, half] = end + NEAR[1]
        else:
            if h == 0:
                begun[z, zq, half, q] = end
            if zq == z:
                final[z, h, half, q] = end
            else:
                summed[z, zq, h, half, q] = put(z, "up" if zq > z else "down", end, 0.5)
    return order, max(final.values())


def encode(events, slots):
    codes = [
        (((KINDS.index(kind) * 4 + zq) * 2 + h) * 2 + half) * 2 + q + 1
        for kind, zq, h, half, q in events
    ]
    codes += [0] * (slots - len(codes))
    return [sum(codes[at + k] * BASE**k for k in range(3)) for at in range(0, slots, 3)]


def layer_kernel(
    n_z,
    most,
    og_hbm,
    ig_hbm,
    ci_hbm,
    res_hbm,
    wo_hbm,
    docs_ref,
    taps_ref,
    mix_ref,
    ffn_ref,
    names_ref,
    share_ref,
    wg_hbm,
    wu_hbm,
    wd_hbm,
    sg_hbm,
    su_hbm,
    sd_hbm,
    out_hbm,
    og,
    ig,
    ci,
    res,
    wo,
    wg,
    wu,
    wd,
    sg,
    su,
    sd,
    ext,
    dext,
    hsend,
    hrecv,
    act,
    ssq,
    srow,
    gsend,
    grecv,
    fg,
    tri,
    blk,
    meta,
    xs,
    hid,
    shid,
    ys,
    acc,
    outgo,
    sib,
    back,
    done,
    load_sem,
    halo_sem,
    sum_sem,
    fg_sem,
    giv_recv,
    z_send,
    x_send,
    c_send,
    b_recv,
    s_recv,
    m_send,
    m_recv,
    hid_send,
    hid_recv,
    sh_send,
    sh_recv,
    sib_send,
    sib_recv,
    back_send,
    back_recv,
    out_sem,
):
    first = [
        pltpu.make_async_copy(src, dst, load_sem.at[n])
        for n, (src, dst) in enumerate(
            ((ig_hbm, ig), (ci_hbm, ci), (og_hbm, og), (wo_hbm, wo), (res_hbm, res))
        )
    ]
    later = [
        pltpu.make_async_copy(src, dst, load_sem.at[5 + n])
        for n, (src, dst) in enumerate(
            ((wg_hbm, wg), (wu_hbm, wu), (wd_hbm, wd), (sg_hbm, sg), (su_hbm, su), (sd_hbm, sd))
        )
    ]
    for load in first:
        load.start()
    s = lax.axis_index("sp")
    t = lax.axis_index("tp")
    z = s // 2
    c = s % 2
    tokens, chan = ig.shape
    cols = res.shape[1]
    width = 2 * cols
    half_rows = tokens // SPLIT
    n_chunks = 2 * SPLIT
    piece = half_rows // 2
    part_rows = piece // 2
    unit = wg.shape[2]
    pad = ext.shape[0] - tokens
    lo = z > 0
    hi = z < n_z - 1
    up, down = {"sp": s + 2}, {"sp": s - 2}
    other, peer = {"sp": s + 1 - 2 * c}, {"tp": 1 - t}
    after = {"sp": s + 1}
    before = {"sp": s - 1}
    targets = (up, down, peer, other)

    def remote(src, dst, ssem, rsem, dev):
        return pltpu.make_async_remote_copy(
            src_ref=src,
            dst_ref=dst,
            send_sem=ssem,
            recv_sem=rsem,
            device_id=dev,
            device_id_type=MESH,
        )

    def chunk(zq, h, half, q, ssem, rsem, dev):
        ref = blk.at[zq * 2 + c, half, h, pl.ds(q * piece, piece)]
        return remote(ref, ref, ssem, rsem, dev)

    def side(h):
        return t + h * (1 - 2 * t)

    def z_copy(way, zq, h, half, q):
        ssem = z_send.at[way, zq + h * (n_z - zq + half * 2 + q)]
        return chunk(
            zq, side(h), half, q, ssem, b_recv.at[zq, side(h), half, q], targets[way]
        )

    def z_sent(way, zq):
        ref = blk.at[0]
        return remote(ref.at[0], ref.at[0], z_send.at[way, zq], b_recv.at[0, 0, 0, 0], targets[way])

    def x_copy(zq, half, q):
        return chunk(zq, t, half, q, x_send.at[zq, half, q], b_recv.at[zq, t, half, q], peer)

    def c_copy(zq, h, half, q):
        return chunk(zq, h, half, q, c_send.at[0], s_recv.at[zq, half], other)

    def c_all():
        ref = blk.at[pl.ds(0, n_z)]
        return remote(ref, ref, c_send.at[0], s_recv.at[0, 0], other)

    def near_by(zq, half):
        ref = blk.at[zq * 2 + 1 - c, half]
        return remote(ref, ref, c_send.at[0], s_recv.at[zq, half], other)

    def arrived(zq, h, half, q):
        chunk(zq, h, half, q, c_send.at[0], b_recv.at[zq, h, half, q], other).wait_recv()

    def m_copy(way, zq, cq, half):
        ref = meta.at[zq * 2 + cq, half]
        ssem = m_send.at[way * n_z + zq * (way < 2)]
        return remote(ref, ref, ssem, m_recv.at[zq * 2 + cq, half], (up, down, other)[way])

    def m_sent(way, zq):
        ref = meta.at[0] if way < 2 else meta.at[pl.ds(0, n_z)]
        return remote(
            ref, ref, m_send.at[way * n_z + zq], m_recv.at[0, 0], (up, down, other)[way]
        )

    def hid_copy(zq, half):
        return remote(
            hid.at[t, zq, half],
            hid.at[t, zq, half],
            hid_send.at[0],
            hid_recv.at[zq, half],
            peer,
        )

    def sh_copy(half):
        return remote(
            shid.at[t, half], shid.at[t, half], sh_send.at[half], sh_recv.at[half], peer
        )

    def sib_copy(zq, half, q):
        rows = pl.ds(q * piece, piece)
        return remote(
            outgo.at[zq, half, rows],
            sib.at[zq, half, rows],
            sib_send.at[0],
            sib_recv.at[zq, half, q],
            other,
        )

    def back_copy(zq, half, p, to, dev):
        rows = pl.ds(p * part_rows, part_rows)
        return remote(
            acc.at[zq, half, rows],
            back.at[to, half, rows],
            back_send.at[0],
            back_recv.at[to, half, p],
            dev,
        )

    def halo_copy():
        return remote(hsend, hrecv, halo_sem.at[0], halo_sem.at[1], after)

    def sum_copy(r):
        return remote(srow.at[0, r], srow.at[1, r], sum_sem.at[n_chunks], sum_sem.at[r], peer)

    def fg_copy():
        return remote(fg.at[t], fg.at[t], fg_sem.at[0], fg_sem.at[1], peer)

    def giv_copy(r):
        return remote(gsend.at[r], grecv.at[r], giv_recv.at[n_chunks], giv_recv.at[r], peer)

    barrier = pltpu.get_barrier_semaphore()
    cross_up = hi & (c == 1)
    cross_down = lo & (c == 0)
    for target, there in ((up, hi), (down, lo), (after, cross_up), (before, cross_down)):

        @pl.when(there)
        def _():
            pl.semaphore_signal(barrier, inc=1, device_id=target, device_id_type=MESH)

    for target in (peer, other):
        pl.semaphore_signal(barrier, inc=1, device_id=target, device_id_type=MESH)

    has_next = s < 2 * n_z - 1
    has_prev = s > 0
    first[0].wait()
    first[1].wait()

    tail = 16

    def product(rows):
        return (ig[rows, :].astype(F32) * ci[rows, :].astype(F32)).astype(BF16).astype(F32)

    lanes = dext.shape[1]
    eye = lax.broadcasted_iota(jnp.int32, (lanes, lanes), 0) == lax.broadcasted_iota(
        jnp.int32, (lanes, lanes), 1
    )

    def upright(line):
        return jnp.sum(jnp.where(eye, line, F32(0.0)), axis=1, keepdims=True)

    docs = docs_ref[...].astype(F32)
    for k in range(tokens // lanes):
        column = upright(docs[k : k + 1, :])
        dext[pad + k * lanes : pad + (k + 1) * lanes, :] = jnp.broadcast_to(column, (lanes, lanes))
    end_rows = product(pl.ds(tokens - tail, tail))
    hsend[:, :chan] = end_rows[tail - 8 :]
    hsend[:, chan:] = dext[pad + tokens - 8 : pad + tokens, :]
    own = z * 2 + c
    names = names_ref[...].astype(F32)
    share = share_ref[...]
    for half in range(SPLIT):
        part = slice(half * half_rows, (half + 1) * half_rows)
        meta[own, half] = jnp.zeros(meta.shape[2:], F32)
        meta[own, half, 0:TOPK, :half_rows] = names[:, part]
        meta[own, half, TOPK : 2 * TOPK, :half_rows] = share[:, part]
    fg[t] = ffn_ref[...]
    step_rows = 32

    @pl.loop(0, tokens // step_rows)
    def _(i):
        at = pl.multiple_of(i * step_rows, step_rows)
        ext[pl.ds(pad + at, step_rows), :] = product(pl.ds(at, step_rows))

    n_tri = tri.shape[0]
    row_id = lax.broadcasted_iota(jnp.int32, (n_tri, n_tri), 0)
    col_id = lax.broadcasted_iota(jnp.int32, (n_tri, n_tri), 1)
    tri[...] = (row_id < col_id).astype(F32).astype(BF16)

    def convolve(r):
        @pl.loop(0, piece // step_rows)
        def _(i):
            at = pl.multiple_of(r * piece + i * step_rows, step_rows)
            v = ext[pl.ds(pl.multiple_of(pad - 8 + at, 8), step_rows + 8), :]
            d = dext[pl.ds(pl.multiple_of(pad - 8 + at, 8), step_rows + 8), :]
            doc = d[8:]
            mixed = None
            for k in range(CONV_K):
                by = CONV_K - 1 - k
                if by:
                    same = (pltpu.roll(d, by, 0)[8:] == doc).astype(F32)
                    same = jnp.concatenate([same] * (chan // lanes), axis=1)
                    term = taps_ref[k : k + 1, :] * pltpu.roll(v, by, 0)[8:] * same
                else:
                    term = taps_ref[k : k + 1, :] * v[8:]
                mixed = term if mixed is None else mixed + term
            rows = pl.ds(at, step_rows)
            conv_out = og[rows, :].astype(F32) * mixed
            total = jnp.sum(conv_out * conv_out, axis=1, keepdims=True)
            ssq[rows, :] = jnp.broadcast_to(total, (step_rows, lanes))
            act[rows, :] = (conv_out * mix_ref[...]).astype(BF16)

    eye_piece = lax.broadcasted_iota(jnp.int32, (piece, lanes), 0) == lax.broadcasted_iota(
        jnp.int32, (piece, lanes), 1
    )

    def out_cols(who):
        return pl.ds(pl.multiple_of(who * cols, cols), cols)

    def sums(r):
        part = ssq[r * piece : (r + 1) * piece, :]
        line = jnp.sum(jnp.where(eye_piece, part, F32(0.0)), axis=0, keepdims=True)
        srow[0, r] = jnp.broadcast_to(line, srow.shape[2:])

    def give(r):
        gsend[r] = mm(act[r * piece : (r + 1) * piece, :], wo[:, out_cols(1 - t)]).astype(BF16)

    def send_given(r):
        sum_copy(r).start()
        giv_copy(r).start()

    first[2].wait()
    convolve(GIVEN[0])
    sums(GIVEN[0])
    first[3].wait()
    give(GIVEN[0])
    arrivals = (
        2
        + lo.astype(jnp.int32)
        + hi.astype(jnp.int32)
        + cross_up.astype(jnp.int32)
        + cross_down.astype(jnp.int32)
    )
    pl.semaphore_wait(barrier, arrivals)

    @pl.when(has_next)
    def _():
        halo_copy().start()

    fg_copy().start()
    send_given(GIVEN[0])
    for half in range(SPLIT):
        m_copy(2, z, c, half).start()

    @pl.when(has_prev)
    def _():
        halo_copy().wait_recv()
        ext[pad - 8 : pad, :] = hrecv[:, :chan]
        dext[pad - 8 : pad, :] = hrecv[:, chan:]

    @pl.when(jnp.logical_not(has_prev))
    def _():
        ext[pad - 8 : pad, :] = jnp.zeros((8, chan), F32)
        dext[pad - 8 : pad, :] = jnp.zeros((8, lanes), F32)

    first[4].wait()
    for r in GIVEN[1:]:
        convolve(r)
        sums(r)
        give(r)
        send_given(r)
    fg_copy().wait_recv()

    def picks(zq, cq, half):
        info = meta[zq * 2 + cq, half][:, :half_rows]
        mine = (lax.broadcasted_iota(jnp.int32, (8, half_rows), 0) + s * EXP_DEV).astype(F32)
        hot0 = info[0:1] == mine
        hot1 = info[1:2] == mine
        hot = hot0 | hot1
        earlier = mm(hot.astype(F32).astype(BF16), tri[...])
        position = jnp.where(hot, earlier, F32(-1.0))
        weight = jnp.where(hot0, info[2:3], F32(0.0)) + jnp.where(hot1, info[3:4], F32(0.0))
        place = lax.broadcasted_iota(jnp.int32, (most, half_rows), 0).astype(F32)
        chosen = [(position[e : e + 1] == place).astype(F32) for e in range(EXP_DEV)]
        return chosen, weight

    def norm_scale(parts):
        total = sum(jnp.sum(part * part, axis=1, keepdims=True) for part in parts)
        return lax.rsqrt(total / width + 1e-06)

    def normal_of(parts):
        scale = norm_scale(parts)
        return [(part * scale * fg[h, 0:1, :]).astype(BF16) for h, part in enumerate(parts)]

    def sides():
        return [(0, c), (1, 1 - c)]

    def hidden(zq, half):
        for p, cq in sides():
            chosen, _ = picks(zq, cq, half)
            sel = jnp.concatenate(chosen, axis=0).astype(BF16)
            got = normal_of([mm(sel, blk[zq * 2 + cq, half, h]) for h in range(2)])
            for h in range(2):
                for e in range(EXP_DEV):
                    xs[e, p * most : (p + 1) * most, h * cols : (h + 1) * cols] = got[h][
                        e * most : (e + 1) * most
                    ]
        for e in range(EXP_DEV):
            hid[t, zq, half, e] = silu_mul(mm(xs[e], wg[e]), mm(xs[e], wu[e]))

    def shared(half):
        whole = normal_of([blk[z * 2 + c, half, h].astype(F32) for h in range(2)])
        gate = mm(whole[0], sg[:cols, :]) + mm(whole[1], sg[cols:, :])
        upper = mm(whole[0], su[:cols, :]) + mm(whole[1], su[cols:, :])
        shid[t, half] = silu_mul(gate, upper)

    def results(zq, half):
        hid_copy(zq, half).wait_recv()
        for e in range(EXP_DEV):
            ys[e] = (
                mm(hid[0, zq, half, e], wd[e, :unit, :]) + mm(hid[1, zq, half, e], wd[e, unit:, :])
            ).astype(BF16)
        for p, cq in sides():
            chosen, weight = picks(zq, cq, half)
            parts = []
            for e in range(EXP_DEV):
                scale = jnp.sum(chosen[e] * weight[e : e + 1], axis=1, keepdims=True)
                part = ys[e, p * most : (p + 1) * most, :].astype(F32)
                parts.append((part * scale).astype(BF16))
            sel = jnp.concatenate(chosen, axis=0).astype(BF16)
            into = acc if p == 0 else outgo
            into[zq, half] = lax.dot_general(
                sel,
                jnp.concatenate(parts, axis=0),
                (((0,), (0,)), ((), ())),
                preferred_element_type=F32,
            ).astype(BF16)
        for q in range(2):
            sib_copy(zq, half, q).start()

    def is_end(zq):
        return ((zq > z) & jnp.logical_not(lo)) | ((zq < z) & jnp.logical_not(hi))

    def strip(q):
        return pl.ds(pl.multiple_of(q * piece, piece), piece)

    def on_stream(zq, h, half, q):
        r = half * 2 + q
        rows = pl.ds(pl.multiple_of(r * piece, piece), piece)
        kept = mm(act[rows, :], wo[:, out_cols(t)])
        sum_copy(r).wait_recv()
        line = srow[1, r, 0:1, :]
        theirs = jnp.sum(jnp.where(eye_piece, line, F32(0.0)), axis=1, keepdims=True)
        scale = lax.rsqrt((ssq[rows, 0:1] + theirs) / (2 * chan) + 1e-06)
        giv_copy(r).wait_recv()
        proj = (kept + grecv[r].astype(F32)) * scale
        blk[z * 2 + c, half, t, strip(q), :] = (res[rows, :].astype(F32) + proj).astype(BF16)
        c_copy(z, t, half, q).start()

        @pl.when(r == GIVEN[0])
        def _():
            for load in later:
                load.start()

        @pl.when(r == GIVEN[-1])
        def _():
            for load in later:
                load.wait()

    def on_land(zq, h, half, q):
        @pl.when((h == 0) & (q == 0))
        def _():
            m_copy(2, zq, c, half).wait_recv()
            m_copy(2, zq, c, half).start()

        arrived(zq, side(h), half, q)
        c_copy(zq, side(h), half, q).start()

    def on_z(way):
        def send(zq, h, half, q):
            @pl.when((h == 0) & (q == 0))
            def _():
                m_copy(way, zq, c, half).start()

            z_copy(way, zq, h, half, q).start()

        return send

    def on_across(zq, h, half, q):
        x_copy(zq, half, q).start()

    def on_hidden(zq, h, half, q):
        m_copy(2, zq, 1 - c, half).wait_recv()
        near_by(zq, half).wait_recv()
        hidden(zq, half)
        hid_copy(zq, half).start()

        @pl.when(zq == z)
        def _():
            shared(half)
            sh_copy(half).start()

    def on_result(zq, h, half, q):
        results(zq, half)

    def out_copy(half, p):
        return pltpu.make_async_copy(
            done.at[half, pl.ds(p * part_rows, part_rows)],
            out_hbm.at[pl.ds(half * half_rows + p * part_rows, part_rows)],
            out_sem.at[half, p],
        )

    def finish(half, p, rows):
        @pl.when(p == 0)
        def _():
            sh_copy(half).wait_recv()

        fin = (
            blk[z * 2 + c, half, t, rows, :].astype(F32)
            + mm(shid[0, half, rows, :], sd[:unit, :])
            + mm(shid[1, half, rows, :], sd[unit:, :])
            + acc[z, half, rows, :].astype(F32)
            + sib[z, half, rows, :].astype(F32)
        )

        @pl.when(lo)
        def _():
            back_copy(z, half, p, z, up).wait_recv()

        @pl.when(hi)
        def _():
            back_copy(z, half, p, n_z, up).wait_recv()

        low = jnp.where(lo, back[z, half, rows, :].astype(F32), F32(0.0))
        high = jnp.where(hi, back[n_z, half, rows, :].astype(F32), F32(0.0))
        done[half, rows, :] = (fin + low + high).astype(BF16)
        out_copy(half, p).start()

    def on_combine(zq, h, half, q):
        p = q * 2 + h
        rows = pl.ds(pl.multiple_of(p * part_rows, part_rows), part_rows)

        @pl.when(h == 0)
        def _():
            sib_copy(zq, half, q).wait_recv()

        @pl.when(zq == z)
        def _():
            finish(half, p, rows)

        @pl.when(zq != z)
        def _():
            @pl.when(is_end(zq))
            def _():
                acc[zq, half, rows, :] = (
                    acc[zq, half, rows, :].astype(F32) + sib[zq, half, rows, :].astype(F32)
                ).astype(BF16)

            @pl.when(jnp.logical_not(is_end(zq)))
            def _():
                back_copy(zq, half, p, zq, up).wait_recv()
                acc[zq, half, rows, :] = (
                    acc[zq, half, rows, :].astype(F32)
                    + sib[zq, half, rows, :].astype(F32)
                    + back[zq, half, rows, :].astype(F32)
                ).astype(BF16)

            @pl.when(zq > z)
            def _():
                back_copy(zq, half, p, zq, up).start()

            @pl.when(zq < z - 1)
            def _():
                back_copy(zq, half, p, zq, down).start()

            @pl.when(zq == z - 1)
            def _():
                back_copy(zq, half, p, n_z, down).start()

    actions = (
        on_stream,
        on_land,
        on_z(0),
        on_z(1),
        on_across,
        on_hidden,
        on_result,
        on_combine,
    )
    order, _ = plan(n_z)
    groups = [-(-len(order[zz]) // 3) for zz in range(n_z)]
    tables = [encode(order[zz], 3 * max(groups)) for zz in range(n_z)]

    def of_zone(numbers):
        return sum((z == zz).astype(jnp.int32) * numbers[zz] for zz in range(n_z))

    def act_on(value):
        def turn(k, rest):
            mark = rest % BASE + 31
            q, half, h = mark % 2, mark // 2 % 2, mark // 4 % 2
            zq, kind = mark // 8 % 4, mark // 32
            for n, action in enumerate(actions):
                @pl.when(kind == n + 1)
                def _():
                    action(zq, h, half, q)

            return rest // BASE

        lax.fori_loop(0, 3, turn, value)

    span = 8
    values = [of_zone([table[g] for table in tables]) for g in range(max(groups))]
    values += [jnp.int32(0)] * (-len(values) % span)

    def among(k, options):
        return sum((k == n).astype(jnp.int32) * option for n, option in enumerate(options))

    count = of_zone(groups)

    @pl.loop(0, len(values) // span)
    def _(page):
        lines = [among(page, values[n::span]) for n in range(span)]

        def line(n, carry):
            act_on(among(n, lines))
            return carry

        lax.fori_loop(0, jnp.clip(count - page * span, 0, span), line, 0)

    @pl.when(has_next)
    def _():
        halo_copy().wait_send()

    fg_copy().wait_send()
    remote(srow.at[0], srow.at[0], sum_sem.at[n_chunks], sum_sem.at[0], peer).wait_send()
    remote(gsend, gsend, giv_recv.at[n_chunks], giv_recv.at[0], peer).wait_send()
    for half in range(SPLIT):
        sh_copy(half).wait_send()
    c_all().wait_send()
    m_sent(2, 0).wait_send()
    remote(hid.at[t], hid.at[t], hid_send.at[0], hid_recv.at[0, 0], peer).wait_send()
    remote(outgo, outgo, sib_send.at[0], sib_recv.at[0, 0, 0], other).wait_send()
    sent = acc.at[pl.ds(0, n_z - 1)]
    remote(sent, sent, back_send.at[0], back_recv.at[0, 0, 0], up).wait_send()

    for half in range(SPLIT):
        for p in range(4):
            out_copy(half, p).wait()

    def listed(source, target, half, q):
        inside = [(one > 0) & (one < n_z - 1) for one in (source, target)]
        to_end, from_end, both = [half * 2 + q in kind for kind in FULL]
        return (
            (jnp.logical_not(inside[1]) & to_end)
            | (inside[1] & jnp.logical_not(inside[0]) & from_end)
            | (inside[1] & inside[0] & both)
        )

    for half in range(SPLIT):
        for q in range(2):
            for way, there, target in ((0, hi, z + 1), (1, lo, z - 1)):

                @pl.when(there & listed(z, target, half, q))
                def _():
                    z_copy(way, z, 1, half, q).wait_send()

    @pl.loop(0, n_z)
    def _(zq):
        for way, there in ((0, hi & (zq <= z)), (1, lo & (zq >= z))):

            @pl.when(there)
            def _():
                m_sent(way, zq).wait_send()
                z_sent(way, zq).wait_send()

        near = (zq == z + 1) | (zq == z - 1)
        for half in range(SPLIT):
            for q in range(2):

                @pl.when(jnp.logical_not(near & listed(zq, z, half, q)))
                def _():
                    x_copy(zq, half, q).wait_send()


def fast(
    out_gate,
    in_gate,
    conv_input,
    doc_ids,
    residual,
    conv_taps,
    mix_gain,
    out_weight,
    ffn_gain,
    routing,
    route_weight,
    expert_gate,
    expert_up,
    expert_down,
    shared_gate,
    shared_up,
    shared_down,
):
    tokens, cols = residual.shape
    chan, width = out_weight.shape
    n_tp, n_sp = lax.axis_size("tp"), lax.axis_size("sp")
    n_z = n_sp // 2
    rows = tokens // n_tp
    experts = n_sp * EXP_DEV
    most = max(1, 2 * rows * TOPK // experts)
    lanes = 128
    piece = rows // 2
    blocks = n_sp
    unit = expert_gate.shape[2]
    vm = pl.BlockSpec(memory_space=pltpu.VMEM)
    hbm = pl.BlockSpec(memory_space=pl.ANY)
    dma = pltpu.SemaphoreType.DMA
    return pl.pallas_call(
        functools.partial(layer_kernel, n_z, most),
        out_shape=jax.ShapeDtypeStruct((tokens, cols), BF16),
        in_specs=[hbm] * 5 + [vm] * 6 + [hbm] * 6,
        out_specs=hbm,
        scratch_shapes=[
            pltpu.VMEM((tokens, chan), BF16),
            pltpu.VMEM((tokens, chan), BF16),
            pltpu.VMEM((tokens, chan), BF16),
            pltpu.VMEM((tokens, cols), BF16),
            pltpu.VMEM((chan, width), BF16),
            pltpu.VMEM(expert_gate.shape, BF16),
            pltpu.VMEM(expert_up.shape, BF16),
            pltpu.VMEM(expert_down.shape, BF16),
            pltpu.VMEM(shared_gate.shape, BF16),
            pltpu.VMEM(shared_up.shape, BF16),
            pltpu.VMEM(shared_down.shape, BF16),
            pltpu.VMEM((tokens + 16, chan), F32),
            pltpu.VMEM((tokens + 16, lanes), F32),
            pltpu.VMEM((8, chan + lanes), F32),
            pltpu.VMEM((8, chan + lanes), F32),
            pltpu.VMEM((tokens, chan), BF16),
            pltpu.VMEM((tokens, lanes), F32),
            pltpu.VMEM((2, 2 * SPLIT, 8, lanes), F32),
            pltpu.VMEM((2 * SPLIT, piece, cols), BF16),
            pltpu.VMEM((2 * SPLIT, piece, cols), BF16),
            pltpu.VMEM((2, 1, cols), F32),
            pltpu.VMEM((rows, rows), BF16),
            pltpu.VMEM((blocks, SPLIT, 2, rows, cols), BF16),
            pltpu.VMEM((blocks, SPLIT, 8, rows + -rows % lanes), F32),
            pltpu.VMEM((EXP_DEV, 2 * most, width), BF16),
            pltpu.VMEM((2, n_z, SPLIT, EXP_DEV, 2 * most, unit), BF16),
            pltpu.VMEM((2, SPLIT, rows, unit), BF16),
            pltpu.VMEM((EXP_DEV, 2 * most, cols), BF16),
            pltpu.VMEM((n_z, SPLIT, rows, cols), BF16),
            pltpu.VMEM((n_z, SPLIT, rows, cols), BF16),
            pltpu.VMEM((n_z, SPLIT, rows, cols), BF16),
            pltpu.VMEM((n_z + 1, SPLIT, rows, cols), BF16),
            pltpu.VMEM((SPLIT, rows, cols), BF16),
            dma((11,)),
            dma((2,)),
            dma((2 * SPLIT + 1,)),
            dma((2,)),
            dma((2 * SPLIT + 1,)),
            dma((2, n_z + 2 * SPLIT)),
            dma((n_z, SPLIT, 2)),
            dma((1,)),
            dma((n_z, 2, SPLIT, 2)),
            dma((n_z, SPLIT)),
            dma((2 * n_z + 1,)),
            dma((blocks, SPLIT)),
            dma((1,)),
            dma((n_z, SPLIT)),
            dma((SPLIT,)),
            dma((SPLIT,)),
            dma((1,)),
            dma((n_z, SPLIT, 2)),
            dma((1,)),
            dma((n_z + 1, SPLIT, 4)),
            dma((SPLIT, 4)),
        ],
        compiler_params=pltpu.CompilerParams(
            collective_id=0, has_side_effects=True, vmem_limit_bytes=64 * 1024 * 1024 - 65536
        ),
    )(
        out_gate,
        in_gate,
        conv_input,
        residual,
        out_weight,
        doc_ids.reshape(tokens // lanes, lanes),
        conv_taps,
        mix_gain[None, :],
        ffn_gain[None, :],
        routing.T,
        route_weight.T,
        expert_gate,
        expert_up,
        expert_down,
        shared_gate,
        shared_up,
        shared_down,
    )


def fits(mesh):
    return mesh.shape["tp"] == 2 and mesh.shape["sp"] in (4, 6, 8)


def solution(mesh):
    return jax.shard_map(
        fast if fits(mesh) else body,
        mesh=mesh,
        in_specs=(
            P(("grp", "sp"), "tp"),
            P(("grp", "sp"), "tp"),
            P(("grp", "sp"), "tp"),
            P(("grp", "sp")),
            P(("grp", "sp"), "tp"),
            P(None, "tp"),
            P("tp"),
            P("tp", None),
            P("tp"),
            P(("grp", "sp"), None),
            P(("grp", "sp"), None),
            P("sp", None, "tp"),
            P("sp", None, "tp"),
            P("sp", None, "tp"),
            P(None, "tp"),
            P(None, "tp"),
            P(None, "tp"),
        ),
        out_specs=P(("grp", "sp"), "tp"),
        check_vma=False,
    )
```

```python
import functools

import jax
import jax.numpy as jnp
from jax import lax
from jax.experimental import pallas as pl
from jax.experimental.pallas import tpu as pltpu
from jax.sharding import PartitionSpec as P

D_CONV = 1024
CONV_K = 3
TOPK = 2
EXP_DEV = 2


def from_behind(value, axis, steps):
    count = lax.axis_size(axis)
    first, last = (max(0, -steps), min(count, count - steps))
    return lax.ppermute(value, axis, [(source, source + steps) for source in range(first, last)])


def body(
    out_gate,
    in_gate,
    conv_input,
    doc_ids,
    residual,
    conv_taps,
    mix_gain,
    out_weight,
    ffn_gain,
    routing,
    route_weight,
    expert_gate,
    expert_up,
    expert_down,
    shared_gate,
    shared_up,
    shared_down,
):
    tokens = residual.shape[0]
    width = out_weight.shape[1]
    n_tp = lax.axis_size("tp")
    n_sp = lax.axis_size("sp")
    rows = tokens // n_tp
    experts = n_sp * EXP_DEV
    most = max(1, 2 * rows * TOPK // experts)
    slots = n_tp * most
    total = experts * slots
    cols = expert_down.shape[2]
    product = (in_gate.astype(jnp.float32) * conv_input.astype(jnp.float32)).astype(jnp.bfloat16)
    tail = (product[tokens - CONV_K + 1 :], doc_ids[tokens - CONV_K + 1 :].astype(jnp.bfloat16))
    prev_rows, prev_docs = from_behind((tail[0], tail[1]), "sp", 1)
    extended = jnp.concatenate([prev_rows, product], axis=0).astype(jnp.float32)
    ext_docs = jnp.concatenate([prev_docs.astype(jnp.int32), doc_ids])
    mixed = jnp.zeros(product.shape, jnp.float32)
    for k in range(CONV_K):
        keep = (ext_docs[k : k + tokens] == doc_ids)[:, None]
        mixed = mixed + jnp.where(keep, conv_taps[k] * extended[k : k + tokens], jnp.float32(0.0))
    conv_out = out_gate.astype(jnp.float32) * mixed
    squares = lax.psum(jnp.sum(conv_out * conv_out, axis=1), "tp")
    normed = (conv_out * lax.rsqrt(squares / D_CONV + 1e-06)[:, None] * mix_gain).astype(
        jnp.bfloat16
    )
    partial_value = jnp.dot(normed, out_weight, preferred_element_type=jnp.float32)
    proj = lax.psum_scatter(
        partial_value.astype(jnp.bfloat16), "tp", scatter_dimension=1, tiled=True
    ).astype(jnp.float32)
    stream = (residual.astype(jnp.float32) + proj).astype(jnp.bfloat16)
    stream32 = stream.astype(jnp.float32)
    stream_sq = lax.psum(jnp.sum(stream32 * stream32, axis=1), "tp")
    normal_cols = (stream32 * lax.rsqrt(stream_sq / width + 1e-06)[:, None] * ffn_gain).astype(
        jnp.bfloat16
    )
    flat_expert = routing.reshape(-1)
    onehot = (flat_expert[:, None] == jnp.arange(experts, dtype=jnp.int32)[None, :]).astype(
        jnp.int32
    )
    blocked = onehot.reshape(n_tp, rows * TOPK, experts)
    earlier = jnp.cumsum(blocked, axis=1) - blocked
    position = jnp.sum(earlier * blocked, axis=2).reshape(-1)
    entry = jnp.arange(tokens * TOPK, dtype=jnp.int32)
    slot = flat_expert * slots + entry // (rows * TOPK) * most + position
    table = jnp.full((total,), tokens, jnp.int32).at[slot].set(entry // TOPK)
    block_rows = lax.all_to_all(normal_cols, "tp", split_axis=0, concat_axis=1, tiled=True)
    mine = lax.dynamic_index_in_dim(
        table.reshape(n_sp, EXP_DEV, n_tp, most), lax.axis_index("tp"), 2, False
    )
    local = jnp.where(mine >= tokens, rows, mine - lax.axis_index("tp") * rows)
    padded_block = jnp.concatenate([block_rows, jnp.zeros((1, width), jnp.bfloat16)], axis=0)
    got = lax.all_to_all(padded_block[local], "sp", split_axis=0, concat_axis=0, tiled=True)
    arrived, whole = (
        lax.all_gather(got, "tp", axis=2, tiled=True),
        lax.all_gather(block_rows.reshape(1, 1, rows, width), "tp", axis=2, tiled=True),
    )
    normal = whole.reshape(tokens, width)
    gate = jnp.einsum("nesd,edh->nesh", arrived, expert_gate, preferred_element_type=jnp.float32)
    upper = jnp.einsum("nesd,edh->nesh", arrived, expert_up, preferred_element_type=jnp.float32)
    hidden = (jax.nn.silu(gate) * upper).astype(jnp.bfloat16)
    hidden_flat = hidden.reshape(n_sp * EXP_DEV * slots, hidden.shape[3])
    shared_hid = (
        jax.nn.silu(jnp.dot(normal, shared_gate, preferred_element_type=jnp.float32))
        * jnp.dot(normal, shared_up, preferred_element_type=jnp.float32)
    ).astype(jnp.bfloat16)
    expert_piece = lax.all_gather(hidden_flat, "tp", axis=1, tiled=True)
    shared_piece = lax.all_gather(shared_hid, "tp", axis=1, tiled=True)
    count = expert_piece.shape[1]
    expert_part = jnp.einsum(
        "nesh,ehd->nesd",
        expert_piece.reshape(n_sp, EXP_DEV, slots, count),
        expert_down,
        preferred_element_type=jnp.float32,
    )
    shared_part = jnp.dot(shared_piece, shared_down, preferred_element_type=jnp.float32)
    returned = lax.all_to_all(
        expert_part.astype(jnp.bfloat16), "sp", split_axis=0, concat_axis=0, tiled=True
    )
    picked = (
        returned.reshape(total, cols)[slot].astype(jnp.float32) * route_weight.reshape(-1)[:, None]
    )
    routed = jnp.sum(picked.reshape(tokens, TOPK, cols), axis=1)
    return (stream32 + shared_part + routed).astype(jnp.bfloat16)


MESH = pl.DeviceIdType.MESH
F32 = jnp.float32
BF16 = jnp.bfloat16


def silu_mul(gate, upper):
    return (gate / (1.0 + jnp.exp(-gate)) * upper).astype(BF16)


def mm(a, b):
    return jnp.dot(a, b, preferred_element_type=F32)


SPLIT = 2


GIVEN = (1, 0, 2, 3)
HOP, START, WIRE, NEAR = 2.8, 4.0, 4.18, (1.4, 2.5)
COST, EXTRA = (0.45, 0.15, 0.15, 0.15, 0.15, 1.65, 1.3, 0.2), (0.9, 0.15)
FULL = ((1, 2, 3), (0,), (1, 2, 3))
ROWX = (2.8, 4.5, -2, 6, -4.8, 0.1, 0.2, -4.4, -7.7, 3.3, -10, 3.7, -0.2, 0.7, 5.9, -0.4)
ROWZ = (0.5, -2.7, 0.5, -2.4, -4.1, -0.1, 2.8, -6.3, 4.6, 2.6, 2.3, 1.4, 0.3, -0.9, -3, 4.4)
ROWF = (1.3, 3, -5.7, 3.9)
COMB = (1.7, 3.6, 3.6, -1.7, 5.9, 5.1, -0.3, -0.2, -6, -1.4, -3.2, -5.6, -1, 1.9, 2, 3.1)
WORK = (6.6, -4.2, -3.5, 5.1, 1.1, 4.1, -1.4, 2.4, -4.3, 4.5, 1.2, -5.4, 2.4, -4.2, -3.7, 5.7)
RANK = (3, 4, 3, 4, 4)
DEPTH = (0.5, 2)
BASE = 257


KINDS = ("stream", "land", "up", "down", "across", "hidden", "result", "combine")


def inner(n_z, z):
    return int(0 < z < n_z - 1)


def full_rows(n_z, source, target, half, q):
    kind = inner(n_z, target) * (1 + inner(n_z, source))
    return abs(source - target) == 1 and half * 2 + q in FULL[kind]


def plan(n_z):
    chunks = [(half, q) for half in range(SPLIT) for q in range(2)]
    zones = range(n_z)
    never = 1e9
    have, told, heard, summed, went, begun, final, arrive = {}, {}, {}, {}, {}, {}, {}, {}
    todo = {z: [] for z in zones}
    for z in zones:
        for k, (half, q) in enumerate(chunks):
            todo[z].append(("stream", z, 0, half, q))
            went[z, half, q] = START + WIRE * (GIVEN.index(k) + 1) + HOP
        for zq in zones:
            for half, q in chunks:
                if zq != z:
                    todo[z].append(("land", zq, 0, half, q))
                todo[z].append(("land", zq, 1, half, q))
                if zq <= z < n_z - 1:
                    todo[z].append(("up", zq, 0, half, q))
                if zq >= z > 0:
                    todo[z].append(("down", zq, 0, half, q))
                if not full_rows(n_z, zq, z, half, q):
                    todo[z].append(("across", zq, 0, half, q))
                todo[z] += [("combine", zq, h, half, q) for h in range(2)]
            for half in range(SPLIT):
                todo[z].append(("hidden", zq, 0, half, 0))
                todo[z].append(("result", zq, 0, half, 0))
        for half, q in chunks:
            if z < n_z - 1 and full_rows(n_z, z, z + 1, half, q):
                todo[z].append(("up", z, 1, half, q))
            if z > 0 and full_rows(n_z, z, z - 1, half, q):
                todo[z].append(("down", z, 1, half, q))
    link = {(z, way): 0.0 for z in zones for way in ("up", "down", "across")}
    for z in zones:
        link[z, "across"] = START + WIRE * len(chunks)
    core = {z: START for z in zones}

    def put(z, way, now, size):
        link[z, way] = max(now, link[z, way]) + WIRE * size
        return link[z, way] + HOP

    def ready(z, event):
        kind, zq, h, half, q = event
        if kind == "stream":
            return went[z, half, q]
        if kind == "land":
            return arrive.get((z, zq, h, half, q), never)
        if kind in ("up", "down", "across"):
            depth = DEPTH[kind == "across"]
            return max(have.get((z, zq, h, half, q), never), link[z, kind] - depth)
        if kind == "hidden":
            parts = [have.get((z, zq, g, half, p), never) for g in range(2) for p in range(2)]
            return max(parts) + NEAR[0]
        if kind == "result":
            return heard.get((z, zq, half), never)
        at = told.get((z, zq, half), never)
        if zq >= z and z > 0:
            at = max(at, summed.get((z - 1, zq, h, half, q), never))
        if zq <= z and z < n_z - 1:
            at = max(at, summed.get((z + 1, zq, h, half, q), never))
        if h > 0:
            at = max(at, begun.get((z, zq, half, q), never))
        if zq == z and q > 0:
            at = max(at, begun.get((z, zq, half, 0), never))
        return at

    def rank(z, event):
        kind, zq, h, half, q = event
        place = (inner(n_z, z) * 4 + abs(zq - z)) * 2 + half
        if kind in ("stream", "land"):
            return (RANK[0], 0.0, q)
        if kind == "combine":
            return (RANK[1], COMB[place], q)
        if kind == "result":
            return (RANK[2], WORK[place], q)
        if kind == "hidden":
            return (RANK[3], WORK[place], q)
        if kind == "across":
            return (RANK[4], ROWX[place], q)
        return (RANK[4], ROWZ[place] if h == 0 else ROWF[inner(n_z, z) * 2 + half], q)

    order = {z: [] for z in zones}
    while any(todo.values()):
        best = None
        for z in zones:
            if not todo[z]:
                continue
            starts = [(max(core[z], ready(z, event)), event) for event in todo[z]]
            at = min(start for start, _ in starts)
            if best is None or at < best[0]:
                best = (at, z, starts)
        at, z, starts = best
        assert at < never
        event = min((e for start, e in starts if start <= at), key=lambda e: rank(z, e))
        kind, zq, h, half, q = event
        todo[z].remove(event)
        order[z].append(event)
        end = at + COST[KINDS.index(kind)]
        if zq == z:
            end = end + (EXTRA[0] if kind == "hidden" else EXTRA[1] if kind == "combine" else 0.0)
        core[z] = end
        if kind in ("stream", "land"):
            have[z, zq, h, half, q] = end
        elif kind in ("up", "down"):
            arrive[z + (1 if kind == "up" else -1), zq, h, half, q] = put(z, kind, end, 1.0)
        elif kind == "across":
            arrive[z, zq, 1, half, q] = put(z, kind, end, 1.0)
        elif kind == "hidden":
            heard[z, zq, half] = put(z, "across", end, 1.0 if zq == z else 0.5)
        elif kind == "result":
            told[z, zq, half] = end + NEAR[1]
        else:
            if h == 0:
                begun[z, zq, half, q] = end
            if zq == z:
                final[z, h, half, q] = end
            else:
                summed[z, zq, h, half, q] = put(z, "up" if zq > z else "down", end, 0.5)
    return order, max(final.values())


def encode(events, slots):
    codes = [
        (((KINDS.index(kind) * 4 + zq) * 2 + h) * 2 + half) * 2 + q + 1
        for kind, zq, h, half, q in events
    ]
    codes += [0] * (slots - len(codes))
    return [sum(codes[at + k] * BASE**k for k in range(3)) for at in range(0, slots, 3)]


def layer_kernel(
    n_z,
    most,
    og_hbm,
    ig_hbm,
    ci_hbm,
    res_hbm,
    wo_hbm,
    docs_ref,
    taps_ref,
    mix_ref,
    ffn_ref,
    names_ref,
    share_ref,
    wg_hbm,
    wu_hbm,
    wd_hbm,
    sg_hbm,
    su_hbm,
    sd_hbm,
    out_hbm,
    og,
    ig,
    ci,
    res,
    wo,
    wg,
    wu,
    wd,
    sg,
    su,
    sd,
    ext,
    dext,
    hsend,
    hrecv,
    act,
    ssq,
    srow,
    gsend,
    grecv,
    fg,
    tri,
    blk,
    meta,
    xs,
    hid,
    shid,
    ys,
    acc,
    outgo,
    sib,
    back,
    done,
    load_sem,
    halo_sem,
    sum_sem,
    fg_sem,
    giv_recv,
    z_send,
    x_send,
    c_send,
    b_recv,
    s_recv,
    m_send,
    m_recv,
    hid_send,
    hid_recv,
    sh_send,
    sh_recv,
    sib_send,
    sib_recv,
    back_send,
    back_recv,
    out_sem,
):
    first = [
        pltpu.make_async_copy(src, dst, load_sem.at[n])
        for n, (src, dst) in enumerate(
            ((ig_hbm, ig), (ci_hbm, ci), (og_hbm, og), (wo_hbm, wo), (res_hbm, res))
        )
    ]
    later = [
        pltpu.make_async_copy(src, dst, load_sem.at[5 + n])
        for n, (src, dst) in enumerate(
            ((wg_hbm, wg), (wu_hbm, wu), (wd_hbm, wd), (sg_hbm, sg), (su_hbm, su), (sd_hbm, sd))
        )
    ]
    for load in first:
        load.start()
    s = lax.axis_index("sp")
    t = lax.axis_index("tp")
    z = s // 2
    c = s % 2
    tokens, chan = ig.shape
    cols = res.shape[1]
    width = 2 * cols
    half_rows = tokens // SPLIT
    n_chunks = 2 * SPLIT
    piece = half_rows // 2
    part_rows = piece // 2
    unit = wg.shape[2]
    pad = ext.shape[0] - tokens
    lo = z > 0
    hi = z < n_z - 1
    up, down = {"sp": s + 2}, {"sp": s - 2}
    other, peer = {"sp": s + 1 - 2 * c}, {"tp": 1 - t}
    after = {"sp": s + 1}
    before = {"sp": s - 1}
    targets = (up, down, peer, other)

    def remote(src, dst, ssem, rsem, dev):
        return pltpu.make_async_remote_copy(
            src_ref=src,
            dst_ref=dst,
            send_sem=ssem,
            recv_sem=rsem,
            device_id=dev,
            device_id_type=MESH,
        )

    def chunk(zq, h, half, q, ssem, rsem, dev):
        ref = blk.at[zq * 2 + c, half, h, pl.ds(q * piece, piece)]
        return remote(ref, ref, ssem, rsem, dev)

    def side(h):
        return t + h * (1 - 2 * t)

    def z_copy(way, zq, h, half, q):
        ssem = z_send.at[way, zq + h * (n_z - zq + half * 2 + q)]
        return chunk(
            zq, side(h), half, q, ssem, b_recv.at[zq, side(h), half, q], targets[way]
        )

    def z_sent(way, zq):
        ref = blk.at[0]
        return remote(ref.at[0], ref.at[0], z_send.at[way, zq], b_recv.at[0, 0, 0, 0], targets[way])

    def x_copy(zq, half, q):
        return chunk(zq, t, half, q, x_send.at[zq, half, q], b_recv.at[zq, t, half, q], peer)

    def c_copy(zq, h, half, q):
        return chunk(zq, h, half, q, c_send.at[0], s_recv.at[zq, half], other)

    def c_all():
        ref = blk.at[pl.ds(0, n_z)]
        return remote(ref, ref, c_send.at[0], s_recv.at[0, 0], other)

    def near_by(zq, half):
        ref = blk.at[zq * 2 + 1 - c, half]
        return remote(ref, ref, c_send.at[0], s_recv.at[zq, half], other)

    def arrived(zq, h, half, q):
        chunk(zq, h, half, q, c_send.at[0], b_recv.at[zq, h, half, q], other).wait_recv()

    def m_copy(way, zq, cq, half):
        ref = meta.at[zq * 2 + cq, half]
        ssem = m_send.at[way * n_z + zq * (way < 2)]
        return remote(ref, ref, ssem, m_recv.at[zq * 2 + cq, half], (up, down, other)[way])

    def m_sent(way, zq):
        ref = meta.at[0] if way < 2 else meta.at[pl.ds(0, n_z)]
        return remote(
            ref, ref, m_send.at[way * n_z + zq], m_recv.at[0, 0], (up, down, other)[way]
        )

    def hid_copy(zq, half):
        return remote(
            hid.at[t, zq, half],
            hid.at[t, zq, half],
            hid_send.at[0],
            hid_recv.at[zq, half],
            peer,
        )

    def sh_copy(half):
        return remote(
            shid.at[t, half], shid.at[t, half], sh_send.at[half], sh_recv.at[half], peer
        )

    def sib_copy(zq, half, q):
        rows = pl.ds(q * piece, piece)
        return remote(
            outgo.at[zq, half, rows],
            sib.at[zq, half, rows],
            sib_send.at[0],
            sib_recv.at[zq, half, q],
            other,
        )

    def back_copy(zq, half, p, to, dev):
        rows = pl.ds(p * part_rows, part_rows)
        return remote(
            acc.at[zq, half, rows],
            back.at[to, half, rows],
            back_send.at[0],
            back_recv.at[to, half, p],
            dev,
        )

    def halo_copy():
        return remote(hsend, hrecv, halo_sem.at[0], halo_sem.at[1], after)

    def sum_copy(r):
        return remote(srow.at[0, r], srow.at[1, r], sum_sem.at[n_chunks], sum_sem.at[r], peer)

    def fg_copy():
        return remote(fg.at[t], fg.at[t], fg_sem.at[0], fg_sem.at[1], peer)

    def giv_copy(r):
        return remote(gsend.at[r], grecv.at[r], giv_recv.at[n_chunks], giv_recv.at[r], peer)

    barrier = pltpu.get_barrier_semaphore()
    cross_up = hi & (c == 1)
    cross_down = lo & (c == 0)
    for target, there in ((up, hi), (down, lo), (after, cross_up), (before, cross_down)):

        @pl.when(there)
        def _():
            pl.semaphore_signal(barrier, inc=1, device_id=target, device_id_type=MESH)

    for target in (peer, other):
        pl.semaphore_signal(barrier, inc=1, device_id=target, device_id_type=MESH)

    has_next = s < 2 * n_z - 1
    has_prev = s > 0
    first[0].wait()
    first[1].wait()

    tail = 16

    def product(rows):
        return (ig[rows, :].astype(F32) * ci[rows, :].astype(F32)).astype(BF16).astype(F32)

    lanes = dext.shape[1]
    eye = lax.broadcasted_iota(jnp.int32, (lanes, lanes), 0) == lax.broadcasted_iota(
        jnp.int32, (lanes, lanes), 1
    )

    def upright(line):
        return jnp.sum(jnp.where(eye, line, F32(0.0)), axis=1, keepdims=True)

    docs = docs_ref[...].astype(F32)
    for k in range(tokens // lanes):
        column = upright(docs[k : k + 1, :])
        dext[pad + k * lanes : pad + (k + 1) * lanes, :] = jnp.broadcast_to(column, (lanes, lanes))
    end_rows = product(pl.ds(tokens - tail, tail))
    hsend[:, :chan] = end_rows[tail - 8 :]
    hsend[:, chan:] = dext[pad + tokens - 8 : pad + tokens, :]
    own = z * 2 + c
    names = names_ref[...].astype(F32)
    share = share_ref[...]
    for half in range(SPLIT):
        part = slice(half * half_rows, (half + 1) * half_rows)
        meta[own, half] = jnp.zeros(meta.shape[2:], F32)
        meta[own, half, 0:TOPK, :half_rows] = names[:, part]
        meta[own, half, TOPK : 2 * TOPK, :half_rows] = share[:, part]
    fg[t] = ffn_ref[...]
    step_rows = 32

    @pl.loop(0, tokens // step_rows)
    def _(i):
        at = pl.multiple_of(i * step_rows, step_rows)
        ext[pl.ds(pad + at, step_rows), :] = product(pl.ds(at, step_rows))

    n_tri = tri.shape[0]
    row_id = lax.broadcasted_iota(jnp.int32, (n_tri, n_tri), 0)
    col_id = lax.broadcasted_iota(jnp.int32, (n_tri, n_tri), 1)
    tri[...] = (row_id < col_id).astype(F32).astype(BF16)

    def convolve(r):
        @pl.loop(0, piece // step_rows)
        def _(i):
            at = pl.multiple_of(r * piece + i * step_rows, step_rows)
            v = ext[pl.ds(pl.multiple_of(pad - 8 + at, 8), step_rows + 8), :]
            d = dext[pl.ds(pl.multiple_of(pad - 8 + at, 8), step_rows + 8), :]
            doc = d[8:]
            mixed = None
            for k in range(CONV_K):
                by = CONV_K - 1 - k
                if by:
                    same = (pltpu.roll(d, by, 0)[8:] == doc).astype(F32)
                    same = jnp.concatenate([same] * (chan // lanes), axis=1)
                    term = taps_ref[k : k + 1, :] * pltpu.roll(v, by, 0)[8:] * same
                else:
                    term = taps_ref[k : k + 1, :] * v[8:]
                mixed = term if mixed is None else mixed + term
            rows = pl.ds(at, step_rows)
            conv_out = og[rows, :].astype(F32) * mixed
            total = jnp.sum(conv_out * conv_out, axis=1, keepdims=True)
            ssq[rows, :] = jnp.broadcast_to(total, (step_rows, lanes))
            act[rows, :] = (conv_out * mix_ref[...]).astype(BF16)

    eye_piece = lax.broadcasted_iota(jnp.int32, (piece, lanes), 0) == lax.broadcasted_iota(
        jnp.int32, (piece, lanes), 1
    )

    def out_cols(who):
        return pl.ds(pl.multiple_of(who * cols, cols), cols)

    def sums(r):
        part = ssq[r * piece : (r + 1) * piece, :]
        line = jnp.sum(jnp.where(eye_piece, part, F32(0.0)), axis=0, keepdims=True)
        srow[0, r] = jnp.broadcast_to(line, srow.shape[2:])

    def give(r):
        gsend[r] = mm(act[r * piece : (r + 1) * piece, :], wo[:, out_cols(1 - t)]).astype(BF16)

    def send_given(r):
        sum_copy(r).start()
        giv_copy(r).start()

    first[2].wait()
    convolve(GIVEN[0])
    sums(GIVEN[0])
    first[3].wait()
    give(GIVEN[0])
    arrivals = (
        2
        + lo.astype(jnp.int32)
        + hi.astype(jnp.int32)
        + cross_up.astype(jnp.int32)
        + cross_down.astype(jnp.int32)
    )
    pl.semaphore_wait(barrier, arrivals)

    @pl.when(has_next)
    def _():
        halo_copy().start()

    fg_copy().start()
    send_given(GIVEN[0])
    for half in range(SPLIT):
        m_copy(2, z, c, half).start()

    @pl.when(has_prev)
    def _():
        halo_copy().wait_recv()
        ext[pad - 8 : pad, :] = hrecv[:, :chan]
        dext[pad - 8 : pad, :] = hrecv[:, chan:]

    @pl.when(jnp.logical_not(has_prev))
    def _():
        ext[pad - 8 : pad, :] = jnp.zeros((8, chan), F32)
        dext[pad - 8 : pad, :] = jnp.zeros((8, lanes), F32)

    first[4].wait()
    for r in GIVEN[1:]:
        convolve(r)
        sums(r)
        give(r)
        send_given(r)
    fg_copy().wait_recv()

    def picks(zq, cq, half):
        info = meta[zq * 2 + cq, half][:, :half_rows]
        mine = (lax.broadcasted_iota(jnp.int32, (8, half_rows), 0) + s * EXP_DEV).astype(F32)
        hot0 = info[0:1] == mine
        hot1 = info[1:2] == mine
        hot = hot0 | hot1
        earlier = mm(hot.astype(F32).astype(BF16), tri[...])
        position = jnp.where(hot, earlier, F32(-1.0))
        weight = jnp.where(hot0, info[2:3], F32(0.0)) + jnp.where(hot1, info[3:4], F32(0.0))
        place = lax.broadcasted_iota(jnp.int32, (most, half_rows), 0).astype(F32)
        chosen = [(position[e : e + 1] == place).astype(F32) for e in range(EXP_DEV)]
        return chosen, weight

    def norm_scale(parts):
        total = sum(jnp.sum(part * part, axis=1, keepdims=True) for part in parts)
        return lax.rsqrt(total / width + 1e-06)

    def normal_of(parts):
        scale = norm_scale(parts)
        return [(part * scale * fg[h, 0:1, :]).astype(BF16) for h, part in enumerate(parts)]

    def sides():
        return [(0, c), (1, 1 - c)]

    def hidden(zq, half):
        for p, cq in sides():
            chosen, _ = picks(zq, cq, half)
            sel = jnp.concatenate(chosen, axis=0).astype(BF16)
            got = normal_of([mm(sel, blk[zq * 2 + cq, half, h]) for h in range(2)])
            for h in range(2):
                for e in range(EXP_DEV):
                    xs[e, p * most : (p + 1) * most, h * cols : (h + 1) * cols] = got[h][
                        e * most : (e + 1) * most
                    ]
        for e in range(EXP_DEV):
            hid[t, zq, half, e] = silu_mul(mm(xs[e], wg[e]), mm(xs[e], wu[e]))

    def shared(half):
        whole = normal_of([blk[z * 2 + c, half, h].astype(F32) for h in range(2)])
        gate = mm(whole[0], sg[:cols, :]) + mm(whole[1], sg[cols:, :])
        upper = mm(whole[0], su[:cols, :]) + mm(whole[1], su[cols:, :])
        shid[t, half] = silu_mul(gate, upper)

    def results(zq, half):
        hid_copy(zq, half).wait_recv()
        for e in range(EXP_DEV):
            ys[e] = (
                mm(hid[0, zq, half, e], wd[e, :unit, :]) + mm(hid[1, zq, half, e], wd[e, unit:, :])
            ).astype(BF16)
        for p, cq in sides():
            chosen, weight = picks(zq, cq, half)
            parts = []
            for e in range(EXP_DEV):
                scale = jnp.sum(chosen[e] * weight[e : e + 1], axis=1, keepdims=True)
                part = ys[e, p * most : (p + 1) * most, :].astype(F32)
                parts.append((part * scale).astype(BF16))
            sel = jnp.concatenate(chosen, axis=0).astype(BF16)
            into = acc if p == 0 else outgo
            into[zq, half] = lax.dot_general(
                sel,
                jnp.concatenate(parts, axis=0),
                (((0,), (0,)), ((), ())),
                preferred_element_type=F32,
            ).astype(BF16)
        for q in range(2):
            sib_copy(zq, half, q).start()

    def is_end(zq):
        return ((zq > z) & jnp.logical_not(lo)) | ((zq < z) & jnp.logical_not(hi))

    def strip(q):
        return pl.ds(pl.multiple_of(q * piece, piece), piece)

    def on_stream(zq, h, half, q):
        r = half * 2 + q
        rows = pl.ds(pl.multiple_of(r * piece, piece), piece)
        kept = mm(act[rows, :], wo[:, out_cols(t)])
        sum_copy(r).wait_recv()
        line = srow[1, r, 0:1, :]
        theirs = jnp.sum(jnp.where(eye_piece, line, F32(0.0)), axis=1, keepdims=True)
        scale = lax.rsqrt((ssq[rows, 0:1] + theirs) / (2 * chan) + 1e-06)
        giv_copy(r).wait_recv()
        proj = (kept + grecv[r].astype(F32)) * scale
        blk[z * 2 + c, half, t, strip(q), :] = (res[rows, :].astype(F32) + proj).astype(BF16)
        c_copy(z, t, half, q).start()

        @pl.when(r == GIVEN[0])
        def _():
            for load in later:
                load.start()

        @pl.when(r == GIVEN[-1])
        def _():
            for load in later:
                load.wait()

    def on_land(zq, h, half, q):
        @pl.when((h == 0) & (q == 0))
        def _():
            m_copy(2, zq, c, half).wait_recv()
            m_copy(2, zq, c, half).start()

        arrived(zq, side(h), half, q)
        c_copy(zq, side(h), half, q).start()

    def on_z(way):
        def send(zq, h, half, q):
            @pl.when((h == 0) & (q == 0))
            def _():
                m_copy(way, zq, c, half).start()

            z_copy(way, zq, h, half, q).start()

        return send

    def on_across(zq, h, half, q):
        x_copy(zq, half, q).start()

    def on_hidden(zq, h, half, q):
        m_copy(2, zq, 1 - c, half).wait_recv()
        near_by(zq, half).wait_recv()
        hidden(zq, half)
        hid_copy(zq, half).start()

        @pl.when(zq == z)
        def _():
            shared(half)
            sh_copy(half).start()

    def on_result(zq, h, half, q):
        results(zq, half)

    def out_copy(half, p):
        return pltpu.make_async_copy(
            done.at[half, pl.ds(p * part_rows, part_rows)],
            out_hbm.at[pl.ds(half * half_rows + p * part_rows, part_rows)],
            out_sem.at[0],
        )

    def finish(half, p, rows):
        @pl.when(p == 0)
        def _():
            sh_copy(half).wait_recv()

        fin = (
            blk[z * 2 + c, half, t, rows, :].astype(F32)
            + mm(shid[0, half, rows, :], sd[:unit, :])
            + mm(shid[1, half, rows, :], sd[unit:, :])
            + acc[z, half, rows, :].astype(F32)
            + sib[z, half, rows, :].astype(F32)
        )

        @pl.when(lo)
        def _():
            back_copy(z, half, p, z, up).wait_recv()

        @pl.when(hi)
        def _():
            back_copy(z, half, p, n_z, up).wait_recv()

        low = jnp.where(lo, back[z, half, rows, :].astype(F32), F32(0.0))
        high = jnp.where(hi, back[n_z, half, rows, :].astype(F32), F32(0.0))
        done[half, rows, :] = (fin + low + high).astype(BF16)
        out_copy(half, p).start()

    def on_combine(zq, h, half, q):
        p = q * 2 + h
        rows = pl.ds(pl.multiple_of(p * part_rows, part_rows), part_rows)

        @pl.when(h == 0)
        def _():
            sib_copy(zq, half, q).wait_recv()

        @pl.when(zq == z)
        def _():
            finish(half, p, rows)

        @pl.when(zq != z)
        def _():
            @pl.when(is_end(zq))
            def _():
                acc[zq, half, rows, :] = (
                    acc[zq, half, rows, :].astype(F32) + sib[zq, half, rows, :].astype(F32)
                ).astype(BF16)

            @pl.when(jnp.logical_not(is_end(zq)))
            def _():
                back_copy(zq, half, p, zq, up).wait_recv()
                acc[zq, half, rows, :] = (
                    acc[zq, half, rows, :].astype(F32)
                    + sib[zq, half, rows, :].astype(F32)
                    + back[zq, half, rows, :].astype(F32)
                ).astype(BF16)

            @pl.when(zq > z)
            def _():
                back_copy(zq, half, p, zq, up).start()

            @pl.when(zq < z - 1)
            def _():
                back_copy(zq, half, p, zq, down).start()

            @pl.when(zq == z - 1)
            def _():
                back_copy(zq, half, p, n_z, down).start()

    actions = (
        on_stream,
        on_land,
        on_z(0),
        on_z(1),
        on_across,
        on_hidden,
        on_result,
        on_combine,
    )
    order, _ = plan(n_z)
    groups = [-(-len(order[zz]) // 3) for zz in range(n_z)]
    tables = [encode(order[zz], 3 * max(groups)) for zz in range(n_z)]

    def of_zone(numbers):
        return sum((z == zz).astype(jnp.int32) * numbers[zz] for zz in range(n_z))

    def act_on(value):
        def turn(k, rest):
            mark = rest % BASE + 31
            q, half, h = mark % 2, mark // 2 % 2, mark // 4 % 2
            zq, kind = mark // 8 % 4, mark // 32
            for n, action in enumerate(actions):
                @pl.when(kind == n + 1)
                def _():
                    action(zq, h, half, q)

            return rest // BASE

        lax.fori_loop(0, 3, turn, value)

    span = 8
    values = [of_zone([table[g] for table in tables]) for g in range(max(groups))]
    values += [jnp.int32(0)] * (-len(values) % span)

    def among(k, options):
        return sum((k == n).astype(jnp.int32) * option for n, option in enumerate(options))

    count = of_zone(groups)

    @pl.loop(0, len(values) // span)
    def _(page):
        lines = [among(page, values[n::span]) for n in range(span)]

        def line(n, carry):
            act_on(among(n, lines))
            return carry

        lax.fori_loop(0, jnp.clip(count - page * span, 0, span), line, 0)

    @pl.when(has_next)
    def _():
        halo_copy().wait_send()

    fg_copy().wait_send()
    remote(srow.at[0], srow.at[0], sum_sem.at[n_chunks], sum_sem.at[0], peer).wait_send()
    remote(gsend, gsend, giv_recv.at[n_chunks], giv_recv.at[0], peer).wait_send()
    for half in range(SPLIT):
        sh_copy(half).wait_send()
    c_all().wait_send()
    m_sent(2, 0).wait_send()
    remote(hid.at[t], hid.at[t], hid_send.at[0], hid_recv.at[0, 0], peer).wait_send()
    remote(outgo, outgo, sib_send.at[0], sib_recv.at[0, 0, 0], other).wait_send()
    sent = acc.at[pl.ds(0, n_z - 1)]
    remote(sent, sent, back_send.at[0], back_recv.at[0, 0, 0], up).wait_send()

    pltpu.make_async_copy(res, out_hbm, out_sem.at[0]).wait()

    def listed(source, target, half, q):
        inside = [(one > 0) & (one < n_z - 1) for one in (source, target)]
        to_end, from_end, both = [half * 2 + q in kind for kind in FULL]
        return (
            (jnp.logical_not(inside[1]) & to_end)
            | (inside[1] & jnp.logical_not(inside[0]) & from_end)
            | (inside[1] & inside[0] & both)
        )

    for half in range(SPLIT):
        for q in range(2):
            for way, there, target in ((0, hi, z + 1), (1, lo, z - 1)):

                @pl.when(there & listed(z, target, half, q))
                def _():
                    z_copy(way, z, 1, half, q).wait_send()

    @pl.loop(0, n_z)
    def _(zq):
        for way, there in ((0, hi & (zq <= z)), (1, lo & (zq >= z))):

            @pl.when(there)
            def _():
                m_sent(way, zq).wait_send()
                z_sent(way, zq).wait_send()

        near = (zq == z + 1) | (zq == z - 1)
        for half in range(SPLIT):
            for q in range(2):

                @pl.when(jnp.logical_not(near & listed(zq, z, half, q)))
                def _():
                    x_copy(zq, half, q).wait_send()


def fast(
    out_gate,
    in_gate,
    conv_input,
    doc_ids,
    residual,
    conv_taps,
    mix_gain,
    out_weight,
    ffn_gain,
    routing,
    route_weight,
    expert_gate,
    expert_up,
    expert_down,
    shared_gate,
    shared_up,
    shared_down,
):
    tokens, cols = residual.shape
    chan, width = out_weight.shape
    n_tp, n_sp = lax.axis_size("tp"), lax.axis_size("sp")
    n_z = n_sp // 2
    rows = tokens // n_tp
    experts = n_sp * EXP_DEV
    most = max(1, 2 * rows * TOPK // experts)
    lanes = 128
    piece = rows // 2
    blocks = n_sp
    unit = expert_gate.shape[2]
    vm = pl.BlockSpec(memory_space=pltpu.VMEM)
    hbm = pl.BlockSpec(memory_space=pl.ANY)
    dma = pltpu.SemaphoreType.DMA
    return pl.pallas_call(
        functools.partial(layer_kernel, n_z, most),
        out_shape=jax.ShapeDtypeStruct((tokens, cols), BF16),
        in_specs=[hbm] * 5 + [vm] * 6 + [hbm] * 6,
        out_specs=hbm,
        scratch_shapes=[
            pltpu.VMEM((tokens, chan), BF16),
            pltpu.VMEM((tokens, chan), BF16),
            pltpu.VMEM((tokens, chan), BF16),
            pltpu.VMEM((tokens, cols), BF16),
            pltpu.VMEM((chan, width), BF16),
            pltpu.VMEM(expert_gate.shape, BF16),
            pltpu.VMEM(expert_up.shape, BF16),
            pltpu.VMEM(expert_down.shape, BF16),
            pltpu.VMEM(shared_gate.shape, BF16),
            pltpu.VMEM(shared_up.shape, BF16),
            pltpu.VMEM(shared_down.shape, BF16),
            pltpu.VMEM((tokens + 16, chan), F32),
            pltpu.VMEM((tokens + 16, lanes), F32),
            pltpu.VMEM((8, chan + lanes), F32),
            pltpu.VMEM((8, chan + lanes), F32),
            pltpu.VMEM((tokens, chan), BF16),
            pltpu.VMEM((tokens, lanes), F32),
            pltpu.VMEM((2, 2 * SPLIT, 8, lanes), F32),
            pltpu.VMEM((2 * SPLIT, piece, cols), BF16),
            pltpu.VMEM((2 * SPLIT, piece, cols), BF16),
            pltpu.VMEM((2, 1, cols), F32),
            pltpu.VMEM((rows, rows), BF16),
            pltpu.VMEM((blocks, SPLIT, 2, rows, cols), BF16),
            pltpu.VMEM((blocks, SPLIT, 8, rows + -rows % lanes), F32),
            pltpu.VMEM((EXP_DEV, 2 * most, width), BF16),
            pltpu.VMEM((2, n_z, SPLIT, EXP_DEV, 2 * most, unit), BF16),
            pltpu.VMEM((2, SPLIT, rows, unit), BF16),
            pltpu.VMEM((EXP_DEV, 2 * most, cols), BF16),
            pltpu.VMEM((n_z, SPLIT, rows, cols), BF16),
            pltpu.VMEM((n_z, SPLIT, rows, cols), BF16),
            pltpu.VMEM((n_z, SPLIT, rows, cols), BF16),
            pltpu.VMEM((n_z + 1, SPLIT, rows, cols), BF16),
            pltpu.VMEM((SPLIT, rows, cols), BF16),
            dma((11,)),
            dma((2,)),
            dma((2 * SPLIT + 1,)),
            dma((2,)),
            dma((2 * SPLIT + 1,)),
            dma((2, n_z + 2 * SPLIT)),
            dma((n_z, SPLIT, 2)),
            dma((1,)),
            dma((n_z, 2, SPLIT, 2)),
            dma((n_z, SPLIT)),
            dma((2 * n_z + 1,)),
            dma((blocks, SPLIT)),
            dma((1,)),
            dma((n_z, SPLIT)),
            dma((SPLIT,)),
            dma((SPLIT,)),
            dma((1,)),
            dma((n_z, SPLIT, 2)),
            dma((1,)),
            dma((n_z + 1, SPLIT, 4)),
            dma((1,)),
        ],
        compiler_params=pltpu.CompilerParams(
            collective_id=0, has_side_effects=True, vmem_limit_bytes=64 * 1024 * 1024 - 65536
        ),
    )(
        out_gate,
        in_gate,
        conv_input,
        residual,
        out_weight,
        doc_ids.reshape(tokens // lanes, lanes),
        conv_taps,
        mix_gain[None, :],
        ffn_gain[None, :],
        routing.T,
        route_weight.T,
        expert_gate,
        expert_up,
        expert_down,
        shared_gate,
        shared_up,
        shared_down,
    )


def fits(mesh):
    return mesh.shape["tp"] == 2 and mesh.shape["sp"] in (4, 6, 8)


def solution(mesh):
    return jax.shard_map(
        fast if fits(mesh) else body,
        mesh=mesh,
        in_specs=(
            P(("grp", "sp"), "tp"),
            P(("grp", "sp"), "tp"),
            P(("grp", "sp"), "tp"),
            P(("grp", "sp")),
            P(("grp", "sp"), "tp"),
            P(None, "tp"),
            P("tp"),
            P("tp", None),
            P("tp"),
            P(("grp", "sp"), None),
            P(("grp", "sp"), None),
            P("sp", None, "tp"),
            P("sp", None, "tp"),
            P("sp", None, "tp"),
            P(None, "tp"),
            P(None, "tp"),
            P(None, "tp"),
        ),
        out_specs=P(("grp", "sp"), "tp"),
        check_vma=False,
    )
```
